256 devices in a mesh: grp: 2 (over y), sp: 16 (over z), tp: 8 (over x, core).
Axes of the slice: x: 4, y: 2, z: 16, core: 2. Of those that a mesh axis runs over, the one named last changes fastest.
The devices are a block of a 4x16x16 slice.
Arguments:
- residual: bfloat16 [16384, 2048], P(('grp', 'sp')), parts along dimension 0, may hold values from -6 to 6
- values: bfloat16 [16384, 4096], P(('grp', 'sp'), 'tp'), parts along dimension 0, may hold values from -6 to 6
- out_gate: bfloat16 [16384, 4096], P(('grp', 'sp'), 'tp'), parts along dimension 0, may hold values from -6 to 6
- writes: bfloat16 [16384, 1024], P(('grp', 'sp'), 'tp'), parts along dimension 0, may hold values from -6 to 6
- reads: bfloat16 [16384, 1024], P(('grp', 'sp'), 'tp'), parts along dimension 0, may hold values from -6 to 6
- step_raw: bfloat16 [64, 16384], P('tp', ('grp', 'sp')), parts along dimension 1, may hold values from -4.5 to 4.5
- decay_rate: float32 [64], P('tp'), may hold values from 0 to 0.1
- decay_jump: float32 [64, 16384], P('tp', ('grp', 'sp')), parts along dimension 1, may hold values from -0.7 to 0
- documents: int32 [16384], P(('grp', 'sp')), parts along dimension 0, may hold values from 0 to 7, never falling along the last dimension, each value on 1 to 1536 neighbouring positions
- taps_values: bfloat16 [4, 4096], P(None, 'tp'), may hold values from -3 to 3
- taps_write: bfloat16 [4, 1024], P(None, 'tp'), may hold values from -3 to 3
- taps_read: bfloat16 [4, 1024], P(None, 'tp'), may hold values from -3 to 3
- mixer_gain: bfloat16 [4096], P('tp'), may hold values from 0.099609375 to 1.8984375
- mixer_out: bfloat16 [4096, 2048], P('tp'), may hold values from -0.09375 to 0.09375
- channel_gain: bfloat16 [2048], replicated, may hold values from 0.099609375 to 1.8984375
- gate_weight: bfloat16 [2048, 5632], P('sp', 'tp'), may hold values from -0.125 to 0.125
- up_weight: bfloat16 [2048, 5632], P('sp', 'tp'), may hold values from -0.125 to 0.125
- down_rows: bfloat16 [2048, 5632], P('sp', 'tp'), may hold values from -0.078125 to 0.078125
Outputs:
- layer_out: bfloat16 [16384, 2048], P(('grp', 'sp'), 'tp'), parts along dimension 0
The draws below stay inside these ranges and needn't reach their ends.
There are 2 independent parts, one for each index of `grp`. The reference program is written for one: setup_inputs(seed, part) draws one part's arguments, and reference() takes and returns one part's arrays. A program takes and returns all parts, laid end to end along the dimension named above; an argument that names none is the same for every part. Nothing has to cross between parts.
Inputs may be any that keep to these rules, and one draw needn't show every extreme that they name: `documents`: document numbers never fall along the sequence; a document starts where the number changes, and is one to 1536 positions long.
All inputs are finite; a program needn't handle non-finite values.
Results may differ from the reference program's by a relative error of at most 0.017.
Values may be sent and summed in bfloat16 or wider, within the bound.
No kernel may reach another device: no remote copies, remote signals or barrier semaphores. Data moves between devices by JAX's collectives and lax.ppermute only.
A program may use at most 64 MiB of HBM per device.

```python
import math
import jax
import jax.numpy as jnp
import numpy as np
from jax import lax

D = 2048
HEADS = 64
HDIM = 64
GROUPS = 8
STATE = 128
CONV = 4
FF = 5632
BLOCK = 128
TOK_DEV = 512
SEQ = 8192
INNER = 4096
GN = 1024
DOCS = 8
DOC_MOST = 1536
N_TP = 8


def draw_step_raw(key, part):
    first_key = jax.random.fold_in(key, 11)
    second_key = jax.random.fold_in(key, 12)
    blocks = SEQ // TOK_DEV
    base = jnp.clip(jax.random.normal(first_key, (HEADS, SEQ), jnp.float32), -3.0, 3.0)
    offset = jax.random.uniform(second_key, (HEADS, blocks, 1), jnp.float32, -1.5, 1.5)
    return (base.reshape(HEADS, blocks, TOK_DEV) + offset).reshape(HEADS, SEQ).astype(jnp.bfloat16)


def draw_decay_rate(key, part):
    pick_key = jax.random.fold_in(key, 21)
    slow_key = jax.random.fold_in(key, 22)
    quick_key = jax.random.fold_in(key, 23)
    order = jax.random.permutation(pick_key, HEADS)
    quick_heads = order < HEADS // 2
    slow = jnp.exp(jax.random.uniform(slow_key, (HEADS,), jnp.float32, math.log(0.05), math.log(0.5))) / SEQ
    quick = jnp.exp(jax.random.uniform(quick_key, (HEADS,), jnp.float32, math.log(0.03), math.log(0.1)))
    return jnp.where(quick_heads, quick, slow).astype(jnp.float32)


def draw_decay_jump(key, part):
    spots_key = jax.random.fold_in(key, 31)
    depth_key = jax.random.fold_in(key, 32)
    spots = jax.random.randint(spots_key, (HEADS, 4, 1), 0, SEQ)
    positions = jnp.arange(SEQ, dtype=jnp.int32)
    hit_mask = jnp.any(spots == positions[None, None, :], axis=1)
    depth = jnp.log(jax.random.uniform(depth_key, (HEADS, SEQ), jnp.float32, 0.5, 0.8))
    return jnp.where(hit_mask, depth, 0.0).astype(jnp.float32)


def block_scale(own_key, extent, split, least, high):
    loudness = 1.0
    for axis_at, blocks in split:
        steps = jax.random.uniform(jax.random.fold_in(jax.random.fold_in(own_key, 6), axis_at), (blocks,), jnp.float32, least / len(split), high / len(split))
        loudness = loudness * jnp.repeat(jnp.exp(steps), extent[axis_at] // blocks).reshape((-1,) + (1,) * (len(extent) - 1 - axis_at))
    return loudness


def split_up(amount, total, most, slope):
    loads = [(1 << 20) // math.isqrt(standing ** slope) + 1 for standing in range(2, amount + 1)]
    surplus, counts = total - most - (amount - 1), [1] * (amount - 1)
    while surplus > 0:
        free = [i for i in range(amount - 1) if counts[i] < most]
        whole, left = sum([loads[i] for i in free]), surplus
        for i in free:
            addition = min(most - counts[i], max(1, left * loads[i] // whole), surplus)
            counts[i] = counts[i] + addition
            surplus = surplus - addition
    return np.array([most] + counts)


def uneven(key, count, total, most, skew):
    if count == 2:
        one = jax.random.randint(key, (), max(1, total - most), min(most, total - 1) + 1)
        return jnp.stack([one, total - one])
    lengths = jnp.asarray(split_up(count, total, most, skew), jnp.int32)
    pairs = (count - 1) // 2
    donor, taker = lengths[1:1 + 2 * pairs:2], lengths[2:2 + 2 * pairs:2]
    margin = jnp.minimum(donor - 1, most - taker)
    shifted = jax.random.randint(jax.random.fold_in(key, 1), (pairs,), 0, 1 << 20) % (margin + 1)
    lengths = lengths.at[1:1 + 2 * pairs:2].set(donor - shifted).at[2:2 + 2 * pairs:2].set(taker + shifted)
    return lengths[jax.random.permutation(jax.random.fold_in(key, 2), count)]


def gaussian(rng, extent, scale, limit, split=(), kind=jnp.bfloat16):
    entries = jax.random.normal(rng, extent, jnp.float32) * scale
    if len(split) > 0:
        entries = block_scale(rng, extent, split, -0.22, 0.18) * entries
    return jnp.clip(entries, min=-limit, max=limit).astype(kind)


def setup_inputs(seed: int = 0, part: int = 0) -> dict:
    arg_keys = jax.random.split(jax.random.key(seed), 19)
    own_keys = jax.random.split(jax.random.fold_in(arg_keys[18], part), 19)
    residual = gaussian(own_keys[0], (SEQ, D), 1.0, 6.0, ((0, 16),))
    values = gaussian(own_keys[1], (SEQ, INNER), 1.0, 6.0, ((0, 16), (1, 8)))
    out_gate = gaussian(own_keys[2], (SEQ, INNER), 1.0, 6.0, ((0, 16), (1, 8)))
    writes = gaussian(own_keys[3], (SEQ, GN), 1.0, 6.0, ((0, 16), (1, 8)))
    reads = gaussian(own_keys[4], (SEQ, GN), 1.0, 6.0, ((0, 16), (1, 8)))
    step_raw = draw_step_raw(jax.random.fold_in(jax.random.fold_in(arg_keys[18], part), 71), part)
    decay_rate = draw_decay_rate(jax.random.fold_in(arg_keys[18], 71), part)
    decay_jump = draw_decay_jump(jax.random.fold_in(jax.random.fold_in(arg_keys[18], part), 71), part)
    documents = jnp.searchsorted(jnp.cumsum(uneven(own_keys[8], DOCS, SEQ, DOC_MOST, 0)), jnp.arange(SEQ), side="right").astype(jnp.int32)
    taps_values = gaussian(arg_keys[9], (CONV, INNER), CONV ** -0.5, 3.0, ((1, 8),))
    taps_write = gaussian(arg_keys[10], (CONV, GN), CONV ** -0.5, 3.0, ((1, 8),))
    taps_read = gaussian(arg_keys[11], (CONV, GN), CONV ** -0.5, 3.0, ((1, 8),))
    mixer_gain = jnp.clip(1.0 + 0.18 * jax.random.normal(arg_keys[12], (INNER,), jnp.float32), 0.099609375, 1.8984375).astype(jnp.bfloat16)
    mixer_out = gaussian(arg_keys[13], (INNER, D), INNER ** -0.5, 0.09375, ((0, 8),))
    channel_gain = jnp.clip(1.0 + 0.18 * jax.random.normal(arg_keys[14], (D,), jnp.float32), 0.099609375, 1.8984375).astype(jnp.bfloat16)
    gate_weight = gaussian(arg_keys[15], (D, FF), D ** -0.5, 0.125, ((0, 16), (1, 8)))
    up_weight = gaussian(arg_keys[16], (D, FF), D ** -0.5, 0.125, ((0, 16), (1, 8)))
    down_rows = gaussian(arg_keys[17], (D, FF), FF ** -0.5, 0.078125, ((0, 16), (1, 8)))
    return dict(residual=residual, values=values, out_gate=out_gate, writes=writes, reads=reads, step_raw=step_raw, decay_rate=decay_rate, decay_jump=decay_jump, documents=documents, taps_values=taps_values, taps_write=taps_write, taps_read=taps_read, mixer_gain=mixer_gain, mixer_out=mixer_out, channel_gain=channel_gain, gate_weight=gate_weight, up_weight=up_weight, down_rows=down_rows)


norm_eps = 1e-06

def short_filter(rows, row_docs, taps):
    width = taps.shape[0]
    count = rows.shape[0] - width + 1
    own_docs = row_docs[width - 1:]
    total = jnp.zeros((count, rows.shape[1]), jnp.float32)
    for offset in range(width):
        alive = (row_docs[offset:offset + count] == own_docs).astype(jnp.float32)
        total = total + rows[offset:offset + count].astype(jnp.float32) * taps[offset].astype(jnp.float32)[None, :] * alive[:, None]
    return jax.nn.silu(total).astype(jnp.bfloat16)

def block_pieces(values, writes, reads, step_size, log_decay, segment, heads_per, block):
    span = values.shape[0]
    block_count = span // block
    heads = step_size.shape[0]
    groups = heads // heads_per
    head_size = values.shape[1] // heads
    state_size = writes.shape[1] // groups
    value_blocks = values.astype(jnp.float32).reshape(block_count, block, groups, heads_per, head_size)
    write_blocks = writes.astype(jnp.float32).reshape(block_count, block, groups, state_size)
    read_blocks = reads.astype(jnp.float32).reshape(block_count, block, groups, state_size)
    block_docs = segment.reshape(block_count, block)
    step_blocks = step_size.reshape(groups, heads_per, block_count, block)
    running = jnp.cumsum(log_decay.reshape(groups, heads_per, block_count, block), axis=3)
    target = lax.broadcasted_iota(jnp.int32, (block, block), 0)
    source = lax.broadcasted_iota(jnp.int32, (block, block), 1)
    allowed = (target >= source)[None] & (block_docs[:, :, None] == block_docs[:, None, :])
    scores = jnp.einsum('kign,kjgn->gkij', read_blocks, write_blocks, precision=lax.Precision.HIGHEST)
    spread = running[..., :, None] - running[..., None, :]
    decay = jnp.exp(jnp.where(allowed[None, None], spread, -jnp.inf))
    weights = (decay * scores[:, None] * step_blocks[..., None, :]).astype(jnp.bfloat16)
    inner = jnp.einsum('gekij,kjgep->kigep', weights.astype(jnp.float32), value_blocks, precision=lax.Precision.HIGHEST)
    last_total = running[..., -1]
    same_end = (block_docs == block_docs[:, -1:]).astype(jnp.float32)
    end_factor = jnp.exp(last_total[..., None] - running) * step_blocks * same_end[None, None]
    scaled = (value_blocks * jnp.transpose(end_factor, (2, 3, 0, 1))[..., None]).astype(jnp.bfloat16)
    states = jnp.einsum('kjgep,kjgn->kgepn', scaled.astype(jnp.float32), write_blocks, precision=lax.Precision.HIGHEST)
    return (inner, states, last_total, running, block_docs)

def block_passing(last_total, block_docs, prior_docs):
    return jnp.exp(last_total) * (block_docs[:, -1] == prior_docs).astype(jnp.float32)[None, None]

def carry_states(states, passing, start):

    def advance(held, entry):
        factor, fresh = entry
        return (factor[..., None, None] * held + fresh, held)
    final, entering = lax.scan(advance, start, (jnp.moveaxis(passing, 2, 0), states))
    return (entering, final)

def read_states(reads, entering, running, block_docs, prior_docs):
    block_count, block = block_docs.shape
    groups = entering.shape[1]
    read_blocks = reads.astype(jnp.float32).reshape(block_count, block, groups, -1)
    alive = (block_docs == prior_docs[:, None]).astype(jnp.float32)
    reach = jnp.exp(running) * alive[None, None]
    taken = jnp.einsum('kign,kgepn->kigep', read_blocks, entering, precision=lax.Precision.HIGHEST)
    return taken * jnp.transpose(reach, (2, 3, 0, 1))[..., None]

def sliced_product(left, right_rows, slices):
    width = left.shape[1] // slices
    total = jnp.zeros((left.shape[0], right_rows.shape[0]), jnp.float32)
    for slice_index in range(slices):
        piece = left[:, slice_index * width:(slice_index + 1) * width]
        other = right_rows[:, slice_index * width:(slice_index + 1) * width]
        term = jnp.dot(piece, other.T, preferred_element_type=jnp.float32).astype(jnp.bfloat16)
        term = lax.optimization_barrier(term)
        total = total + term.astype(jnp.float32)
    return total

def reference(residual, values, out_gate, writes, reads, step_raw, decay_rate, decay_jump, documents, taps_values, taps_write, taps_read, mixer_gain, mixer_out, channel_gain, gate_weight, up_weight, down_rows):
    edge = CONV - 1
    segment = documents.astype(jnp.float32)
    row_docs = jnp.concatenate([jnp.full((edge,), -1.0, jnp.float32), segment])

    def padded(rows):
        return jnp.concatenate([jnp.zeros((edge, rows.shape[1]), rows.dtype), rows])
    short_values = short_filter(padded(values), row_docs, taps_values)
    short_writes = short_filter(padded(writes), row_docs, taps_write)
    short_reads = short_filter(padded(reads), row_docs, taps_read)
    step_size = jax.nn.softplus(step_raw.astype(jnp.float32))
    log_decay = decay_jump - decay_rate[:, None] * step_size
    heads_per = HEADS // GROUPS

    def advance(carry, index):
        held, prior = carry
        first = index * BLOCK
        reads_here = lax.dynamic_slice_in_dim(short_reads, first, BLOCK, 0)
        inner, states, last_total, running, block_docs = block_pieces(lax.dynamic_slice_in_dim(short_values, first, BLOCK, 0), lax.dynamic_slice_in_dim(short_writes, first, BLOCK, 0), reads_here, lax.dynamic_slice_in_dim(step_size, first, BLOCK, 1), lax.dynamic_slice_in_dim(log_decay, first, BLOCK, 1), lax.dynamic_slice_in_dim(segment, first, BLOCK, 0), heads_per, BLOCK)
        prior_docs = prior.reshape(1)
        passing = block_passing(last_total, block_docs, prior_docs)
        entering, final = carry_states(states, passing, held)
        mixed = inner + read_states(reads_here, entering, running, block_docs, prior_docs)
        return ((final, block_docs[0, -1]), mixed.reshape(BLOCK, INNER))
    start_state = jnp.zeros((GROUPS, heads_per, HDIM, STATE), jnp.float32)
    start_doc = jnp.asarray(-1.0, jnp.float32)
    indices = jnp.arange(SEQ // BLOCK, dtype=jnp.int32)
    _, outputs = lax.scan(advance, (start_state, start_doc), indices)
    mixed = outputs.reshape(SEQ, INNER)
    gated = mixed * jax.nn.silu(out_gate.astype(jnp.float32))
    grouped = gated.reshape(SEQ, GROUPS, INNER // GROUPS)
    grouped = grouped * lax.rsqrt(lax.optimization_barrier(jnp.mean(grouped * grouped, axis=2, keepdims=True)) + norm_eps)
    mixer_in = (grouped.reshape(SEQ, INNER) * mixer_gain.astype(jnp.float32)[None, :]).astype(jnp.bfloat16)
    mix = sliced_product(mixer_in, mixer_out.T, N_TP)
    after = (residual.astype(jnp.float32) + mix).astype(jnp.bfloat16)
    after_wide = after.astype(jnp.float32)
    normal = after_wide * lax.rsqrt(lax.optimization_barrier(jnp.mean(after_wide * after_wide, axis=1, keepdims=True)) + norm_eps)
    normal = (normal * channel_gain.astype(jnp.float32)[None, :]).astype(jnp.bfloat16)
    gate = jnp.dot(normal, gate_weight, preferred_element_type=jnp.float32)
    up = jnp.dot(normal, up_weight, preferred_element_type=jnp.float32)
    hidden = (jax.nn.silu(gate) * up).astype(jnp.bfloat16)
    down = sliced_product(hidden, down_rows, N_TP)
    return (after.astype(jnp.float32) + down).astype(jnp.bfloat16)
```

```python
import jax
import jax.numpy as jnp
from jax import lax
from jax.sharding import PartitionSpec as P

HEADS = 64
GROUPS = 8
BLOCK = 128


norm_eps = 1e-06


def from_behind(value, axis, by):
    peers = lax.axis_size(axis)
    pairs = [(i, i + by) for i in range(peers) if 0 <= i + by < peers]
    return lax.ppermute(value, axis, pairs)


def state_behind(final, decay, axis):
    shape = final.shape
    rows = final.reshape(-1, shape[-1])
    tail = jnp.broadcast_to(decay.reshape(-1, 1), (decay.size, shape[-1]))
    packed = jnp.concatenate([rows, tail]).astype(jnp.bfloat16)
    first = from_behind(packed, axis, 1).astype(jnp.float32)
    near = first[: len(rows)].reshape(shape)
    near_decay = first[len(rows) :, 0].reshape(decay.shape)
    two = (final + decay[..., None, None] * near).astype(jnp.bfloat16)
    far = from_behind(two, axis, 2).astype(jnp.float32)
    return near + near_decay[..., None, None] * far


def cut_along(value, dim, peers):
    shape = value.shape
    blocks = value.reshape(*shape[:dim], peers, shape[dim] // peers, *shape[dim + 1 :])
    return jnp.moveaxis(blocks, dim, 0)


def sum_at_owner(value, axis, dim):
    peers = lax.axis_size(axis)
    blocks = lax.all_to_all(cut_along(value, dim, peers), axis, 0, 0, tiled=True)
    return jnp.sum(blocks.astype(jnp.float32), axis=0)


def laid_out(blocks, dim):
    blocks = jnp.moveaxis(blocks, 0, dim)
    shape = blocks.shape
    return blocks.reshape(*shape[:dim], shape[dim] * shape[dim + 1], *shape[dim + 2 :])


def sent_to_all(value, axis):
    peers = lax.axis_size(axis)
    return lax.all_to_all(
        jnp.broadcast_to(value[None], (peers, *value.shape)), axis, 0, 0, tiled=True
    )


def gather_directly(value, axis, dim):
    return laid_out(sent_to_all(value, axis), dim)


def in_one_piece(arrays, axis, dim, along):
    both = jnp.concatenate(arrays, axis=along)
    result, at, gathered = (lax.all_gather(both, axis, axis=dim, tiled=True), 0, [])
    for a in arrays:
        gathered.append(lax.slice_in_dim(result, at, at + a.shape[along], axis=along))
        at += a.shape[along]
    return tuple(gathered)


def short_filter(rows, row_docs, taps):
    width = taps.shape[0]
    count = rows.shape[0] - width + 1
    own_docs = row_docs[width - 1 :]
    total = jnp.zeros((count, rows.shape[1]), jnp.float32)
    for offset in range(width):
        alive = (row_docs[offset : offset + count] == own_docs).astype(jnp.float32)
        total = (
            total
            + rows[offset : offset + count].astype(jnp.float32)
            * taps[offset].astype(jnp.float32)[None, :]
            * alive[:, None]
        )
    return jax.nn.silu(total).astype(jnp.bfloat16)


def block_pieces(values, writes, reads, step_size, log_decay, segment, heads_per, block):
    span = values.shape[0]
    block_count = span // block
    heads = step_size.shape[0]
    groups = heads // heads_per
    head_size = values.shape[1] // heads
    state_size = writes.shape[1] // groups
    value_blocks = values.reshape(block_count, block, groups, heads_per, head_size)
    write_blocks = writes.reshape(block_count, block, groups, state_size)
    read_blocks = reads.reshape(block_count, block, groups, state_size)
    block_docs = segment.reshape(block_count, block)
    step_blocks = step_size.reshape(groups, heads_per, block_count, block)
    running = jnp.cumsum(log_decay.reshape(groups, heads_per, block_count, block), axis=3)
    target = lax.broadcasted_iota(jnp.int32, (block, block), 0)
    source = lax.broadcasted_iota(jnp.int32, (block, block), 1)
    allowed = (target >= source)[None] & (block_docs[:, :, None] == block_docs[:, None, :])
    scores = jnp.einsum(
        "kign,kjgn->gkij", read_blocks, write_blocks, preferred_element_type=jnp.float32
    )
    spread = running[..., :, None] - running[..., None, :]
    decay = jnp.exp(jnp.where(allowed[None, None], spread, -jnp.inf))
    weights = (decay * scores[:, None] * step_blocks[..., None, :]).astype(jnp.bfloat16)
    inner = jnp.einsum(
        "gekij,kjgep->kigep", weights, value_blocks, preferred_element_type=jnp.float32
    )
    last_total = running[..., -1]
    same_end = (block_docs == block_docs[:, -1:]).astype(jnp.float32)
    end_factor = jnp.exp(last_total[..., None] - running) * step_blocks * same_end[None, None]
    scaled = (
        value_blocks.astype(jnp.float32) * jnp.transpose(end_factor, (2, 3, 0, 1))[..., None]
    ).astype(jnp.bfloat16)
    states = jnp.einsum(
        "kjgep,kjgn->kgepn", scaled, write_blocks, preferred_element_type=jnp.float32
    )
    return (inner, states, last_total, running, block_docs)


def block_passing(last_total, block_docs, prior_docs):
    return jnp.exp(last_total) * (block_docs[:, -1] == prior_docs).astype(jnp.float32)[None, None]


def carry_states(states, passing, start):

    def advance(held, entry):
        factor, fresh = entry
        return (factor[..., None, None] * held + fresh, held)

    final, entering = lax.scan(advance, start, (jnp.moveaxis(passing, 2, 0), states))
    return (entering, final)


def read_states(reads, entering, running, block_docs, prior_docs):
    block_count, block = block_docs.shape
    groups = entering.shape[1]
    read_blocks = reads.astype(jnp.float32).reshape(block_count, block, groups, -1)
    alive = (block_docs == prior_docs[:, None]).astype(jnp.float32)
    reach = jnp.exp(running) * alive[None, None]
    taken = jnp.einsum("kign,kgepn->kigep", read_blocks, entering)
    return taken * jnp.transpose(reach, (2, 3, 0, 1))[..., None]


def down_product(hidden, rows):
    return lax.dot_general(
        hidden, rows, (((1,), (1,)), ((), ())), preferred_element_type=jnp.float32
    )


def on_device(
    residual,
    values,
    out_gate,
    writes,
    reads,
    step_raw,
    decay_rate,
    decay_jump,
    documents,
    taps_values,
    taps_write,
    taps_read,
    mixer_gain,
    mixer_out,
    channel_gain,
    gate_weight,
    up_weight,
    down_rows,
):
    tokens = values.shape[0]
    edge = taps_values.shape[0] - 1
    late_weights = in_one_piece((gate_weight, up_weight, down_rows), "sp", 0, 1)
    segment = documents.astype(jnp.float32)
    last_rows = jnp.concatenate(
        [
            values[tokens - edge :],
            writes[tokens - edge :],
            reads[tokens - edge :],
            jnp.broadcast_to(segment[tokens - edge :, None].astype(jnp.bfloat16), (edge, 128)),
        ],
        axis=1,
    )
    before = from_behind(last_rows, "sp", 1)
    wide, narrow = values.shape[1], writes.shape[1]
    before_values = before[:, :wide]
    before_writes = before[:, wide : wide + narrow]
    before_reads = before[:, wide + narrow : wide + 2 * narrow]
    before_docs = before[:, wide + 2 * narrow].astype(jnp.float32)
    before_docs = jnp.where(lax.axis_index("sp") == 0, -1.0, before_docs)
    row_docs = jnp.concatenate([before_docs, segment])
    short_values = short_filter(jnp.concatenate([before_values, values]), row_docs, taps_values)
    short_writes = short_filter(jnp.concatenate([before_writes, writes]), row_docs, taps_write)
    short_reads = short_filter(jnp.concatenate([before_reads, reads]), row_docs, taps_read)
    step_size = jax.nn.softplus(step_raw.astype(jnp.float32))
    log_decay = decay_jump - decay_rate[:, None] * step_size
    heads_per = HEADS // GROUPS
    inner, states, last_total, running, block_docs = block_pieces(
        short_values, short_writes, short_reads, step_size, log_decay, segment, heads_per, BLOCK
    )
    groups = states.shape[1]
    local_prior = jnp.concatenate([jnp.full((1,), -1.0, jnp.float32), block_docs[:-1, -1]])
    zero_state = jnp.zeros(states.shape[1:], jnp.float32)
    entering, final = carry_states(
        states, block_passing(last_total, block_docs, local_prior), zero_state
    )
    behind_doc = before_docs[edge - 1 :]
    whole_decay = jnp.exp(jnp.sum(last_total, axis=2)) * (behind_doc[0] == segment[-1]).astype(
        jnp.float32
    )
    held = state_behind(final, whole_decay, "sp")
    prior_docs = jnp.concatenate([behind_doc, block_docs[:-1, -1]])
    passing_in = block_passing(last_total, block_docs, prior_docs)
    gains = jnp.cumprod(passing_in, axis=2)
    gains = jnp.concatenate([jnp.ones_like(gains[..., :1]), gains[..., :-1]], axis=2)
    entering = entering + jnp.moveaxis(gains, 2, 0)[..., None, None] * held[None]
    mixed = inner + read_states(short_reads, entering, running, block_docs, prior_docs)
    gated = mixed.reshape(tokens, -1) * jax.nn.silu(out_gate.astype(jnp.float32))
    grouped = gated.reshape(tokens, groups, -1)
    grouped = grouped * lax.rsqrt(jnp.mean(grouped * grouped, axis=2, keepdims=True) + norm_eps)
    mixer_in = (grouped.reshape(tokens, -1) * mixer_gain.astype(jnp.float32)[None, :]).astype(
        jnp.bfloat16
    )
    partial_value = jnp.dot(mixer_in, mixer_out, preferred_element_type=jnp.float32)
    share = residual.shape[1] // lax.axis_size("tp")
    mix_share = sum_at_owner(partial_value.astype(jnp.bfloat16), "tp", 1)
    own_residual = lax.dynamic_slice_in_dim(residual, lax.axis_index("tp") * share, share, 1)
    own_after = (own_residual.astype(jnp.float32) + mix_share).astype(jnp.bfloat16)
    after = gather_directly(own_after, "tp", 1)
    after_wide = after.astype(jnp.float32)
    normal = after_wide * lax.rsqrt(
        jnp.mean(after_wide * after_wide, axis=1, keepdims=True) + norm_eps
    )
    normal = (normal * channel_gain.astype(jnp.float32)[None, :]).astype(jnp.bfloat16)
    gate = jnp.dot(normal, late_weights[0], preferred_element_type=jnp.float32)
    up = jnp.dot(normal, late_weights[1], preferred_element_type=jnp.float32)
    hidden = (jax.nn.silu(gate) * up).astype(jnp.bfloat16)
    down = down_product(hidden, late_weights[2])
    down_share = sum_at_owner(down.astype(jnp.bfloat16), "tp", 1)
    return (own_after.astype(jnp.float32) + down_share).astype(jnp.bfloat16)


def solution(mesh):
    return jax.shard_map(
        on_device,
        mesh=mesh,
        in_specs=(
            P(("grp", "sp"), None),
            P(("grp", "sp"), "tp"),
            P(("grp", "sp"), "tp"),
            P(("grp", "sp"), "tp"),
            P(("grp", "sp"), "tp"),
            P("tp", ("grp", "sp")),
            P("tp"),
            P("tp", ("grp", "sp")),
            P(("grp", "sp")),
            P(None, "tp"),
            P(None, "tp"),
            P(None, "tp"),
            P("tp"),
            P("tp", None),
            P(),
            P("sp", "tp"),
            P("sp", "tp"),
            P("sp", "tp"),
        ),
        out_specs=P(("grp", "sp"), "tp"),
        check_vma=False,
    )
```

```python
import functools

import jax
import jax.numpy as jnp
from jax import lax
from jax.experimental import pallas as pl
from jax.experimental.pallas import tpu as pltpu
from jax.sharding import PartitionSpec as P

HEADS = 64
GROUPS = 8
BLOCK = 128
EDGE = 16
LANES = 128

norm_eps = 1e-06

F32 = jnp.float32
BF16 = jnp.bfloat16


def from_behind(value, axis, by):
    peers = lax.axis_size(axis)
    pairs = [(i, i + by) for i in range(peers) if 0 <= i + by < peers]
    return lax.ppermute(value, axis, pairs)


def silu(x):
    return x * jax.nn.sigmoid(x)


def shape(dims, kind):
    return jax.ShapeDtypeStruct(dims, kind)


def transposed(rows):
    return jnp.transpose(rows, (1, 0))


def doc_rows(docs_ref):
    return docs_ref[...].astype(F32)


def running_sum(x):
    lane = lax.broadcasted_iota(jnp.int32, x.shape, 1)
    shift = 1
    while shift < x.shape[1]:
        x = x + jnp.where(lane >= shift, pltpu.roll(x, shift, 1), 0.0)
        shift *= 2
    return x


def per_channel(columns, pair, rows):
    lane = lax.broadcasted_iota(jnp.int32, (rows, LANES), 1)
    return jnp.where(
        lane < LANES // 2,
        jnp.broadcast_to(columns[:, 2 * pair : 2 * pair + 1], (rows, LANES)),
        jnp.broadcast_to(columns[:, 2 * pair + 1 : 2 * pair + 2], (rows, LANES)),
    )


def place_docs(dext_ref, prior_ref, docs, blocks):
    dext_ref[0:EDGE] = prior_ref[...].astype(F32)
    padded = jnp.concatenate([docs, jnp.zeros((8 - blocks, BLOCK), F32)]) if blocks < 8 else docs
    columns = transposed(padded)
    for b in range(blocks):
        dext_ref[EDGE + b * BLOCK : EDGE + (b + 1) * BLOCK] = jnp.broadcast_to(
            columns[:, b : b + 1], (BLOCK, LANES)
        )


def short_filter(ext_ref, dext_ref, taps_ref, out_ref, blocks, width):
    taps = taps_ref[...].astype(F32)
    count = taps.shape[0]
    for b in range(blocks):
        first = EDGE + b * BLOCK
        own = dext_ref[first : first + BLOCK]
        masks = [
            dext_ref[first - count + 1 + k : first - count + 1 + k + BLOCK] == own
            for k in range(count - 1)
        ]
        for c in range(width // LANES):
            cols = slice(c * LANES, (c + 1) * LANES)
            total = None
            for k in range(count):
                start = first - count + 1 + k
                term = ext_ref[start : start + BLOCK, cols] * taps[k : k + 1, cols]
                if k < count - 1:
                    term = jnp.where(masks[k], term, 0.0)
                total = term if total is None else total + term
            out_ref[b * BLOCK : (b + 1) * BLOCK, cols] = silu(total).astype(BF16)


def pack_kernel(values_ref, writes_ref, reads_ref, docs_ref, out_ref):
    wide, narrow = values_ref.shape[1], writes_ref.shape[1]
    out_ref[:, 0:wide] = values_ref[...]
    out_ref[:, wide : wide + narrow] = writes_ref[...]
    out_ref[:, wide + narrow : wide + 2 * narrow] = reads_ref[...]
    blocks = docs_ref.shape[0]
    last = jnp.broadcast_to(doc_rows(docs_ref)[blocks - 1 :], (8, BLOCK))
    column = transposed(last)[BLOCK - EDGE :, 0:1]
    out_ref[:, wide + 2 * narrow :] = jnp.broadcast_to(column, (EDGE, LANES)).astype(BF16)


def pack_edge(values, writes, reads, docs):
    tokens, wide = values.shape
    narrow = writes.shape[1]
    at = tokens // EDGE - 1
    return pl.pallas_call(
        pack_kernel,
        grid=(1,),
        in_specs=[
            pl.BlockSpec((EDGE, wide), lambda i: (at, 0)),
            pl.BlockSpec((EDGE, narrow), lambda i: (at, 0)),
            pl.BlockSpec((EDGE, narrow), lambda i: (at, 0)),
            pl.BlockSpec(docs.shape, lambda i: (0, 0)),
        ],
        out_specs=pl.BlockSpec((EDGE, wide + 2 * narrow + LANES), lambda i: (0, 0)),
        out_shape=shape((EDGE, wide + 2 * narrow + LANES), BF16),
        name="pack_edge",
    )(values, writes, reads, docs)


def state_kernel(
    before_ref,
    values_ref,
    writes_ref,
    step_ref,
    rate_ref,
    jump_ref,
    docs_ref,
    taps_values_ref,
    taps_write_ref,
    sv_ref,
    sw_ref,
    run_ref,
    stepped_ref,
    enter_ref,
    send_ref,
    ext_ref,
    wext_ref,
    dext_ref,
):
    tokens, wide = values_ref.shape
    narrow = writes_ref.shape[1]
    blocks = tokens // BLOCK
    heads = step_ref.shape[0]
    docs = doc_rows(docs_ref)
    place_docs(dext_ref, before_ref.at[:, wide + 2 * narrow :], docs, blocks)
    ext_ref[0:EDGE] = before_ref[:, 0:wide].astype(F32)
    ext_ref[EDGE:] = values_ref[...].astype(F32)
    wext_ref[0:EDGE] = before_ref[:, wide : wide + narrow].astype(F32)
    wext_ref[EDGE:] = writes_ref[...].astype(F32)
    short_filter(wext_ref, dext_ref, taps_write_ref, sw_ref, blocks, narrow)
    short_filter(ext_ref, dext_ref, taps_values_ref, sv_ref, blocks, wide)

    raw = step_ref[...].astype(F32)
    step = jnp.maximum(raw, 0.0) + jnp.log1p(jnp.exp(-jnp.abs(raw)))
    stepped_ref[...] = step
    log_decay = jump_ref[...] - rate_ref[...] * step
    held = None
    total = jnp.zeros((heads, 1), F32)
    head_size = wide // heads
    for b in range(blocks):
        span = slice(b * BLOCK, (b + 1) * BLOCK)
        run = running_sum(log_decay[:, span])
        run_ref[:, span] = run
        last = run[:, BLOCK - 1 :]
        total = total + last
        row = docs[b : b + 1]
        end = row[:, BLOCK - 1 :]
        factor = jnp.where(row == end, jnp.exp(last - run) * step[:, span], 0.0)
        columns = transposed(factor)
        scaled = jnp.concatenate(
            [
                (
                    sv_ref[span, p * LANES : (p + 1) * LANES].astype(F32)
                    * per_channel(columns, p, BLOCK)
                ).astype(BF16)
                for p in range(wide // LANES)
            ],
            axis=1,
        )
        fresh = lax.dot_general(
            scaled, sw_ref[span], (((0,), (0,)), ((), ())), preferred_element_type=F32
        )
        if held is None:
            held = fresh
        else:
            enter_ref[b - 1] = held.astype(BF16)
            passing = jnp.where(docs[b - 1 : b, BLOCK - 1 :] == end, jnp.exp(last), 0.0)
            held = jnp.concatenate(
                [
                    held[h * head_size : (h + 1) * head_size] * passing[h : h + 1]
                    + fresh[h * head_size : (h + 1) * head_size]
                    for h in range(heads)
                ]
            )
    send_ref[0:wide] = held.astype(BF16)
    behind = before_ref[EDGE - 1 : EDGE, wide + 2 * narrow :].astype(F32)
    whole = jnp.where(
        behind == docs[blocks - 1 :, BLOCK - 1 :], jnp.broadcast_to(jnp.exp(total), (heads, LANES)), 0.0
    )
    send_ref[wide:] = jnp.concatenate([whole, jnp.zeros((16 - heads, LANES), F32)]).astype(BF16)


def local_states(before, values, writes, step_raw, rate, jump, docs, taps_values, taps_write):
    tokens, wide = values.shape
    narrow = writes.shape[1]
    heads = step_raw.shape[0]
    blocks = tokens // BLOCK
    return pl.pallas_call(
        state_kernel,
        out_shape=(
            shape((tokens, wide), BF16),
            shape((tokens, narrow), BF16),
            shape((heads, tokens), F32),
            shape((heads, tokens), F32),
            shape((blocks - 1, wide, narrow), BF16),
            shape((wide + 16, narrow), BF16),
        ),
        scratch_shapes=[
            pltpu.VMEM((EDGE + tokens, wide), F32),
            pltpu.VMEM((EDGE + tokens, narrow), F32),
            pltpu.VMEM((EDGE + tokens, LANES), F32),
        ],
        cost_estimate=pl.CostEstimate(flops=400_000_000, transcendentals=0, bytes_accessed=4_000_000),
        name="local_states",
    )(before, values, writes, step_raw, rate, jump, docs, taps_values, taps_write)


def decayed(near, decay, far, heads):
    size = near.shape[0] // heads
    return jnp.concatenate(
        [
            near[h * size : (h + 1) * size] + decay[h : h + 1] * far[h * size : (h + 1) * size]
            for h in range(heads)
        ]
    )


def join_kernel(heads, own_ref, near_ref, out_ref):
    wide = out_ref.shape[0]
    own = own_ref[0:wide].astype(F32)
    decay = own_ref[wide:].astype(F32)
    out_ref[...] = decayed(own, decay, near_ref[0:wide].astype(F32), heads).astype(BF16)


def join_states(own, near, heads):
    return pl.pallas_call(
        functools.partial(join_kernel, heads),
        out_shape=shape((own.shape[0] - 16, own.shape[1]), BF16),
        name="join_states",
    )(own, near)


def inner_kernel(
    before_ref,
    reads_ref,
    docs_ref,
    taps_ref,
    sv_ref,
    sw_ref,
    run_ref,
    step_ref,
    enter_ref,
    sr_ref,
    mixed_ref,
    reach_ref,
    ext_ref,
    dext_ref,
):
    tokens, narrow = reads_ref.shape
    wide = sv_ref.shape[1]
    blocks = tokens // BLOCK
    heads = step_ref.shape[0]
    docs = doc_rows(docs_ref)
    place_docs(dext_ref, before_ref.at[:, wide + 2 * narrow :], docs, blocks)
    ext_ref[0:EDGE] = before_ref[:, wide + narrow : wide + 2 * narrow].astype(F32)
    ext_ref[EDGE:] = reads_ref[...].astype(F32)
    short_filter(ext_ref, dext_ref, taps_ref, sr_ref, blocks, narrow)
    target = lax.broadcasted_iota(jnp.int32, (BLOCK, BLOCK), 0)
    source = lax.broadcasted_iota(jnp.int32, (BLOCK, BLOCK), 1)
    low = source < LANES // 2
    gain = None
    for b in range(blocks):
        span = slice(b * BLOCK, (b + 1) * BLOCK)
        row = docs[b : b + 1]
        column = dext_ref[EDGE + b * BLOCK : EDGE + (b + 1) * BLOCK]
        allowed = (target >= source) & (column == row)
        reads, writes = sr_ref[span], sw_ref[span]
        scores = lax.dot_general(
            reads, writes, (((1,), (1,)), ((), ())), preferred_element_type=F32
        )
        run, step = run_ref[:, span], step_ref[:, span]
        run_columns = transposed(run)
        if b == 0:
            prior = before_ref[EDGE - 1 : EDGE, wide + 2 * narrow :].astype(F32)
        else:
            prior = jnp.broadcast_to(docs[b - 1 : b, BLOCK - 1 :], (1, BLOCK))
        reach = jnp.where(row == prior, jnp.exp(run), 0.0)
        last = run[:, BLOCK - 1 :]
        passing = jnp.where(row[:, BLOCK - 1 :] == prior[:, 0:1], jnp.exp(last), 0.0)
        reach_ref[:, span] = reach if gain is None else reach * gain
        gain = passing if gain is None else gain * passing
        reach_columns = transposed(reach)
        if b > 0:
            taken = lax.dot_general(
                reads, enter_ref[b - 1], (((1,), (1,)), ((), ())), preferred_element_type=F32
            )
        for p in range(wide // LANES):
            cols = slice(p * LANES, (p + 1) * LANES)
            weights = []
            for h in (2 * p, 2 * p + 1):
                spread = run_columns[:, h : h + 1] - run[h : h + 1]
                decay = jnp.exp(jnp.where(allowed, spread, -1e30))
                weights.append((decay * scores * step[h : h + 1]).astype(BF16))
            here = sv_ref[span, cols]
            zero = jnp.zeros_like(here)
            both = jnp.concatenate([jnp.where(low, here, zero), jnp.where(low, zero, here)])
            mixed = jnp.dot(
                jnp.concatenate(weights, axis=1), both, preferred_element_type=F32
            )
            if b > 0:
                mixed = mixed + taken[:, cols] * per_channel(reach_columns, p, BLOCK)
            mixed_ref[span, cols] = mixed


def local_mix(before, reads, docs, taps, sv, sw, run, step, enter):
    tokens, narrow = reads.shape
    wide = sv.shape[1]
    heads = step.shape[0]
    return pl.pallas_call(
        inner_kernel,
        out_shape=(
            shape((tokens, narrow), BF16),
            shape((tokens, wide), F32),
            shape((heads, tokens), F32),
        ),
        scratch_shapes=[
            pltpu.VMEM((EDGE + tokens, narrow), F32),
            pltpu.VMEM((EDGE + tokens, LANES), F32),
        ],
        cost_estimate=pl.CostEstimate(flops=800_000_000, transcendentals=0, bytes_accessed=4_000_000),
        name="local_mix",
    )(before, reads, docs, taps, sv, sw, run, step, enter)


def project_kernel(
    core_ref,
    near_ref,
    far_ref,
    sr_ref,
    mixed_ref,
    reach_ref,
    gate_ref,
    gain_ref,
    weight_ref,
    mine_ref,
    other_ref,
    in_ref,
):
    tokens, wide = mixed_ref.shape
    heads = reach_ref.shape[0]
    share = mine_ref.shape[2]
    near = near_ref[0:wide].astype(F32)
    decay = near_ref[wide:].astype(F32)
    held = decayed(near, decay, far_ref[...].astype(F32), heads).astype(BF16)
    for b in range(tokens // BLOCK):
        span = slice(b * BLOCK, (b + 1) * BLOCK)
        taken = lax.dot_general(
            sr_ref[span], held, (((1,), (1,)), ((), ())), preferred_element_type=F32
        )
        columns = transposed(reach_ref[:, span])
        parts, square = [], None
        for p in range(wide // LANES):
            cols = slice(p * LANES, (p + 1) * LANES)
            mixed = mixed_ref[span, cols] + taken[:, cols] * per_channel(columns, p, BLOCK)
            part = mixed * silu(gate_ref[span, cols].astype(F32))
            parts.append(part)
            square = part * part if square is None else square + part * part
        mean = jnp.sum(square, axis=1, keepdims=True) / wide
        scale = lax.rsqrt(mean + norm_eps)
        for p, part in enumerate(parts):
            cols = slice(p * LANES, (p + 1) * LANES)
            in_ref[span, cols] = (part * scale * gain_ref[:, cols].astype(F32)).astype(BF16)
    core = core_ref[0]
    rows = in_ref[...]
    for flip, out_ref in ((1, other_ref), (0, mine_ref)):
        for k in range(out_ref.shape[0]):
            c = 2 * k + (core ^ flip)
            cols = pl.ds(pl.multiple_of(c * share, share), share)
            out_ref[k] = jnp.dot(rows, weight_ref[:, cols], preferred_element_type=F32).astype(BF16)


def vmem():
    return pl.BlockSpec(memory_space=pltpu.VMEM)


def smem():
    return pl.BlockSpec(memory_space=pltpu.SMEM)


def project(core, near, far, sr, mixed, reach, gate, gain, weight, owners):
    tokens, wide = mixed.shape
    share = weight.shape[1] // (2 * owners)
    return pl.pallas_call(
        project_kernel,
        in_specs=[smem()] + [vmem()] * 8,
        out_shape=(shape((owners, tokens, share), BF16),) * 2,
        scratch_shapes=[pltpu.VMEM((tokens, wide), BF16)],
        cost_estimate=pl.CostEstimate(
            flops=2 * tokens * wide * weight.shape[1], transcendentals=0, bytes_accessed=6_000_000
        ),
        name="project",
    )(core, near, far, sr, mixed, reach, gate, gain, weight)


def after_kernel(at_ref, parts_ref, residual_ref, own_ref, out_ref):
    total = residual_ref[...].astype(F32)
    for k in range(parts_ref.shape[0]):
        total = total + parts_ref[k].astype(F32)
    after = total.astype(BF16)
    own_ref[...] = after
    for k in range(out_ref.shape[0]):
        out_ref[k] = after


def after_mix(at, parts, residual):
    owners, tokens, share = parts.shape
    return pl.pallas_call(
        after_kernel,
        grid_spec=pltpu.PrefetchScalarGridSpec(
            num_scalar_prefetch=1,
            grid=(1,),
            in_specs=[
                pl.BlockSpec((owners, tokens, share), lambda i, at: (0, 0, 0)),
                pl.BlockSpec((tokens, share), lambda i, at: (0, at[0])),
            ],
            out_specs=[
                pl.BlockSpec((tokens, share), lambda i, at: (0, 0)),
                pl.BlockSpec((owners, tokens, share), lambda i, at: (0, 0, 0)),
            ],
        ),
        out_shape=(shape((tokens, share), BF16), shape((owners, tokens, share), BF16)),
        name="after_mix",
    )(at, parts, residual)


def mixer_kernel(at_ref, mine_ref, other_ref, gain_ref, weight_ref, *refs):
    out_refs = refs[:2]
    after, normal, late, downs, hidden_ref, out, after_sem, late_sem, down_sem, out_sem = refs[2:]
    _, owners, tokens, share = after.shape
    peers, _, depth = weight_ref.shape
    units = hidden_ref.shape[1]
    core = at_ref[0]

    loads = [
        pltpu.make_async_copy(ref, after.at[k], after_sem.at[k])
        for k, ref in enumerate((mine_ref, other_ref))
    ]
    heavy, rows = [], []
    for k in range(peers):
        cols = pl.ds(k * depth, depth)
        heavy.append(
            pltpu.make_async_copy(
                weight_ref.at[k, pl.ds(0, 2 * units)], late.at[:, cols], late_sem.at[k]
            )
        )
        rows.append(
            pltpu.make_async_copy(
                weight_ref.at[k, pl.ds(2 * units, units)], downs.at[:, cols], down_sem.at[k]
            )
        )
    for copy in (*loads, *heavy, *rows):
        copy.start()

    for copy in loads:
        copy.wait()
    square = None
    for flip in range(2):
        for k in range(owners):
            x = after[flip, k].astype(F32)
            square = x * x if square is None else square + x * x
    scale = lax.rsqrt(jnp.sum(square, axis=1, keepdims=True) / (2 * owners * share) + norm_eps)
    for flip in range(2):
        for k in range(owners):
            c = 2 * k + (core ^ flip)
            normal[:, pl.ds(pl.multiple_of(c * share, share), share)] = (
                after[flip, k].astype(F32) * scale * gain_ref[c].astype(F32)
            ).astype(BF16)
    for copy in heavy:
        copy.wait()
    across = (((1,), (1,)), ((), ()))
    gate = lax.dot_general(normal[...], late[0:units], across, preferred_element_type=F32)
    up = lax.dot_general(normal[...], late[units:], across, preferred_element_type=F32)
    hidden_ref[...] = (silu(gate) * up).astype(BF16)
    for copy in rows:
        copy.wait()
    stores = []
    for flip in (1, 0):
        for k in range(owners):
            c = 2 * k + (core ^ flip)
            part = downs[:, pl.ds(pl.multiple_of(c * share, share), share)]
            out[flip, k] = jnp.dot(hidden_ref[...], part, preferred_element_type=F32).astype(BF16)
        store = pltpu.make_async_copy(out.at[flip], out_refs[flip], out_sem.at[flip])
        store.start()
        stores.append(store)
    for store in stores:
        store.wait()


def channel_mixer(core, mine, other, gain, weights):
    owners, tokens, share = mine.shape
    peers, units, depth = weights.shape[0], weights.shape[1] // 3, weights.shape[2]
    anywhere = pl.BlockSpec(memory_space=pl.ANY)
    out = shape((owners, tokens, share), BF16)
    return pl.pallas_call(
        mixer_kernel,
        in_specs=[smem(), anywhere, anywhere, vmem(), anywhere],
        out_specs=[anywhere, anywhere],
        out_shape=(out, out),
        scratch_shapes=[
            pltpu.VMEM((2, owners, tokens, share), BF16),
            pltpu.VMEM((tokens, peers * depth), BF16),
            pltpu.VMEM((2 * units, peers * depth), BF16),
            pltpu.VMEM((units, peers * depth), BF16),
            pltpu.VMEM((tokens, units), BF16),
            pltpu.VMEM((2, owners, tokens, share), BF16),
            pltpu.SemaphoreType.DMA((2,)),
            pltpu.SemaphoreType.DMA((peers,)),
            pltpu.SemaphoreType.DMA((peers,)),
            pltpu.SemaphoreType.DMA((2,)),
        ],
        cost_estimate=pl.CostEstimate(
            flops=12 * tokens * owners * share * units, transcendentals=0, bytes_accessed=14_000_000
        ),
        name="channel_mixer",
    )(core, mine, other, gain, weights)


def out_kernel(parts_ref, own_ref, out_ref):
    total = None
    for k in range(parts_ref.shape[0]):
        part = parts_ref[k].astype(F32)
        total = part if total is None else total + part
    out_ref[...] = (own_ref[...].astype(F32) + total).astype(BF16)


def add_down(parts, own):
    return pl.pallas_call(out_kernel, out_shape=shape(own.shape, BF16), name="add_down")(parts, own)


def to_partner(value):
    return lax.ppermute(value, "tp", [(i, i ^ 1) for i in range(lax.axis_size("tp"))])


def exchange(value):
    peers = lax.axis_size("tp")
    rows = [[i for i in range(peers) if i % 2 == core] for core in range(2)]
    return lax.all_to_all(value, "tp", 0, 0, axis_index_groups=rows, tiled=True)


def sum_pairs(both):
    return (both[0].astype(F32) + to_partner(both[1]).astype(F32)).astype(BF16)


def on_device(
    residual,
    values,
    out_gate,
    writes,
    reads,
    step_raw,
    decay_rate,
    decay_jump,
    documents,
    taps_values,
    taps_write,
    taps_read,
    mixer_gain,
    mixer_out,
    channel_gain,
    gate_weight,
    up_weight,
    down_rows,
):
    heads = step_raw.shape[0]
    owners = lax.axis_size("tp") // 2
    me = lax.axis_index("tp").astype(jnp.int32)
    at = me.reshape(1)
    core = (me % 2).reshape(1)
    late = jnp.concatenate([gate_weight.T, up_weight.T, down_rows.T], axis=0)
    weights = lax.all_gather(late, "sp", axis=0)

    docs = documents.reshape(-1, BLOCK)
    before = from_behind(pack_edge(values, writes, reads, docs), "sp", 1)
    rate = decay_rate.reshape(-1, 1)
    sv, sw, run, step, enter, send = local_states(
        before, values, writes, step_raw, rate, decay_jump, docs, taps_values, taps_write
    )
    near = from_behind(send, "sp", 1)
    sr, mixed, reach = local_mix(before, reads, docs, taps_read, sv, sw, run, step, enter)
    far = from_behind(join_states(send, near, heads), "sp", 2)
    both = project(
        core, near, far, sr, mixed, reach, out_gate, mixer_gain.reshape(1, -1), mixer_out, owners
    )
    own_after, spread = after_mix(at, exchange(sum_pairs(both)), residual)
    mine = exchange(spread)
    other = to_partner(mine)
    gain = channel_gain.reshape(2 * owners, 1, -1)
    both = channel_mixer(core, mine, other, gain, weights)
    return add_down(exchange(sum_pairs(both)), own_after)


def solution(mesh):
    return jax.shard_map(
        on_device,
        mesh=mesh,
        in_specs=(
            P(("grp", "sp"), None),
            P(("grp", "sp"), "tp"),
            P(("grp", "sp"), "tp"),
            P(("grp", "sp"), "tp"),
            P(("grp", "sp"), "tp"),
            P("tp", ("grp", "sp")),
            P("tp"),
            P("tp", ("grp", "sp")),
            P(("grp", "sp")),
            P(None, "tp"),
            P(None, "tp"),
            P(None, "tp"),
            P("tp"),
            P("tp", None),
            P(),
            P("sp", "tp"),
            P("sp", "tp"),
            P("sp", "tp"),
        ),
        out_specs=P(("grp", "sp"), "tp"),
        check_vma=False,
    )
```

```python
import functools

import jax
import jax.numpy as jnp
from jax import lax
from jax.experimental import pallas as pl
from jax.experimental.pallas import tpu as pltpu
from jax.sharding import PartitionSpec as P


BLOCK = 128
EDGE = 16
LANES = 128

norm_eps = 1e-06

F32 = jnp.float32
BF16 = jnp.bfloat16


def from_behind(value, axis, by):
    peers = lax.axis_size(axis)
    pairs = [(i, i + by) for i in range(peers) if 0 <= i + by < peers]
    return lax.ppermute(value, axis, pairs)


def silu(x):
    return x * jax.nn.sigmoid(x)


def shape(dims, kind):
    return jax.ShapeDtypeStruct(dims, kind)


def transposed(rows):
    return jnp.transpose(rows, (1, 0))


def doc_rows(docs_ref):
    return docs_ref[...].astype(F32)


def running_sum(x):
    lane = lax.broadcasted_iota(jnp.int32, x.shape, 1)
    shift = 1
    while shift < x.shape[1]:
        x = x + jnp.where(lane >= shift, pltpu.roll(x, shift, 1), 0.0)
        shift *= 2
    return x


def per_channel(columns, pair, rows):
    lane = lax.broadcasted_iota(jnp.int32, (rows, LANES), 1)
    return jnp.where(
        lane < LANES // 2,
        jnp.broadcast_to(columns[:, 2 * pair : 2 * pair + 1], (rows, LANES)),
        jnp.broadcast_to(columns[:, 2 * pair + 1 : 2 * pair + 2], (rows, LANES)),
    )


def place_docs(dext_ref, prior_ref, docs, blocks):
    dext_ref[0:EDGE] = prior_ref[...].astype(F32)
    padded = jnp.concatenate([docs, jnp.zeros((8 - blocks, BLOCK), F32)]) if blocks < 8 else docs
    columns = transposed(padded)
    for b in range(blocks):
        dext_ref[EDGE + b * BLOCK : EDGE + (b + 1) * BLOCK] = jnp.broadcast_to(
            columns[:, b : b + 1], (BLOCK, LANES)
        )


def short_filter(ext_ref, dext_ref, taps_ref, out_ref, blocks, width):
    taps = taps_ref[...].astype(F32)
    count = taps.shape[0]
    for b in range(blocks):
        first = EDGE + b * BLOCK
        own = dext_ref[first : first + BLOCK]
        masks = [
            dext_ref[first - count + 1 + k : first - count + 1 + k + BLOCK] == own
            for k in range(count - 1)
        ]
        for c in range(width // LANES):
            cols = slice(c * LANES, (c + 1) * LANES)
            total = None
            for k in range(count):
                start = first - count + 1 + k
                term = ext_ref[start : start + BLOCK, cols] * taps[k : k + 1, cols]
                if k < count - 1:
                    term = jnp.where(masks[k], term, 0.0)
                total = term if total is None else total + term
            out_ref[b * BLOCK : (b + 1) * BLOCK, cols] = silu(total).astype(BF16)


def pack_kernel(values_ref, writes_ref, reads_ref, docs_ref, out_ref):
    wide, narrow = values_ref.shape[1], writes_ref.shape[1]
    out_ref[:, 0:wide] = values_ref[...]
    out_ref[:, wide : wide + narrow] = writes_ref[...]
    out_ref[:, wide + narrow : wide + 2 * narrow] = reads_ref[...]
    blocks = docs_ref.shape[0]
    last = jnp.broadcast_to(doc_rows(docs_ref)[blocks - 1 :], (8, BLOCK))
    column = transposed(last)[BLOCK - EDGE :, 0:1]
    out_ref[:, wide + 2 * narrow :] = jnp.broadcast_to(column, (EDGE, LANES)).astype(BF16)


def pack_edge(values, writes, reads, docs):
    tokens, wide = values.shape
    narrow = writes.shape[1]
    at = tokens // EDGE - 1
    return pl.pallas_call(
        pack_kernel,
        grid=(1,),
        in_specs=[
            pl.BlockSpec((EDGE, wide), lambda i: (at, 0)),
            pl.BlockSpec((EDGE, narrow), lambda i: (at, 0)),
            pl.BlockSpec((EDGE, narrow), lambda i: (at, 0)),
            pl.BlockSpec(docs.shape, lambda i: (0, 0)),
        ],
        out_specs=pl.BlockSpec((EDGE, wide + 2 * narrow + LANES), lambda i: (0, 0)),
        out_shape=shape((EDGE, wide + 2 * narrow + LANES), BF16),
        name="pack_edge",
    )(values, writes, reads, docs)


def state_kernel(
    before_ref,
    values_ref,
    writes_ref,
    step_ref,
    rate_ref,
    jump_ref,
    docs_ref,
    taps_values_ref,
    taps_write_ref,
    sv_ref,
    sw_ref,
    run_ref,
    stepped_ref,
    enter_ref,
    send_ref,
    ext_ref,
    wext_ref,
    dext_ref,
):
    tokens, wide = values_ref.shape
    narrow = writes_ref.shape[1]
    blocks = tokens // BLOCK
    heads = step_ref.shape[0]
    docs = doc_rows(docs_ref)
    place_docs(dext_ref, before_ref.at[:, wide + 2 * narrow :], docs, blocks)
    ext_ref[0:EDGE] = before_ref[:, 0:wide].astype(F32)
    ext_ref[EDGE:] = values_ref[...].astype(F32)
    wext_ref[0:EDGE] = before_ref[:, wide : wide + narrow].astype(F32)
    wext_ref[EDGE:] = writes_ref[...].astype(F32)
    short_filter(wext_ref, dext_ref, taps_write_ref, sw_ref, blocks, narrow)
    short_filter(ext_ref, dext_ref, taps_values_ref, sv_ref, blocks, wide)

    raw = step_ref[...].astype(F32)
    step = jnp.maximum(raw, 0.0) + jnp.log1p(jnp.exp(-jnp.abs(raw)))
    stepped_ref[...] = step
    log_decay = jump_ref[...] - rate_ref[...] * step
    held = None
    total = jnp.zeros((heads, 1), F32)
    head_size = wide // heads
    for b in range(blocks):
        span = slice(b * BLOCK, (b + 1) * BLOCK)
        run = running_sum(log_decay[:, span])
        run_ref[:, span] = run
        last = run[:, BLOCK - 1 :]
        total = total + last
        row = docs[b : b + 1]
        end = row[:, BLOCK - 1 :]
        factor = jnp.where(row == end, jnp.exp(last - run) * step[:, span], 0.0)
        columns = transposed(factor)
        scaled = jnp.concatenate(
            [
                (
                    sv_ref[span, p * LANES : (p + 1) * LANES].astype(F32)
                    * per_channel(columns, p, BLOCK)
                ).astype(BF16)
                for p in range(wide // LANES)
            ],
            axis=1,
        )
        fresh = lax.dot_general(
            scaled, sw_ref[span], (((0,), (0,)), ((), ())), preferred_element_type=F32
        )
        if held is None:
            held = fresh
        else:
            enter_ref[b - 1] = held.astype(BF16)
            passing = jnp.where(docs[b - 1 : b, BLOCK - 1 :] == end, jnp.exp(last), 0.0)
            held = jnp.concatenate(
                [
                    held[h * head_size : (h + 1) * head_size] * passing[h : h + 1]
                    + fresh[h * head_size : (h + 1) * head_size]
                    for h in range(heads)
                ]
            )
    send_ref[0:wide] = held.astype(BF16)
    behind = before_ref[EDGE - 1 : EDGE, wide + 2 * narrow :].astype(F32)
    whole = jnp.where(
        behind == docs[blocks - 1 :, BLOCK - 1 :], jnp.broadcast_to(jnp.exp(total), (heads, LANES)), 0.0
    )
    send_ref[wide:] = jnp.concatenate([whole, jnp.zeros((16 - heads, LANES), F32)]).astype(BF16)


def local_states(before, values, writes, step_raw, rate, jump, docs, taps_values, taps_write):
    tokens, wide = values.shape
    narrow = writes.shape[1]
    heads = step_raw.shape[0]
    blocks = tokens // BLOCK
    return pl.pallas_call(
        state_kernel,
        out_shape=(
            shape((tokens, wide), BF16),
            shape((tokens, narrow), BF16),
            shape((heads, tokens), F32),
            shape((heads, tokens), F32),
            shape((blocks - 1, wide, narrow), BF16),
            shape((wide + 16, narrow), BF16),
        ),
        scratch_shapes=[
            pltpu.VMEM((EDGE + tokens, wide), F32),
            pltpu.VMEM((EDGE + tokens, narrow), F32),
            pltpu.VMEM((EDGE + tokens, LANES), F32),
        ],
        cost_estimate=pl.CostEstimate(flops=400_000_000, transcendentals=0, bytes_accessed=4_000_000),
        name="local_states",
    )(before, values, writes, step_raw, rate, jump, docs, taps_values, taps_write)


def decayed(near, decay, far, heads):
    size = near.shape[0] // heads
    return jnp.concatenate(
        [
            near[h * size : (h + 1) * size] + decay[h : h + 1] * far[h * size : (h + 1) * size]
            for h in range(heads)
        ]
    )


def join_kernel(heads, own_ref, near_ref, out_ref):
    wide = out_ref.shape[0]
    own = own_ref[0:wide].astype(F32)
    decay = own_ref[wide:].astype(F32)
    out_ref[...] = decayed(own, decay, near_ref[0:wide].astype(F32), heads).astype(BF16)


def join_states(own, near, heads):
    return pl.pallas_call(
        functools.partial(join_kernel, heads),
        out_shape=shape((own.shape[0] - 16, own.shape[1]), BF16),
        name="join_states",
    )(own, near)


def inner_kernel(
    before_ref,
    reads_ref,
    docs_ref,
    taps_ref,
    sv_ref,
    sw_ref,
    run_ref,
    step_ref,
    enter_ref,
    sr_ref,
    mixed_ref,
    reach_ref,
    ext_ref,
    dext_ref,
):
    tokens, narrow = reads_ref.shape
    wide = sv_ref.shape[1]
    blocks = tokens // BLOCK
    docs = doc_rows(docs_ref)
    place_docs(dext_ref, before_ref.at[:, wide + 2 * narrow :], docs, blocks)
    ext_ref[0:EDGE] = before_ref[:, wide + narrow : wide + 2 * narrow].astype(F32)
    ext_ref[EDGE:] = reads_ref[...].astype(F32)
    short_filter(ext_ref, dext_ref, taps_ref, sr_ref, blocks, narrow)
    target = lax.broadcasted_iota(jnp.int32, (BLOCK, BLOCK), 0)
    source = lax.broadcasted_iota(jnp.int32, (BLOCK, BLOCK), 1)
    low = source < LANES // 2
    gain = None
    for b in range(blocks):
        span = slice(b * BLOCK, (b + 1) * BLOCK)
        row = docs[b : b + 1]
        column = dext_ref[EDGE + b * BLOCK : EDGE + (b + 1) * BLOCK]
        allowed = (target >= source) & (column == row)
        reads, writes = sr_ref[span], sw_ref[span]
        scores = lax.dot_general(
            reads, writes, (((1,), (1,)), ((), ())), preferred_element_type=F32
        )
        run, step = run_ref[:, span], step_ref[:, span]
        run_columns = transposed(run)
        if b == 0:
            prior = before_ref[EDGE - 1 : EDGE, wide + 2 * narrow :].astype(F32)
        else:
            prior = jnp.broadcast_to(docs[b - 1 : b, BLOCK - 1 :], (1, BLOCK))
        reach = jnp.where(row == prior, jnp.exp(run), 0.0)
        last = run[:, BLOCK - 1 :]
        passing = jnp.where(row[:, BLOCK - 1 :] == prior[:, 0:1], jnp.exp(last), 0.0)
        reach_ref[:, span] = reach if gain is None else reach * gain
        gain = passing if gain is None else gain * passing
        reach_columns = transposed(reach)
        if b > 0:
            taken = lax.dot_general(
                reads, enter_ref[b - 1], (((1,), (1,)), ((), ())), preferred_element_type=F32
            )
        for p in range(wide // LANES):
            cols = slice(p * LANES, (p + 1) * LANES)
            weights = []
            for h in (2 * p, 2 * p + 1):
                spread = run_columns[:, h : h + 1] - run[h : h + 1]
                decay = jnp.exp(jnp.where(allowed, spread, -1e30))
                weights.append((decay * scores * step[h : h + 1]).astype(BF16))
            here = sv_ref[span, cols]
            zero = jnp.zeros_like(here)
            both = jnp.concatenate([jnp.where(low, here, zero), jnp.where(low, zero, here)])
            mixed = jnp.dot(
                jnp.concatenate(weights, axis=1), both, preferred_element_type=F32
            )
            if b > 0:
                mixed = mixed + taken[:, cols] * per_channel(reach_columns, p, BLOCK)
            mixed_ref[span, cols] = mixed


def local_mix(before, reads, docs, taps, sv, sw, run, step, enter):
    tokens, narrow = reads.shape
    wide = sv.shape[1]
    heads = step.shape[0]
    return pl.pallas_call(
        inner_kernel,
        out_shape=(
            shape((tokens, narrow), BF16),
            shape((tokens, wide), F32),
            shape((heads, tokens), F32),
        ),
        scratch_shapes=[
            pltpu.VMEM((EDGE + tokens, narrow), F32),
            pltpu.VMEM((EDGE + tokens, LANES), F32),
        ],
        cost_estimate=pl.CostEstimate(flops=800_000_000, transcendentals=0, bytes_accessed=4_000_000),
        name="local_mix",
    )(before, reads, docs, taps, sv, sw, run, step, enter)


def project_kernel(
    core_ref,
    near_ref,
    far_ref,
    sr_ref,
    mixed_ref,
    reach_ref,
    gate_ref,
    gain_ref,
    weight_ref,
    mine_ref,
    other_ref,
    in_ref,
):
    tokens, wide = mixed_ref.shape
    heads = reach_ref.shape[0]
    share = mine_ref.shape[2]
    near = near_ref[0:wide].astype(F32)
    decay = near_ref[wide:].astype(F32)
    held = decayed(near, decay, far_ref[...].astype(F32), heads).astype(BF16)
    for b in range(tokens // BLOCK):
        span = slice(b * BLOCK, (b + 1) * BLOCK)
        taken = lax.dot_general(
            sr_ref[span], held, (((1,), (1,)), ((), ())), preferred_element_type=F32
        )
        columns = transposed(reach_ref[:, span])
        parts, square = [], None
        for p in range(wide // LANES):
            cols = slice(p * LANES, (p + 1) * LANES)
            mixed = mixed_ref[span, cols] + taken[:, cols] * per_channel(columns, p, BLOCK)
            part = mixed * silu(gate_ref[span, cols].astype(F32))
            parts.append(part)
            square = part * part if square is None else square + part * part
        mean = jnp.sum(square, axis=1, keepdims=True) / wide
        scale = lax.rsqrt(mean + norm_eps)
        for p, part in enumerate(parts):
            cols = slice(p * LANES, (p + 1) * LANES)
            in_ref[span, cols] = (part * scale * gain_ref[:, cols].astype(F32)).astype(BF16)
    core = core_ref[0]
    rows = in_ref[...]
    for flip, out_ref in ((1, other_ref), (0, mine_ref)):
        for k in range(out_ref.shape[0]):
            c = 2 * k + (core ^ flip)
            cols = pl.ds(pl.multiple_of(c * share, share), share)
            out_ref[k] = jnp.dot(rows, weight_ref[:, cols], preferred_element_type=F32).astype(BF16)


def vmem():
    return pl.BlockSpec(memory_space=pltpu.VMEM)


def smem():
    return pl.BlockSpec(memory_space=pltpu.SMEM)


def project(core, near, far, sr, mixed, reach, gate, gain, weight, owners):
    tokens, wide = mixed.shape
    share = weight.shape[1] // (2 * owners)
    return pl.pallas_call(
        project_kernel,
        in_specs=[smem()] + [vmem()] * 8,
        out_shape=(shape((owners, tokens, share), BF16),) * 2,
        scratch_shapes=[pltpu.VMEM((tokens, wide), BF16)],
        cost_estimate=pl.CostEstimate(
            flops=2 * tokens * wide * weight.shape[1], transcendentals=0, bytes_accessed=6_000_000
        ),
        name="project",
    )(core, near, far, sr, mixed, reach, gate, gain, weight)


def after_kernel(at_ref, parts_ref, residual_ref, own_ref, out_ref):
    total = residual_ref[...].astype(F32)
    for k in range(parts_ref.shape[0]):
        total = total + parts_ref[k].astype(F32)
    after = total.astype(BF16)
    own_ref[...] = after
    for k in range(out_ref.shape[0]):
        out_ref[k] = after


def after_mix(at, parts, residual):
    owners, tokens, share = parts.shape
    return pl.pallas_call(
        after_kernel,
        grid_spec=pltpu.PrefetchScalarGridSpec(
            num_scalar_prefetch=1,
            grid=(1,),
            in_specs=[
                pl.BlockSpec((owners, tokens, share), lambda i, at: (0, 0, 0)),
                pl.BlockSpec((tokens, share), lambda i, at: (0, at[0])),
            ],
            out_specs=[
                pl.BlockSpec((tokens, share), lambda i, at: (0, 0)),
                pl.BlockSpec((owners, tokens, share), lambda i, at: (0, 0, 0)),
            ],
        ),
        out_shape=(shape((tokens, share), BF16), shape((owners, tokens, share), BF16)),
        name="after_mix",
    )(at, parts, residual)


def mixer_kernel(peers, at_ref, mine_ref, other_ref, gain_ref, weight_ref, *refs):
    down_refs = refs[:peers]
    out_refs = refs[peers : peers + 2]
    after, normal, late, downs, hidden_ref, out, after_sem, late_sem, down_sem, out_sem = refs[
        peers + 2 :
    ]
    _, owners, _, share = after.shape
    _, units, _ = downs.shape
    core, place = at_ref[0], at_ref[1]

    loads = [
        pltpu.make_async_copy(ref, after.at[k], after_sem.at[k])
        for k, ref in enumerate((mine_ref, other_ref))
    ]
    heavy = pltpu.make_async_copy(weight_ref, late, late_sem)
    rows = []
    for k, ref in enumerate(down_refs):
        index = lax.rem(place - k + peers, peers)
        rows.append(pltpu.make_async_copy(ref, downs.at[index], down_sem.at[k]))
    for copy in (*loads, heavy):
        copy.start()

    for copy in loads:
        copy.wait()
    square = None
    for flip in range(2):
        for k in range(owners):
            x = after[flip, k].astype(F32)
            square = x * x if square is None else square + x * x
    scale = lax.rsqrt(jnp.sum(square, axis=1, keepdims=True) / (2 * owners * share) + norm_eps)
    for flip in range(2):
        for k in range(owners):
            c = 2 * k + (core ^ flip)
            normal[:, pl.ds(pl.multiple_of(c * share, share), share)] = (
                after[flip, k].astype(F32) * scale * gain_ref[c].astype(F32)
            ).astype(BF16)
    heavy.wait()
    for copy in rows:
        copy.start()
    across = (((1,), (1,)), ((), ()))
    gates = jnp.concatenate([late[k, 0:units] for k in range(peers)], axis=1)
    gate = lax.dot_general(normal[...], gates, across, preferred_element_type=F32)
    ups = jnp.concatenate([late[k, units:] for k in range(peers)], axis=1)
    up = lax.dot_general(normal[...], ups, across, preferred_element_type=F32)
    hidden_ref[...] = (silu(gate) * up).astype(BF16)
    for copy in rows:
        copy.wait()
    stores = []
    for flip in (1, 0):
        for k in range(owners):
            c = 2 * k + (core ^ flip)
            part = jnp.concatenate([downs[2 * c], downs[2 * c + 1]], axis=1)
            out[flip, k] = jnp.dot(hidden_ref[...], part, preferred_element_type=F32).astype(BF16)
            store = pltpu.make_async_copy(
                out.at[flip, k], out_refs[flip].at[k], out_sem.at[flip, k]
            )
            store.start()
            stores.append(store)
    for store in stores:
        store.wait()


def channel_mixer(at, mine, other, gain, weights, downs):
    owners, tokens, share = mine.shape
    peers, units, depth = len(downs), *downs[0].shape
    anywhere = pl.BlockSpec(memory_space=pl.ANY)
    out = shape((owners, tokens, share), BF16)
    return pl.pallas_call(
        functools.partial(mixer_kernel, peers),
        in_specs=[smem(), anywhere, anywhere, vmem(), anywhere] + [anywhere] * peers,
        out_specs=[anywhere, anywhere],
        out_shape=(out, out),
        scratch_shapes=[
            pltpu.VMEM((2, owners, tokens, share), BF16),
            pltpu.VMEM((tokens, peers * depth), BF16),
            pltpu.VMEM((peers, 2 * units, depth), BF16),
            pltpu.VMEM((peers, units, depth), BF16),
            pltpu.VMEM((tokens, units), BF16),
            pltpu.VMEM((2, owners, tokens, share), BF16),
            pltpu.SemaphoreType.DMA((2,)),
            pltpu.SemaphoreType.DMA,
            pltpu.SemaphoreType.DMA((peers,)),
            pltpu.SemaphoreType.DMA((2, owners)),
        ],
        cost_estimate=pl.CostEstimate(
            flops=12 * tokens * owners * share * units, transcendentals=0, bytes_accessed=14_000_000
        ),
        name="channel_mixer",
    )(at, mine, other, gain, weights, *downs)


def ring_of(value, axis):
    peers = lax.axis_size(axis)
    found = {0: value}
    up = down = value
    for k in range(1, peers // 2 + 1):
        up = lax.ppermute(up, axis, [(i, (i + 1) % peers) for i in range(peers)])
        found[k] = up
        if k < peers - k:
            down = lax.ppermute(down, axis, [(i, (i - 1) % peers) for i in range(peers)])
            found[peers - k] = down
    return [found[k] for k in range(peers)]


def out_kernel(parts_ref, own_ref, out_ref):
    total = None
    for k in range(parts_ref.shape[0]):
        part = parts_ref[k].astype(F32)
        total = part if total is None else total + part
    out_ref[...] = (own_ref[...].astype(F32) + total).astype(BF16)


def add_down(parts, own):
    return pl.pallas_call(out_kernel, out_shape=shape(own.shape, BF16), name="add_down")(parts, own)


def to_partner(value):
    return lax.ppermute(value, "tp", [(i, i ^ 1) for i in range(lax.axis_size("tp"))])


def exchange(value):
    peers = lax.axis_size("tp")
    rows = [[i for i in range(peers) if i % 2 == core] for core in range(2)]
    return lax.all_to_all(value, "tp", 0, 0, axis_index_groups=rows, tiled=True)


def sum_pairs(both):
    return (both[0].astype(F32) + to_partner(both[1]).astype(F32)).astype(BF16)


def on_device(
    residual,
    values,
    out_gate,
    writes,
    reads,
    step_raw,
    decay_rate,
    decay_jump,
    documents,
    taps_values,
    taps_write,
    taps_read,
    mixer_gain,
    mixer_out,
    channel_gain,
    gate_weight,
    up_weight,
    down_rows,
):
    heads = step_raw.shape[0]
    owners = lax.axis_size("tp") // 2
    me = lax.axis_index("tp").astype(jnp.int32)
    at = me.reshape(1)
    core = (me % 2).reshape(1)
    place = jnp.stack([me % 2, lax.axis_index("sp").astype(jnp.int32)])
    late = jnp.concatenate([gate_weight.T, up_weight.T], axis=0)
    weights = lax.all_gather(late, "sp", axis=0)
    downs = ring_of(down_rows.T, "sp")

    docs = documents.reshape(-1, BLOCK)
    before = from_behind(pack_edge(values, writes, reads, docs), "sp", 1)
    rate = decay_rate.reshape(-1, 1)
    sv, sw, run, step, enter, send = local_states(
        before, values, writes, step_raw, rate, decay_jump, docs, taps_values, taps_write
    )
    near = from_behind(send, "sp", 1)
    sr, mixed, reach = local_mix(before, reads, docs, taps_read, sv, sw, run, step, enter)
    joined = join_states(send, near, heads)
    far = from_behind(joined, "sp", 2)
    gain = mixer_gain.reshape(1, -1)
    both = project(core, near, far, sr, mixed, reach, out_gate, gain, mixer_out, owners)
    parts = sum_pairs(both)
    parts = exchange(parts)
    own_after, spread = after_mix(at, parts, residual)
    mine = exchange(spread)
    other = to_partner(mine)
    gain = channel_gain.reshape(2 * owners, 1, -1)
    both = channel_mixer(place, mine, other, gain, weights, downs)
    parts = sum_pairs(both)
    parts = exchange(parts)
    return add_down(parts, own_after)


def solution(mesh):
    return jax.shard_map(
        on_device,
        mesh=mesh,
        in_specs=(
            P(("grp", "sp"), None),
            P(("grp", "sp"), "tp"),
            P(("grp", "sp"), "tp"),
            P(("grp", "sp"), "tp"),
            P(("grp", "sp"), "tp"),
            P("tp", ("grp", "sp")),
            P("tp"),
            P("tp", ("grp", "sp")),
            P(("grp", "sp")),
            P(None, "tp"),
            P(None, "tp"),
            P(None, "tp"),
            P("tp"),
            P("tp", None),
            P(),
            P("sp", "tp"),
            P("sp", "tp"),
            P("sp", "tp"),
        ),
        out_specs=P(("grp", "sp"), "tp"),
        check_vma=False,
    )
```

```python
import functools

import jax
import jax.numpy as jnp
from jax import lax
from jax.experimental import pallas as pl
from jax.experimental.pallas import tpu as pltpu
from jax.sharding import PartitionSpec as P


BLOCK = 128
EDGE = 16
LANES = 128

norm_eps = 1e-06

F32 = jnp.float32
BF16 = jnp.bfloat16


def from_behind(value, axis, by):
    peers = lax.axis_size(axis)
    pairs = [(i, i + by) for i in range(peers) if 0 <= i + by < peers]
    return lax.ppermute(value, axis, pairs)


def silu(x):
    return x * jax.nn.sigmoid(x)


def shape(dims, kind):
    return jax.ShapeDtypeStruct(dims, kind)


def transposed(rows):
    return jnp.transpose(rows, (1, 0))


def doc_rows(docs_ref):
    return docs_ref[...].astype(F32)


def running_sum(x):
    lane = lax.broadcasted_iota(jnp.int32, x.shape, 1)
    shift = 1
    while shift < x.shape[1]:
        x = x + jnp.where(lane >= shift, pltpu.roll(x, shift, 1), 0.0)
        shift *= 2
    return x


def per_channel(columns, pair, rows):
    lane = lax.broadcasted_iota(jnp.int32, (rows, LANES), 1)
    return jnp.where(
        lane < LANES // 2,
        jnp.broadcast_to(columns[:, 2 * pair : 2 * pair + 1], (rows, LANES)),
        jnp.broadcast_to(columns[:, 2 * pair + 1 : 2 * pair + 2], (rows, LANES)),
    )


def place_docs(dext_ref, prior_ref, docs, blocks):
    dext_ref[0:EDGE] = prior_ref[...].astype(F32)
    padded = jnp.concatenate([docs, jnp.zeros((8 - blocks, BLOCK), F32)]) if blocks < 8 else docs
    columns = transposed(padded)
    for b in range(blocks):
        dext_ref[EDGE + b * BLOCK : EDGE + (b + 1) * BLOCK] = jnp.broadcast_to(
            columns[:, b : b + 1], (BLOCK, LANES)
        )


def short_filter(ext_ref, dext_ref, taps_ref, out_ref, blocks, width):
    taps = taps_ref[...].astype(F32)
    count = taps.shape[0]
    for b in range(blocks):
        first = EDGE + b * BLOCK
        own = dext_ref[first : first + BLOCK]
        masks = [
            dext_ref[first - count + 1 + k : first - count + 1 + k + BLOCK] == own
            for k in range(count - 1)
        ]
        for c in range(width // LANES):
            cols = slice(c * LANES, (c + 1) * LANES)
            total = None
            for k in range(count):
                start = first - count + 1 + k
                term = ext_ref[start : start + BLOCK, cols] * taps[k : k + 1, cols]
                if k < count - 1:
                    term = jnp.where(masks[k], term, 0.0)
                total = term if total is None else total + term
            out_ref[b * BLOCK : (b + 1) * BLOCK, cols] = silu(total).astype(BF16)


def pack_kernel(values_ref, writes_ref, reads_ref, docs_ref, out_ref):
    wide, narrow = values_ref.shape[1], writes_ref.shape[1]
    out_ref[:, 0:wide] = values_ref[...]
    out_ref[:, wide : wide + narrow] = writes_ref[...]
    out_ref[:, wide + narrow : wide + 2 * narrow] = reads_ref[...]
    blocks = docs_ref.shape[0]
    last = jnp.broadcast_to(doc_rows(docs_ref)[blocks - 1 :], (8, BLOCK))
    column = transposed(last)[BLOCK - EDGE :, 0:1]
    out_ref[:, wide + 2 * narrow :] = jnp.broadcast_to(column, (EDGE, LANES)).astype(BF16)


def pack_edge(values, writes, reads, docs):
    tokens, wide = values.shape
    narrow = writes.shape[1]
    at = tokens // EDGE - 1
    return pl.pallas_call(
        pack_kernel,
        grid=(1,),
        in_specs=[
            pl.BlockSpec((EDGE, wide), lambda i: (at, 0)),
            pl.BlockSpec((EDGE, narrow), lambda i: (at, 0)),
            pl.BlockSpec((EDGE, narrow), lambda i: (at, 0)),
            pl.BlockSpec(docs.shape, lambda i: (0, 0)),
        ],
        out_specs=pl.BlockSpec((EDGE, wide + 2 * narrow + LANES), lambda i: (0, 0)),
        out_shape=shape((EDGE, wide + 2 * narrow + LANES), BF16),
        name="pack_edge",
    )(values, writes, reads, docs)


def state_kernel(
    before_ref,
    values_ref,
    writes_ref,
    step_ref,
    rate_ref,
    jump_ref,
    docs_ref,
    taps_values_ref,
    taps_write_ref,
    sv_ref,
    sw_ref,
    run_ref,
    stepped_ref,
    enter_ref,
    send_ref,
    ext_ref,
    wext_ref,
    dext_ref,
):
    tokens, wide = values_ref.shape
    narrow = writes_ref.shape[1]
    blocks = tokens // BLOCK
    heads = step_ref.shape[0]
    docs = doc_rows(docs_ref)
    place_docs(dext_ref, before_ref.at[:, wide + 2 * narrow :], docs, blocks)
    ext_ref[0:EDGE] = before_ref[:, 0:wide].astype(F32)
    ext_ref[EDGE:] = values_ref[...].astype(F32)
    wext_ref[0:EDGE] = before_ref[:, wide : wide + narrow].astype(F32)
    wext_ref[EDGE:] = writes_ref[...].astype(F32)
    short_filter(wext_ref, dext_ref, taps_write_ref, sw_ref, blocks, narrow)
    short_filter(ext_ref, dext_ref, taps_values_ref, sv_ref, blocks, wide)

    raw = step_ref[...].astype(F32)
    step = jnp.maximum(raw, 0.0) + jnp.log1p(jnp.exp(-jnp.abs(raw)))
    stepped_ref[...] = step
    rate = jnp.concatenate([jnp.full((1, tokens), rate_ref[h], F32) for h in range(heads)])
    log_decay = jump_ref[...] - rate * step
    held = None
    total = jnp.zeros((heads, 1), F32)
    head_size = wide // heads
    for b in range(blocks):
        span = slice(b * BLOCK, (b + 1) * BLOCK)
        run = running_sum(log_decay[:, span])
        run_ref[:, span] = run
        last = run[:, BLOCK - 1 :]
        total = total + last
        row = docs[b : b + 1]
        end = row[:, BLOCK - 1 :]
        factor = jnp.where(row == end, jnp.exp(last - run) * step[:, span], 0.0)
        columns = transposed(factor)
        scaled = jnp.concatenate(
            [
                (
                    sv_ref[span, p * LANES : (p + 1) * LANES].astype(F32)
                    * per_channel(columns, p, BLOCK)
                ).astype(BF16)
                for p in range(wide // LANES)
            ],
            axis=1,
        )
        fresh = lax.dot_general(
            scaled, sw_ref[span], (((0,), (0,)), ((), ())), preferred_element_type=F32
        )
        if held is None:
            held = fresh
        else:
            enter_ref[b - 1] = held.astype(BF16)
            passing = jnp.where(docs[b - 1 : b, BLOCK - 1 :] == end, jnp.exp(last), 0.0)
            held = jnp.concatenate(
                [
                    held[h * head_size : (h + 1) * head_size] * passing[h : h + 1]
                    + fresh[h * head_size : (h + 1) * head_size]
                    for h in range(heads)
                ]
            )
    send_ref[0:wide] = held.astype(BF16)
    behind = before_ref[EDGE - 1 : EDGE, wide + 2 * narrow :].astype(F32)
    whole = jnp.where(
        behind == docs[blocks - 1 :, BLOCK - 1 :], jnp.broadcast_to(jnp.exp(total), (heads, LANES)), 0.0
    )
    send_ref[wide:] = jnp.concatenate([whole, jnp.zeros((16 - heads, LANES), F32)]).astype(BF16)


def local_states(before, values, writes, step_raw, rate, jump, docs, taps_values, taps_write):
    tokens, wide = values.shape
    narrow = writes.shape[1]
    heads = step_raw.shape[0]
    blocks = tokens // BLOCK
    return pl.pallas_call(
        state_kernel,
        in_specs=[vmem()] * 4 + [smem()] + [vmem()] * 4,
        out_shape=(
            shape((tokens, wide), BF16),
            shape((tokens, narrow), BF16),
            shape((heads, tokens), F32),
            shape((heads, tokens), F32),
            shape((blocks - 1, wide, narrow), BF16),
            shape((wide + 16, narrow), BF16),
        ),
        scratch_shapes=[
            pltpu.VMEM((EDGE + tokens, wide), F32),
            pltpu.VMEM((EDGE + tokens, narrow), F32),
            pltpu.VMEM((EDGE + tokens, LANES), F32),
        ],
        cost_estimate=pl.CostEstimate(flops=400_000_000, transcendentals=0, bytes_accessed=4_000_000),
        name="local_states",
    )(before, values, writes, step_raw, rate, jump, docs, taps_values, taps_write)


def decayed(near, decay, far, heads):
    size = near.shape[0] // heads
    return jnp.concatenate(
        [
            near[h * size : (h + 1) * size] + decay[h : h + 1] * far[h * size : (h + 1) * size]
            for h in range(heads)
        ]
    )


def join_kernel(heads, own_ref, near_ref, out_ref):
    wide = out_ref.shape[0]
    own = own_ref[0:wide].astype(F32)
    decay = own_ref[wide:].astype(F32)
    out_ref[...] = decayed(own, decay, near_ref[0:wide].astype(F32), heads).astype(BF16)


def join_states(own, near, heads):
    return pl.pallas_call(
        functools.partial(join_kernel, heads),
        out_shape=shape((own.shape[0] - 16, own.shape[1]), BF16),
        name="join_states",
    )(own, near)


def inner_kernel(
    before_ref,
    reads_ref,
    docs_ref,
    taps_ref,
    sv_ref,
    sw_ref,
    run_ref,
    step_ref,
    enter_ref,
    sr_ref,
    mixed_ref,
    reach_ref,
    ext_ref,
    dext_ref,
):
    tokens, narrow = reads_ref.shape
    wide = sv_ref.shape[1]
    blocks = tokens // BLOCK
    docs = doc_rows(docs_ref)
    place_docs(dext_ref, before_ref.at[:, wide + 2 * narrow :], docs, blocks)
    ext_ref[0:EDGE] = before_ref[:, wide + narrow : wide + 2 * narrow].astype(F32)
    ext_ref[EDGE:] = reads_ref[...].astype(F32)
    short_filter(ext_ref, dext_ref, taps_ref, sr_ref, blocks, narrow)
    target = lax.broadcasted_iota(jnp.int32, (BLOCK, BLOCK), 0)
    source = lax.broadcasted_iota(jnp.int32, (BLOCK, BLOCK), 1)
    low = source < LANES // 2
    gain = None
    for b in range(blocks):
        span = slice(b * BLOCK, (b + 1) * BLOCK)
        row = docs[b : b + 1]
        column = dext_ref[EDGE + b * BLOCK : EDGE + (b + 1) * BLOCK]
        allowed = (target >= source) & (column == row)
        reads, writes = sr_ref[span], sw_ref[span]
        scores = lax.dot_general(
            reads, writes, (((1,), (1,)), ((), ())), preferred_element_type=F32
        )
        run, step = run_ref[:, span], step_ref[:, span]
        run_columns = transposed(run)
        if b == 0:
            prior = before_ref[EDGE - 1 : EDGE, wide + 2 * narrow :].astype(F32)
        else:
            prior = jnp.broadcast_to(docs[b - 1 : b, BLOCK - 1 :], (1, BLOCK))
        reach = jnp.where(row == prior, jnp.exp(run), 0.0)
        last = run[:, BLOCK - 1 :]
        passing = jnp.where(row[:, BLOCK - 1 :] == prior[:, 0:1], jnp.exp(last), 0.0)
        reach_ref[:, span] = reach if gain is None else reach * gain
        gain = passing if gain is None else gain * passing
        reach_columns = transposed(reach)
        if b > 0:
            taken = lax.dot_general(
                reads, enter_ref[b - 1], (((1,), (1,)), ((), ())), preferred_element_type=F32
            )
        for p in range(wide // LANES):
            cols = slice(p * LANES, (p + 1) * LANES)
            weights = []
            for h in (2 * p, 2 * p + 1):
                spread = run_columns[:, h : h + 1] - run[h : h + 1]
                decay = jnp.exp(jnp.where(allowed, spread, -1e30))
                weights.append((decay * scores * step[h : h + 1]).astype(BF16))
            here = sv_ref[span, cols]
            zero = jnp.zeros_like(here)
            both = jnp.concatenate([jnp.where(low, here, zero), jnp.where(low, zero, here)])
            mixed = jnp.dot(
                jnp.concatenate(weights, axis=1), both, preferred_element_type=F32
            )
            if b > 0:
                mixed = mixed + taken[:, cols] * per_channel(reach_columns, p, BLOCK)
            mixed_ref[span, cols] = mixed


def local_mix(before, reads, docs, taps, sv, sw, run, step, enter):
    tokens, narrow = reads.shape
    wide = sv.shape[1]
    heads = step.shape[0]
    return pl.pallas_call(
        inner_kernel,
        out_shape=(
            shape((tokens, narrow), BF16),
            shape((tokens, wide), F32),
            shape((heads, tokens), F32),
        ),
        scratch_shapes=[
            pltpu.VMEM((EDGE + tokens, narrow), F32),
            pltpu.VMEM((EDGE + tokens, LANES), F32),
        ],
        cost_estimate=pl.CostEstimate(flops=800_000_000, transcendentals=0, bytes_accessed=4_000_000),
        name="local_mix",
    )(before, reads, docs, taps, sv, sw, run, step, enter)


def project_kernel(
    core_ref,
    near_ref,
    far_ref,
    sr_ref,
    mixed_ref,
    reach_ref,
    gate_ref,
    gain_ref,
    weight_ref,
    mine_ref,
    other_ref,
    in_ref,
):
    tokens, wide = mixed_ref.shape
    heads = reach_ref.shape[0]
    share = mine_ref.shape[2]
    near = near_ref[0:wide].astype(F32)
    decay = near_ref[wide:].astype(F32)
    held = decayed(near, decay, far_ref[...].astype(F32), heads).astype(BF16)
    for b in range(tokens // BLOCK):
        span = slice(b * BLOCK, (b + 1) * BLOCK)
        taken = lax.dot_general(
            sr_ref[span], held, (((1,), (1,)), ((), ())), preferred_element_type=F32
        )
        columns = transposed(reach_ref[:, span])
        parts, square = [], None
        for p in range(wide // LANES):
            cols = slice(p * LANES, (p + 1) * LANES)
            mixed = mixed_ref[span, cols] + taken[:, cols] * per_channel(columns, p, BLOCK)
            part = mixed * silu(gate_ref[span, cols].astype(F32))
            parts.append(part)
            square = part * part if square is None else square + part * part
        mean = jnp.sum(square, axis=1, keepdims=True) / wide
        scale = lax.rsqrt(mean + norm_eps)
        for p, part in enumerate(parts):
            cols = slice(p * LANES, (p + 1) * LANES)
            in_ref[span, cols] = (part * scale * gain_ref[:, cols].astype(F32)).astype(BF16)
    core = core_ref[0]
    rows = in_ref[...]
    for flip, out_ref in ((1, other_ref), (0, mine_ref)):
        for k in range(out_ref.shape[0]):
            c = 2 * k + (core ^ flip)
            cols = pl.ds(pl.multiple_of(c * share, share), share)
            out_ref[k] = jnp.dot(rows, weight_ref[:, cols], preferred_element_type=F32).astype(BF16)


def vmem():
    return pl.BlockSpec(memory_space=pltpu.VMEM)


def smem():
    return pl.BlockSpec(memory_space=pltpu.SMEM)


def project(core, near, far, sr, mixed, reach, gate, gain, weight, owners):
    tokens, wide = mixed.shape
    share = weight.shape[1] // (2 * owners)
    return pl.pallas_call(
        project_kernel,
        in_specs=[smem()] + [vmem()] * 8,
        out_shape=(shape((owners, tokens, share), BF16),) * 2,
        scratch_shapes=[pltpu.VMEM((tokens, wide), BF16)],
        cost_estimate=pl.CostEstimate(
            flops=2 * tokens * wide * weight.shape[1], transcendentals=0, bytes_accessed=6_000_000
        ),
        name="project",
    )(core, near, far, sr, mixed, reach, gate, gain, weight)


def after_kernel(at_ref, parts_ref, residual_ref, own_ref, out_ref):
    total = residual_ref[...].astype(F32)
    for k in range(parts_ref.shape[0]):
        total = total + parts_ref[k].astype(F32)
    after = total.astype(BF16)
    own_ref[...] = after
    for k in range(out_ref.shape[0]):
        out_ref[k] = after


def after_mix(at, parts, residual):
    owners, tokens, share = parts.shape
    return pl.pallas_call(
        after_kernel,
        grid_spec=pltpu.PrefetchScalarGridSpec(
            num_scalar_prefetch=1,
            grid=(1,),
            in_specs=[
                pl.BlockSpec((owners, tokens, share), lambda i, at: (0, 0, 0)),
                pl.BlockSpec((tokens, share), lambda i, at: (0, at[0])),
            ],
            out_specs=[
                pl.BlockSpec((tokens, share), lambda i, at: (0, 0)),
                pl.BlockSpec((owners, tokens, share), lambda i, at: (0, 0, 0)),
            ],
        ),
        out_shape=(shape((tokens, share), BF16), shape((owners, tokens, share), BF16)),
        name="after_mix",
    )(at, parts, residual)


def mixer_kernel(peers, at_ref, place_ref, group_ref, mine_ref, other_ref, gain_ref, weight_ref, *refs):
    down_refs = refs[:peers]
    out_refs = refs[peers : peers + 2]
    after, normal, late, downs, hidden_ref, out, after_sem, late_sem, down_sem, out_sem = refs[
        peers + 2 :
    ]
    _, owners, _, share = after.shape
    _, units, _ = downs.shape
    core, place, group = at_ref[0], place_ref[0], group_ref[0]

    loads = [
        pltpu.make_async_copy(ref, after.at[k], after_sem.at[k])
        for k, ref in enumerate((mine_ref, other_ref))
    ]
    heavy = pltpu.make_async_copy(weight_ref, late, late_sem)
    rows = []
    for k, ref in enumerate(down_refs):
        turn = jnp.where(lax.rem(group, 2) == 0, peers - k, k)
        index = lax.rem(place + turn, peers)
        rows.append(pltpu.make_async_copy(ref, downs.at[index], down_sem.at[k]))
    for copy in (*loads, heavy):
        copy.start()

    for copy in loads:
        copy.wait()
    square = None
    for flip in range(2):
        for k in range(owners):
            x = after[flip, k].astype(F32)
            square = x * x if square is None else square + x * x
    scale = lax.rsqrt(jnp.sum(square, axis=1, keepdims=True) / (2 * owners * share) + norm_eps)
    for flip in range(2):
        for k in range(owners):
            c = 2 * k + (core ^ flip)
            cols = pl.ds(pl.multiple_of(c * share, share), share)
            normal[:, cols] = (
                after[flip, k].astype(F32) * scale * gain_ref[:, cols].astype(F32)
            ).astype(BF16)
    heavy.wait()
    for copy in rows:
        copy.start()
    across = (((1,), (1,)), ((), ()))
    gates = jnp.concatenate([late[k, 0:units] for k in range(peers)], axis=1)
    gate = lax.dot_general(normal[...], gates, across, preferred_element_type=F32)
    ups = jnp.concatenate([late[k, units:] for k in range(peers)], axis=1)
    up = lax.dot_general(normal[...], ups, across, preferred_element_type=F32)
    hidden_ref[...] = (silu(gate) * up).astype(BF16)
    for copy in rows:
        copy.wait()
    stores = []
    for flip in (1, 0):
        for k in range(owners):
            c = 2 * k + (core ^ flip)
            part = jnp.concatenate([downs[2 * c], downs[2 * c + 1]], axis=1)
            out[flip, k] = jnp.dot(hidden_ref[...], part, preferred_element_type=F32).astype(BF16)
            store = pltpu.make_async_copy(
                out.at[flip, k], out_refs[flip].at[k], out_sem.at[flip, k]
            )
            store.start()
            stores.append(store)
    for store in stores:
        store.wait()


def channel_mixer(at, place, group, mine, other, gain, weights, downs):
    owners, tokens, share = mine.shape
    peers, units, depth = len(downs), *downs[0].shape
    anywhere = pl.BlockSpec(memory_space=pl.ANY)
    out = shape((owners, tokens, share), BF16)
    return pl.pallas_call(
        functools.partial(mixer_kernel, peers),
        in_specs=[smem()] * 3 + [anywhere, anywhere, vmem(), anywhere] + [anywhere] * peers,
        out_specs=[anywhere, anywhere],
        out_shape=(out, out),
        scratch_shapes=[
            pltpu.VMEM((2, owners, tokens, share), BF16),
            pltpu.VMEM((tokens, peers * depth), BF16),
            pltpu.VMEM((peers, 2 * units, depth), BF16),
            pltpu.VMEM((peers, units, depth), BF16),
            pltpu.VMEM((tokens, units), BF16),
            pltpu.VMEM((2, owners, tokens, share), BF16),
            pltpu.SemaphoreType.DMA((2,)),
            pltpu.SemaphoreType.DMA,
            pltpu.SemaphoreType.DMA((peers,)),
            pltpu.SemaphoreType.DMA((2, owners)),
        ],
        cost_estimate=pl.CostEstimate(
            flops=12 * tokens * owners * share * units, transcendentals=0, bytes_accessed=14_000_000
        ),
        name="channel_mixer",
    )(at, place, group, mine, other, gain, weights, *downs)


def gathered(value, axis, groups):
    peers, count = lax.axis_size(axis), lax.axis_size(groups)
    around = [
        (g * peers + i, g * peers + (i + 1 - 2 * (g % 2)) % peers)
        for g in range(count)
        for i in range(peers)
    ]
    across = [(g, g ^ 1) for g in range(count)]
    found = {0: value}
    for k in range(1, peers // 2 + 1):
        value = lax.ppermute(value, (groups, axis), around)
        found[k] = value
        if k < peers - k:
            found[peers - k] = lax.ppermute(value, groups, across)
    return [found[k] for k in range(peers)]


def out_kernel(parts_ref, own_ref, out_ref):
    total = None
    for k in range(parts_ref.shape[0]):
        part = parts_ref[k].astype(F32)
        total = part if total is None else total + part
    out_ref[...] = (own_ref[...].astype(F32) + total).astype(BF16)


def add_down(parts, own):
    return pl.pallas_call(out_kernel, out_shape=shape(own.shape, BF16), name="add_down")(parts, own)


def to_partner(value):
    return lax.ppermute(value, "tp", [(i, i ^ 1) for i in range(lax.axis_size("tp"))])


def exchange(value):
    peers = lax.axis_size("tp")
    rows = [[i for i in range(peers) if i % 2 == core] for core in range(2)]
    return lax.all_to_all(value, "tp", 0, 0, axis_index_groups=rows, tiled=True)


def sum_pairs(both):
    return (both[0].astype(F32) + to_partner(both[1]).astype(F32)).astype(BF16)


def on_device(
    residual,
    values,
    out_gate,
    writes,
    reads,
    step_raw,
    decay_rate,
    decay_jump,
    documents,
    taps_values,
    taps_write,
    taps_read,
    mixer_gain,
    mixer_out,
    channel_gain,
    gate_weight,
    up_weight,
    down_rows,
):
    heads = step_raw.shape[0]
    owners = lax.axis_size("tp") // 2
    me = lax.axis_index("tp").astype(jnp.int32)
    at = me.reshape(1)
    core = (me % 2).reshape(1)
    place = lax.axis_index("sp").astype(jnp.int32).reshape(1)
    group = lax.axis_index("grp").astype(jnp.int32).reshape(1)
    late = jnp.concatenate([gate_weight.T, up_weight.T], axis=0)
    weights = lax.all_gather(late, "sp", axis=0)
    downs = gathered(down_rows.T, "sp", "grp")

    docs = documents.reshape(-1, BLOCK)
    before = from_behind(pack_edge(values, writes, reads, docs), "sp", 1)
    sv, sw, run, step, enter, send = local_states(
        before, values, writes, step_raw, decay_rate, decay_jump, docs, taps_values, taps_write
    )
    near = from_behind(send, "sp", 1)
    gains = mixer_gain.reshape(1, -1), channel_gain.reshape(1, -1)
    near, gains = lax.optimization_barrier((near, gains))
    sr, mixed, reach = local_mix(before, reads, docs, taps_read, sv, sw, run, step, enter)
    joined = join_states(send, near, heads)
    far = from_behind(joined, "sp", 2)
    both = project(core, near, far, sr, mixed, reach, out_gate, gains[0], mixer_out, owners)
    parts = sum_pairs(both)
    parts = exchange(parts)
    own_after, spread = after_mix(at, parts, residual)
    mine = exchange(spread)
    other = to_partner(mine)
    both = channel_mixer(core, place, group, mine, other, gains[1], weights, downs)
    parts = sum_pairs(both)
    parts = exchange(parts)
    return add_down(parts, own_after)


def solution(mesh):
    return jax.shard_map(
        on_device,
        mesh=mesh,
        in_specs=(
            P(("grp", "sp"), None),
            P(("grp", "sp"), "tp"),
            P(("grp", "sp"), "tp"),
            P(("grp", "sp"), "tp"),
            P(("grp", "sp"), "tp"),
            P("tp", ("grp", "sp")),
            P("tp"),
            P("tp", ("grp", "sp")),
            P(("grp", "sp")),
            P(None, "tp"),
            P(None, "tp"),
            P(None, "tp"),
            P("tp"),
            P("tp", None),
            P(),
            P("sp", "tp"),
            P("sp", "tp"),
            P("sp", "tp"),
        ),
        out_specs=P(("grp", "sp"), "tp"),
        check_vma=False,
    )
```

```python
import functools

import jax
import jax.numpy as jnp
from jax import lax
from jax.experimental import pallas as pl
from jax.experimental.pallas import tpu as pltpu
from jax.sharding import PartitionSpec as P


BLOCK = 128
EDGE = 16
LANES = 128

norm_eps = 1e-06

F32 = jnp.float32
BF16 = jnp.bfloat16


def from_behind(value, axis, by):
    peers = lax.axis_size(axis)
    pairs = [(i, i + by) for i in range(peers) if 0 <= i + by < peers]
    return lax.ppermute(value, axis, pairs)


def silu(x):
    return x * jax.nn.sigmoid(x)


def shape(dims, kind):
    return jax.ShapeDtypeStruct(dims, kind)


def transposed(rows):
    return jnp.transpose(rows, (1, 0))


def doc_rows(docs_ref):
    return docs_ref[...].astype(F32)


def running_sum(x):
    lane = lax.broadcasted_iota(jnp.int32, x.shape, 1)
    shift = 1
    while shift < x.shape[1]:
        x = x + jnp.where(lane >= shift, pltpu.roll(x, shift, 1), 0.0)
        shift *= 2
    return x


def per_channel(columns, pair, rows):
    lane = lax.broadcasted_iota(jnp.int32, (rows, LANES), 1)
    return jnp.where(
        lane < LANES // 2,
        jnp.broadcast_to(columns[:, 2 * pair : 2 * pair + 1], (rows, LANES)),
        jnp.broadcast_to(columns[:, 2 * pair + 1 : 2 * pair + 2], (rows, LANES)),
    )


def place_docs(dext_ref, prior_ref, docs, blocks):
    dext_ref[0:EDGE] = prior_ref[...].astype(F32)
    padded = jnp.concatenate([docs, jnp.zeros((8 - blocks, BLOCK), F32)]) if blocks < 8 else docs
    columns = transposed(padded)
    for b in range(blocks):
        dext_ref[EDGE + b * BLOCK : EDGE + (b + 1) * BLOCK] = jnp.broadcast_to(
            columns[:, b : b + 1], (BLOCK, LANES)
        )


def short_filter(ext_ref, dext_ref, taps_ref, out_ref, blocks, width):
    taps = taps_ref[...].astype(F32)
    count = taps.shape[0]
    for b in range(blocks):
        first = EDGE + b * BLOCK
        own = dext_ref[first : first + BLOCK]
        masks = [
            dext_ref[first - count + 1 + k : first - count + 1 + k + BLOCK] == own
            for k in range(count - 1)
        ]
        for c in range(width // LANES):
            cols = slice(c * LANES, (c + 1) * LANES)
            total = None
            for k in range(count):
                start = first - count + 1 + k
                term = ext_ref[start : start + BLOCK, cols] * taps[k : k + 1, cols]
                if k < count - 1:
                    term = jnp.where(masks[k], term, 0.0)
                total = term if total is None else total + term
            out_ref[b * BLOCK : (b + 1) * BLOCK, cols] = silu(total).astype(BF16)


def pack_kernel(values_ref, writes_ref, reads_ref, docs_ref, out_ref):
    wide, narrow = values_ref.shape[1], writes_ref.shape[1]
    out_ref[:, 0:wide] = values_ref[...]
    out_ref[:, wide : wide + narrow] = writes_ref[...]
    out_ref[:, wide + narrow : wide + 2 * narrow] = reads_ref[...]
    blocks = docs_ref.shape[0]
    last = jnp.broadcast_to(doc_rows(docs_ref)[blocks - 1 :], (8, BLOCK))
    column = transposed(last)[BLOCK - EDGE :, 0:1]
    out_ref[:, wide + 2 * narrow :] = jnp.broadcast_to(column, (EDGE, LANES)).astype(BF16)


def pack_edge(values, writes, reads, docs):
    tokens, wide = values.shape
    narrow = writes.shape[1]
    at = tokens // EDGE - 1
    return pl.pallas_call(
        pack_kernel,
        grid=(1,),
        in_specs=[
            pl.BlockSpec((EDGE, wide), lambda i: (at, 0)),
            pl.BlockSpec((EDGE, narrow), lambda i: (at, 0)),
            pl.BlockSpec((EDGE, narrow), lambda i: (at, 0)),
            pl.BlockSpec(docs.shape, lambda i: (0, 0)),
        ],
        out_specs=pl.BlockSpec((EDGE, wide + 2 * narrow + LANES), lambda i: (0, 0)),
        out_shape=shape((EDGE, wide + 2 * narrow + LANES), BF16),
        name="pack_edge",
    )(values, writes, reads, docs)


def state_kernel(
    before_ref,
    values_ref,
    writes_ref,
    step_ref,
    rate_ref,
    jump_ref,
    docs_ref,
    taps_values_ref,
    taps_write_ref,
    sv_ref,
    sw_ref,
    run_ref,
    stepped_ref,
    enter_ref,
    send_ref,
    ext_ref,
    wext_ref,
    dext_ref,
):
    tokens, wide = values_ref.shape
    narrow = writes_ref.shape[1]
    blocks = tokens // BLOCK
    heads = step_ref.shape[0]
    docs = doc_rows(docs_ref)
    place_docs(dext_ref, before_ref.at[:, wide + 2 * narrow :], docs, blocks)
    ext_ref[0:EDGE] = before_ref[:, 0:wide].astype(F32)
    ext_ref[EDGE:] = values_ref[...].astype(F32)
    wext_ref[0:EDGE] = before_ref[:, wide : wide + narrow].astype(F32)
    wext_ref[EDGE:] = writes_ref[...].astype(F32)
    short_filter(wext_ref, dext_ref, taps_write_ref, sw_ref, blocks, narrow)
    short_filter(ext_ref, dext_ref, taps_values_ref, sv_ref, blocks, wide)

    raw = step_ref[...].astype(F32)
    step = jnp.maximum(raw, 0.0) + jnp.log1p(jnp.exp(-jnp.abs(raw)))
    stepped_ref[...] = step
    log_decay = jump_ref[...] - rate_ref[...] * step
    held = None
    total = jnp.zeros((heads, 1), F32)
    head_size = wide // heads
    for b in range(blocks):
        span = slice(b * BLOCK, (b + 1) * BLOCK)
        run = running_sum(log_decay[:, span])
        run_ref[:, span] = run
        last = run[:, BLOCK - 1 :]
        total = total + last
        row = docs[b : b + 1]
        end = row[:, BLOCK - 1 :]
        factor = jnp.where(row == end, jnp.exp(last - run) * step[:, span], 0.0)
        columns = transposed(factor)
        scaled = jnp.concatenate(
            [
                (
                    sv_ref[span, p * LANES : (p + 1) * LANES].astype(F32)
                    * per_channel(columns, p, BLOCK)
                ).astype(BF16)
                for p in range(wide // LANES)
            ],
            axis=1,
        )
        fresh = lax.dot_general(
            scaled, sw_ref[span], (((0,), (0,)), ((), ())), preferred_element_type=F32
        )
        if held is None:
            held = fresh
        else:
            enter_ref[b - 1] = held.astype(BF16)
            passing = jnp.where(docs[b - 1 : b, BLOCK - 1 :] == end, jnp.exp(last), 0.0)
            held = jnp.concatenate(
                [
                    held[h * head_size : (h + 1) * head_size] * passing[h : h + 1]
                    + fresh[h * head_size : (h + 1) * head_size]
                    for h in range(heads)
                ]
            )
    send_ref[0:wide] = held.astype(BF16)
    behind = before_ref[EDGE - 1 : EDGE, wide + 2 * narrow :].astype(F32)
    whole = jnp.where(
        behind == docs[blocks - 1 :, BLOCK - 1 :], jnp.broadcast_to(jnp.exp(total), (heads, LANES)), 0.0
    )
    send_ref[wide:] = jnp.concatenate([whole, jnp.zeros((16 - heads, LANES), F32)]).astype(BF16)


def local_states(before, values, writes, step_raw, rate, jump, docs, taps_values, taps_write):
    tokens, wide = values.shape
    narrow = writes.shape[1]
    heads = step_raw.shape[0]
    blocks = tokens // BLOCK
    return pl.pallas_call(
        state_kernel,
        out_shape=(
            shape((tokens, wide), BF16),
            shape((tokens, narrow), BF16),
            shape((heads, tokens), F32),
            shape((heads, tokens), F32),
            shape((blocks - 1, wide, narrow), BF16),
            shape((wide + 16, narrow), BF16),
        ),
        scratch_shapes=[
            pltpu.VMEM((EDGE + tokens, wide), F32),
            pltpu.VMEM((EDGE + tokens, narrow), F32),
            pltpu.VMEM((EDGE + tokens, LANES), F32),
        ],
        cost_estimate=pl.CostEstimate(flops=400_000_000, transcendentals=0, bytes_accessed=4_000_000),
        name="local_states",
    )(before, values, writes, step_raw, rate, jump, docs, taps_values, taps_write)


def decayed(near, decay, far, heads):
    size = near.shape[0] // heads
    return jnp.concatenate(
        [
            near[h * size : (h + 1) * size] + decay[h : h + 1] * far[h * size : (h + 1) * size]
            for h in range(heads)
        ]
    )


def join_kernel(heads, own_ref, near_ref, out_ref):
    wide = out_ref.shape[0]
    own = own_ref[0:wide].astype(F32)
    decay = own_ref[wide:].astype(F32)
    out_ref[...] = decayed(own, decay, near_ref[0:wide].astype(F32), heads).astype(BF16)


def join_states(own, near, heads):
    return pl.pallas_call(
        functools.partial(join_kernel, heads),
        out_shape=shape((own.shape[0] - 16, own.shape[1]), BF16),
        name="join_states",
    )(own, near)


def inner_kernel(
    before_ref,
    reads_ref,
    docs_ref,
    taps_ref,
    sv_ref,
    sw_ref,
    run_ref,
    step_ref,
    enter_ref,
    sr_ref,
    mixed_ref,
    reach_ref,
    ext_ref,
    dext_ref,
):
    tokens, narrow = reads_ref.shape
    wide = sv_ref.shape[1]
    blocks = tokens // BLOCK
    docs = doc_rows(docs_ref)
    place_docs(dext_ref, before_ref.at[:, wide + 2 * narrow :], docs, blocks)
    ext_ref[0:EDGE] = before_ref[:, wide + narrow : wide + 2 * narrow].astype(F32)
    ext_ref[EDGE:] = reads_ref[...].astype(F32)
    short_filter(ext_ref, dext_ref, taps_ref, sr_ref, blocks, narrow)
    target = lax.broadcasted_iota(jnp.int32, (BLOCK, BLOCK), 0)
    source = lax.broadcasted_iota(jnp.int32, (BLOCK, BLOCK), 1)
    low = source < LANES // 2
    gain = None
    for b in range(blocks):
        span = slice(b * BLOCK, (b + 1) * BLOCK)
        row = docs[b : b + 1]
        column = dext_ref[EDGE + b * BLOCK : EDGE + (b + 1) * BLOCK]
        allowed = (target >= source) & (column == row)
        reads, writes = sr_ref[span], sw_ref[span]
        scores = lax.dot_general(
            reads, writes, (((1,), (1,)), ((), ())), preferred_element_type=F32
        )
        run, step = run_ref[:, span], step_ref[:, span]
        run_columns = transposed(run)
        if b == 0:
            prior = before_ref[EDGE - 1 : EDGE, wide + 2 * narrow :].astype(F32)
        else:
            prior = jnp.broadcast_to(docs[b - 1 : b, BLOCK - 1 :], (1, BLOCK))
        reach = jnp.where(row == prior, jnp.exp(run), 0.0)
        last = run[:, BLOCK - 1 :]
        passing = jnp.where(row[:, BLOCK - 1 :] == prior[:, 0:1], jnp.exp(last), 0.0)
        reach_ref[:, span] = reach if gain is None else reach * gain
        gain = passing if gain is None else gain * passing
        reach_columns = transposed(reach)
        if b > 0:
            taken = lax.dot_general(
                reads, enter_ref[b - 1], (((1,), (1,)), ((), ())), preferred_element_type=F32
            )
        for p in range(wide // LANES):
            cols = slice(p * LANES, (p + 1) * LANES)
            weights = []
            for h in (2 * p, 2 * p + 1):
                spread = run_columns[:, h : h + 1] - run[h : h + 1]
                decay = jnp.exp(jnp.where(allowed, spread, -1e30))
                weights.append((decay * scores * step[h : h + 1]).astype(BF16))
            here = sv_ref[span, cols]
            zero = jnp.zeros_like(here)
            both = jnp.concatenate([jnp.where(low, here, zero), jnp.where(low, zero, here)])
            mixed = jnp.dot(
                jnp.concatenate(weights, axis=1), both, preferred_element_type=F32
            )
            if b > 0:
                mixed = mixed + taken[:, cols] * per_channel(reach_columns, p, BLOCK)
            mixed_ref[span, cols] = mixed


def local_mix(before, reads, docs, taps, sv, sw, run, step, enter):
    tokens, narrow = reads.shape
    wide = sv.shape[1]
    heads = step.shape[0]
    return pl.pallas_call(
        inner_kernel,
        out_shape=(
            shape((tokens, narrow), BF16),
            shape((tokens, wide), F32),
            shape((heads, tokens), F32),
        ),
        scratch_shapes=[
            pltpu.VMEM((EDGE + tokens, narrow), F32),
            pltpu.VMEM((EDGE + tokens, LANES), F32),
        ],
        cost_estimate=pl.CostEstimate(flops=800_000_000, transcendentals=0, bytes_accessed=4_000_000),
        name="local_mix",
    )(before, reads, docs, taps, sv, sw, run, step, enter)


def project_kernel(
    core_ref,
    near_ref,
    far_ref,
    sr_ref,
    mixed_ref,
    reach_ref,
    gate_ref,
    gain_ref,
    weight_ref,
    mine_ref,
    other_ref,
    in_ref,
):
    tokens, wide = mixed_ref.shape
    heads = reach_ref.shape[0]
    share = mine_ref.shape[2]
    near = near_ref[0:wide].astype(F32)
    decay = near_ref[wide:].astype(F32)
    held = decayed(near, decay, far_ref[...].astype(F32), heads).astype(BF16)
    for b in range(tokens // BLOCK):
        span = slice(b * BLOCK, (b + 1) * BLOCK)
        taken = lax.dot_general(
            sr_ref[span], held, (((1,), (1,)), ((), ())), preferred_element_type=F32
        )
        columns = transposed(reach_ref[:, span])
        parts, square = [], None
        for p in range(wide // LANES):
            cols = slice(p * LANES, (p + 1) * LANES)
            mixed = mixed_ref[span, cols] + taken[:, cols] * per_channel(columns, p, BLOCK)
            part = mixed * silu(gate_ref[span, cols].astype(F32))
            parts.append(part)
            square = part * part if square is None else square + part * part
        mean = jnp.sum(square, axis=1, keepdims=True) / wide
        scale = lax.rsqrt(mean + norm_eps)
        for p, part in enumerate(parts):
            cols = slice(p * LANES, (p + 1) * LANES)
            in_ref[span, cols] = (part * scale * gain_ref[:, cols].astype(F32)).astype(BF16)
    core = core_ref[0]
    rows = in_ref[...]
    for flip, out_ref in ((1, other_ref), (0, mine_ref)):
        for k in range(out_ref.shape[0]):
            c = 2 * k + (core ^ flip)
            cols = pl.ds(pl.multiple_of(c * share, share), share)
            out_ref[k] = jnp.dot(rows, weight_ref[:, cols], preferred_element_type=F32).astype(BF16)


def vmem():
    return pl.BlockSpec(memory_space=pltpu.VMEM)


def smem():
    return pl.BlockSpec(memory_space=pltpu.SMEM)


def project(core, near, far, sr, mixed, reach, gate, gain, weight, owners):
    tokens, wide = mixed.shape
    share = weight.shape[1] // (2 * owners)
    return pl.pallas_call(
        project_kernel,
        in_specs=[smem()] + [vmem()] * 8,
        out_shape=(shape((owners, tokens, share), BF16),) * 2,
        scratch_shapes=[pltpu.VMEM((tokens, wide), BF16)],
        cost_estimate=pl.CostEstimate(
            flops=2 * tokens * wide * weight.shape[1], transcendentals=0, bytes_accessed=6_000_000
        ),
        name="project",
    )(core, near, far, sr, mixed, reach, gate, gain, weight)


def after_kernel(at_ref, parts_ref, residual_ref, own_ref, out_ref):
    total = residual_ref[...].astype(F32)
    for k in range(parts_ref.shape[0]):
        total = total + parts_ref[k].astype(F32)
    after = total.astype(BF16)
    own_ref[...] = after
    for k in range(out_ref.shape[0]):
        out_ref[k] = after


def after_mix(at, parts, residual):
    owners, tokens, share = parts.shape
    return pl.pallas_call(
        after_kernel,
        grid_spec=pltpu.PrefetchScalarGridSpec(
            num_scalar_prefetch=1,
            grid=(1,),
            in_specs=[
                pl.BlockSpec((owners, tokens, share), lambda i, at: (0, 0, 0)),
                pl.BlockSpec((tokens, share), lambda i, at: (0, at[0])),
            ],
            out_specs=[
                pl.BlockSpec((tokens, share), lambda i, at: (0, 0)),
                pl.BlockSpec((owners, tokens, share), lambda i, at: (0, 0, 0)),
            ],
        ),
        out_shape=(shape((tokens, share), BF16), shape((owners, tokens, share), BF16)),
        name="after_mix",
    )(at, parts, residual)


def normal_kernel(at_ref, mine_ref, other_ref, gain_ref, out_ref):
    owners, _, share = mine_ref.shape
    core = lax.rem(at_ref[0], 2)
    square = None
    for ref in (mine_ref, other_ref):
        for k in range(owners):
            x = ref[k].astype(F32)
            square = x * x if square is None else square + x * x
    scale = lax.rsqrt(jnp.sum(square, axis=1, keepdims=True) / (2 * owners * share) + norm_eps)
    for flip, ref in enumerate((mine_ref, other_ref)):
        for k in range(owners):
            c = 2 * k + (core ^ flip)
            cols = pl.ds(pl.multiple_of(c * share, share), share)
            out_ref[:, cols] = (
                ref[k].astype(F32) * scale * gain_ref[:, cols].astype(F32)
            ).astype(BF16)


def normalised(at, mine, other, gain):
    owners, tokens, share = mine.shape
    return pl.pallas_call(
        normal_kernel,
        in_specs=[smem(), vmem(), vmem(), vmem()],
        out_shape=shape((tokens, 2 * owners * share), BF16),
        name="normalised",
    )(at, mine, other, gain)


def mixer_kernel(tiles, at_ref, normal_ref, weight_ref, *refs):
    mine_far, other_far, mine_near, other_near = refs[:4]
    late, downs, hidden_ref, far, near, late_sem, down_sem, far_sem, near_sem = refs[4:]
    peers, units, _ = downs.shape
    _, turns, _, _ = near.shape
    core, chip = lax.rem(at_ref[0], 2), lax.div(at_ref[0], 2)

    heavy = []
    for t, (first, count) in enumerate(tiles):
        heavy.append(
            [
                pltpu.make_async_copy(
                    weight_ref.at[:, pl.ds(base + first, count)],
                    late.at[:, pl.ds(base + first, count)],
                    late_sem.at[t, half],
                )
                for half, base in enumerate((0, units))
            ]
        )
    heavy.append([pltpu.make_async_copy(weight_ref.at[:, pl.ds(2 * units, units)], downs, down_sem)])
    for copy in (*heavy[0], *heavy[1]):
        copy.start()
    across = (((1,), (1,)), ((), ()))
    normal = normal_ref[...]
    for t, (first, count) in enumerate(tiles):
        for copy in heavy[t]:
            copy.wait()
        if t + 2 < len(heavy):
            for copy in heavy[t + 2]:
                copy.start()
        products = []
        for base in (first, units + first):
            part = jnp.concatenate([late[k, base : base + count] for k in range(peers)], axis=1)
            products.append(
                lax.dot_general(normal, part, across, preferred_element_type=F32)
            )
        hidden_ref[:, first : first + count] = (silu(products[0]) * products[1]).astype(BF16)
    heavy[-1][0].wait()
    hidden = hidden_ref[...]
    stores = []

    def store(source, target, sem):
        copy = pltpu.make_async_copy(source, target, sem)
        copy.start()
        stores.append(copy)

    for turn in (2, 0, 1, 3):
        for flip in (1, 0):
            c = 2 * lax.rem(chip + turn, turns + 1) + (core ^ flip)
            part = jnp.concatenate([downs[2 * c], downs[2 * c + 1]], axis=1)
            product = jnp.dot(hidden, part, preferred_element_type=F32).astype(BF16)
            if turn == 2:
                far[flip] = product
                store(far.at[flip], (mine_far, other_far)[flip], far_sem.at[flip])
            else:
                k = (0, 1, None, 2)[turn]
                near[flip, k] = product
                store(near.at[flip, k], (mine_near, other_near)[flip].at[k], near_sem.at[flip, k])
    for copy in stores:
        copy.wait()


def channel_mixer(at, normal, weights, share):
    tokens = normal.shape[0]
    peers, units, depth = weights.shape[0], weights.shape[1] // 3, weights.shape[2]
    turns = normal.shape[1] // (2 * share) - 1
    tiles = [(f, min(256, units - f)) for f in range(0, units, 256)]
    anywhere = pl.BlockSpec(memory_space=pl.ANY)
    far, near = shape((tokens, share), BF16), shape((turns, tokens, share), BF16)
    return pl.pallas_call(
        functools.partial(mixer_kernel, tiles),
        in_specs=[smem(), vmem(), anywhere],
        out_specs=[anywhere] * 4,
        out_shape=(far, far, near, near),
        scratch_shapes=[
            pltpu.VMEM((peers, 2 * units, depth), BF16),
            pltpu.VMEM((peers, units, depth), BF16),
            pltpu.VMEM((tokens, units), BF16),
            pltpu.VMEM((2, tokens, share), BF16),
            pltpu.VMEM((2, turns, tokens, share), BF16),
            pltpu.SemaphoreType.DMA((len(tiles), 2)),
            pltpu.SemaphoreType.DMA,
            pltpu.SemaphoreType.DMA((2,)),
            pltpu.SemaphoreType.DMA((2, turns)),
        ],
        cost_estimate=pl.CostEstimate(
            flops=6 * tokens * normal.shape[1] * units, transcendentals=0, bytes_accessed=14_000_000
        ),
        name="channel_mixer",
    )(at, normal, weights)


def halves_kernel(mine_ref, other_ref, low_ref, high_ref):
    half = low_ref.shape[0]
    low_ref[...] = (mine_ref[:half].astype(F32) + other_ref[:half].astype(F32)).astype(BF16)
    high_ref[...] = (mine_ref[half:].astype(F32) + other_ref[half:].astype(F32)).astype(BF16)


def halves(mine, other):
    part = shape((mine.shape[0] // 2, mine.shape[1]), BF16)
    return pl.pallas_call(halves_kernel, out_shape=(part, part), name="halves")(mine, other)


def onward_kernel(mine_ref, other_ref, low_ref, high_ref, own_ref, right_ref, left_ref):
    half = low_ref.shape[0]
    for k, ref in enumerate((own_ref, right_ref, left_ref)):
        for rows in (slice(0, half), slice(half, 2 * half)):
            total = mine_ref[k, rows].astype(F32) + other_ref[k, rows].astype(F32)
            if k == 1 and rows.start == 0:
                total = total + low_ref[...].astype(F32)
            if k == 2 and rows.start > 0:
                total = total + high_ref[...].astype(F32)
            ref[rows] = total.astype(BF16)


def onward(mine, other, low, high):
    part = shape(mine.shape[1:], BF16)
    return pl.pallas_call(onward_kernel, out_shape=(part,) * 3, name="onward")(mine, other, low, high)


def last_kernel(after_ref, own_ref, right_ref, left_ref, out_ref):
    down = own_ref[...].astype(F32) + right_ref[...].astype(F32) + left_ref[...].astype(F32)
    out_ref[...] = (after_ref[...].astype(F32) + down).astype(BF16)


def add_last(after, own, right, left):
    return pl.pallas_call(last_kernel, out_shape=shape(after.shape, BF16), name="add_last")(
        after, own, right, left
    )


def to_chip(value, by):
    peers = lax.axis_size("tp")
    return lax.ppermute(value, "tp", [(i, (i + 2 * by) % peers) for i in range(peers)])


def sum_round(parts, after):
    mine_far, other_far, mine_near, other_near = parts
    other_far = to_partner(other_far)
    other_near = to_partner(other_near)
    low, high = halves(mine_far, other_far)
    low, high = to_chip(low, 1), to_chip(high, -1)
    own, right, left = onward(mine_near, other_near, low, high)
    return add_last(after, own, to_chip(right, 1), to_chip(left, -1))


def to_partner(value):
    return lax.ppermute(value, "tp", [(i, i ^ 1) for i in range(lax.axis_size("tp"))])


def exchange(value):
    peers = lax.axis_size("tp")
    rows = [[i for i in range(peers) if i % 2 == core] for core in range(2)]
    return lax.all_to_all(value, "tp", 0, 0, axis_index_groups=rows, tiled=True)


def sum_pairs(both):
    return (both[0].astype(F32) + to_partner(both[1]).astype(F32)).astype(BF16)


def on_device(
    residual,
    values,
    out_gate,
    writes,
    reads,
    step_raw,
    decay_rate,
    decay_jump,
    documents,
    taps_values,
    taps_write,
    taps_read,
    mixer_gain,
    mixer_out,
    channel_gain,
    gate_weight,
    up_weight,
    down_rows,
):
    heads = step_raw.shape[0]
    owners = lax.axis_size("tp") // 2
    me = lax.axis_index("tp").astype(jnp.int32)
    at = me.reshape(1)
    core = (me % 2).reshape(1)
    late = jnp.concatenate([gate_weight.T, up_weight.T, down_rows.T], axis=0)
    weights = lax.all_gather(late, "sp", axis=0)

    docs = documents.reshape(-1, BLOCK)
    before = from_behind(pack_edge(values, writes, reads, docs), "sp", 1)
    rate = decay_rate.reshape(-1, 1)
    sv, sw, run, step, enter, send = local_states(
        before, values, writes, step_raw, rate, decay_jump, docs, taps_values, taps_write
    )
    near = from_behind(send, "sp", 1)
    sr, mixed, reach = local_mix(before, reads, docs, taps_read, sv, sw, run, step, enter)
    far = from_behind(join_states(send, near, heads), "sp", 2)
    both = project(
        core, near, far, sr, mixed, reach, out_gate, mixer_gain.reshape(1, -1), mixer_out, owners
    )
    own_after, spread = after_mix(at, exchange(sum_pairs(both)), residual)
    mine = exchange(spread)
    other = to_partner(mine)
    normal = normalised(at, mine, other, channel_gain.reshape(1, -1))
    return sum_round(channel_mixer(at, normal, weights, own_after.shape[1]), own_after)


def solution(mesh):
    return jax.shard_map(
        on_device,
        mesh=mesh,
        in_specs=(
            P(("grp", "sp"), None),
            P(("grp", "sp"), "tp"),
            P(("grp", "sp"), "tp"),
            P(("grp", "sp"), "tp"),
            P(("grp", "sp"), "tp"),
            P("tp", ("grp", "sp")),
            P("tp"),
            P("tp", ("grp", "sp")),
            P(("grp", "sp")),
            P(None, "tp"),
            P(None, "tp"),
            P(None, "tp"),
            P("tp"),
            P("tp", None),
            P(),
            P("sp", "tp"),
            P("sp", "tp"),
            P("sp", "tp"),
        ),
        out_specs=P(("grp", "sp"), "tp"),
        check_vma=False,
    )
```

```python
import functools

import jax
import jax.numpy as jnp
from jax import lax
from jax.experimental import pallas as pl
from jax.experimental.pallas import tpu as pltpu
from jax.sharding import PartitionSpec as P


BLOCK = 128
EDGE = 16
LANES = 128

norm_eps = 1e-06

F32 = jnp.float32
BF16 = jnp.bfloat16


def from_behind(value, axis, by):
    peers = lax.axis_size(axis)
    pairs = [(i, i + by) for i in range(peers) if 0 <= i + by < peers]
    return lax.ppermute(value, axis, pairs)


def silu(x):
    return x * jax.nn.sigmoid(x)


def shape(dims, kind):
    return jax.ShapeDtypeStruct(dims, kind)


def transposed(rows):
    return jnp.transpose(rows, (1, 0))


def doc_rows(docs_ref):
    return docs_ref[...].astype(F32)


def running_sum(x):
    lane = lax.broadcasted_iota(jnp.int32, x.shape, 1)
    shift = 1
    while shift < x.shape[1]:
        x = x + jnp.where(lane >= shift, pltpu.roll(x, shift, 1), 0.0)
        shift *= 2
    return x


def per_channel(columns, pair, rows):
    lane = lax.broadcasted_iota(jnp.int32, (rows, LANES), 1)
    return jnp.where(
        lane < LANES // 2,
        jnp.broadcast_to(columns[:, 2 * pair : 2 * pair + 1], (rows, LANES)),
        jnp.broadcast_to(columns[:, 2 * pair + 1 : 2 * pair + 2], (rows, LANES)),
    )


def place_docs(dext_ref, prior_ref, docs, blocks):
    dext_ref[0:EDGE] = prior_ref[...].astype(F32)
    padded = jnp.concatenate([docs, jnp.zeros((8 - blocks, BLOCK), F32)]) if blocks < 8 else docs
    columns = transposed(padded)
    for b in range(blocks):
        dext_ref[EDGE + b * BLOCK : EDGE + (b + 1) * BLOCK] = jnp.broadcast_to(
            columns[:, b : b + 1], (BLOCK, LANES)
        )


def short_filter(ext_ref, dext_ref, taps_ref, out_ref, blocks, width):
    taps = taps_ref[...].astype(F32)
    count = taps.shape[0]
    for b in range(blocks):
        first = EDGE + b * BLOCK
        own = dext_ref[first : first + BLOCK]
        masks = [
            dext_ref[first - count + 1 + k : first - count + 1 + k + BLOCK] == own
            for k in range(count - 1)
        ]
        for c in range(width // LANES):
            cols = slice(c * LANES, (c + 1) * LANES)
            total = None
            for k in range(count):
                start = first - count + 1 + k
                term = ext_ref[start : start + BLOCK, cols] * taps[k : k + 1, cols]
                if k < count - 1:
                    term = jnp.where(masks[k], term, 0.0)
                total = term if total is None else total + term
            out_ref[b * BLOCK : (b + 1) * BLOCK, cols] = silu(total).astype(BF16)


def pack_kernel(values_ref, writes_ref, reads_ref, docs_ref, out_ref):
    wide, narrow = values_ref.shape[1], writes_ref.shape[1]
    out_ref[:, 0:wide] = values_ref[...]
    out_ref[:, wide : wide + narrow] = writes_ref[...]
    out_ref[:, wide + narrow : wide + 2 * narrow] = reads_ref[...]
    blocks = docs_ref.shape[0]
    last = jnp.broadcast_to(doc_rows(docs_ref)[blocks - 1 :], (8, BLOCK))
    column = transposed(last)[BLOCK - EDGE :, 0:1]
    out_ref[:, wide + 2 * narrow :] = jnp.broadcast_to(column, (EDGE, LANES)).astype(BF16)


def pack_edge(values, writes, reads, docs):
    tokens, wide = values.shape
    narrow = writes.shape[1]
    at = tokens // EDGE - 1
    return pl.pallas_call(
        pack_kernel,
        grid=(1,),
        in_specs=[
            pl.BlockSpec((EDGE, wide), lambda i: (at, 0)),
            pl.BlockSpec((EDGE, narrow), lambda i: (at, 0)),
            pl.BlockSpec((EDGE, narrow), lambda i: (at, 0)),
            pl.BlockSpec(docs.shape, lambda i: (0, 0)),
        ],
        out_specs=pl.BlockSpec((EDGE, wide + 2 * narrow + LANES), lambda i: (0, 0)),
        out_shape=shape((EDGE, wide + 2 * narrow + LANES), BF16),
        name="pack_edge",
    )(values, writes, reads, docs)


def state_kernel(
    before_ref,
    values_ref,
    writes_ref,
    step_ref,
    rate_ref,
    jump_ref,
    docs_ref,
    taps_values_ref,
    taps_write_ref,
    sv_ref,
    sw_ref,
    run_ref,
    stepped_ref,
    enter_ref,
    send_ref,
    ext_ref,
    wext_ref,
    dext_ref,
):
    tokens, wide = values_ref.shape
    narrow = writes_ref.shape[1]
    blocks = tokens // BLOCK
    heads = step_ref.shape[0]
    docs = doc_rows(docs_ref)
    place_docs(dext_ref, before_ref.at[:, wide + 2 * narrow :], docs, blocks)
    ext_ref[0:EDGE] = before_ref[:, 0:wide].astype(F32)
    ext_ref[EDGE:] = values_ref[...].astype(F32)
    wext_ref[0:EDGE] = before_ref[:, wide : wide + narrow].astype(F32)
    wext_ref[EDGE:] = writes_ref[...].astype(F32)
    short_filter(wext_ref, dext_ref, taps_write_ref, sw_ref, blocks, narrow)
    short_filter(ext_ref, dext_ref, taps_values_ref, sv_ref, blocks, wide)

    raw = step_ref[...].astype(F32)
    step = jnp.maximum(raw, 0.0) + jnp.log1p(jnp.exp(-jnp.abs(raw)))
    stepped_ref[...] = step
    log_decay = jump_ref[...] - rate_ref[...] * step
    held = None
    total = jnp.zeros((heads, 1), F32)
    head_size = wide // heads
    for b in range(blocks):
        span = slice(b * BLOCK, (b + 1) * BLOCK)
        run = running_sum(log_decay[:, span])
        run_ref[:, span] = run
        last = run[:, BLOCK - 1 :]
        total = total + last
        row = docs[b : b + 1]
        end = row[:, BLOCK - 1 :]
        factor = jnp.where(row == end, jnp.exp(last - run) * step[:, span], 0.0)
        columns = transposed(factor)
        scaled = jnp.concatenate(
            [
                (
                    sv_ref[span, p * LANES : (p + 1) * LANES].astype(F32)
                    * per_channel(columns, p, BLOCK)
                ).astype(BF16)
                for p in range(wide // LANES)
            ],
            axis=1,
        )
        fresh = lax.dot_general(
            scaled, sw_ref[span], (((0,), (0,)), ((), ())), preferred_element_type=F32
        )
        if held is None:
            held = fresh
        else:
            enter_ref[b - 1] = held.astype(BF16)
            passing = jnp.where(docs[b - 1 : b, BLOCK - 1 :] == end, jnp.exp(last), 0.0)
            held = jnp.concatenate(
                [
                    held[h * head_size : (h + 1) * head_size] * passing[h : h + 1]
                    + fresh[h * head_size : (h + 1) * head_size]
                    for h in range(heads)
                ]
            )
    send_ref[0:wide] = held.astype(BF16)
    behind = before_ref[EDGE - 1 : EDGE, wide + 2 * narrow :].astype(F32)
    whole = jnp.where(
        behind == docs[blocks - 1 :, BLOCK - 1 :], jnp.broadcast_to(jnp.exp(total), (heads, LANES)), 0.0
    )
    send_ref[wide:] = jnp.concatenate([whole, jnp.zeros((16 - heads, LANES), F32)]).astype(BF16)


def local_states(before, values, writes, step_raw, rate, jump, docs, taps_values, taps_write):
    tokens, wide = values.shape
    narrow = writes.shape[1]
    heads = step_raw.shape[0]
    blocks = tokens // BLOCK
    return pl.pallas_call(
        state_kernel,
        out_shape=(
            shape((tokens, wide), BF16),
            shape((tokens, narrow), BF16),
            shape((heads, tokens), F32),
            shape((heads, tokens), F32),
            shape((blocks - 1, wide, narrow), BF16),
            shape((wide + 16, narrow), BF16),
        ),
        scratch_shapes=[
            pltpu.VMEM((EDGE + tokens, wide), F32),
            pltpu.VMEM((EDGE + tokens, narrow), F32),
            pltpu.VMEM((EDGE + tokens, LANES), F32),
        ],
        cost_estimate=pl.CostEstimate(flops=400_000_000, transcendentals=0, bytes_accessed=4_000_000),
        name="local_states",
    )(before, values, writes, step_raw, rate, jump, docs, taps_values, taps_write)


def decayed(near, decay, far, heads):
    size = near.shape[0] // heads
    return jnp.concatenate(
        [
            near[h * size : (h + 1) * size] + decay[h : h + 1] * far[h * size : (h + 1) * size]
            for h in range(heads)
        ]
    )


def join_kernel(heads, own_ref, near_ref, out_ref):
    wide = out_ref.shape[0]
    own = own_ref[0:wide].astype(F32)
    decay = own_ref[wide:].astype(F32)
    out_ref[...] = decayed(own, decay, near_ref[0:wide].astype(F32), heads).astype(BF16)


def join_states(own, near, heads):
    return pl.pallas_call(
        functools.partial(join_kernel, heads),
        out_shape=shape((own.shape[0] - 16, own.shape[1]), BF16),
        name="join_states",
    )(own, near)


def inner_kernel(
    before_ref,
    reads_ref,
    docs_ref,
    taps_ref,
    sv_ref,
    sw_ref,
    run_ref,
    step_ref,
    enter_ref,
    sr_ref,
    mixed_ref,
    reach_ref,
    ext_ref,
    dext_ref,
):
    tokens, narrow = reads_ref.shape
    wide = sv_ref.shape[1]
    blocks = tokens // BLOCK
    docs = doc_rows(docs_ref)
    place_docs(dext_ref, before_ref.at[:, wide + 2 * narrow :], docs, blocks)
    ext_ref[0:EDGE] = before_ref[:, wide + narrow : wide + 2 * narrow].astype(F32)
    ext_ref[EDGE:] = reads_ref[...].astype(F32)
    short_filter(ext_ref, dext_ref, taps_ref, sr_ref, blocks, narrow)
    target = lax.broadcasted_iota(jnp.int32, (BLOCK, BLOCK), 0)
    source = lax.broadcasted_iota(jnp.int32, (BLOCK, BLOCK), 1)
    low = source < LANES // 2
    gain = None
    for b in range(blocks):
        span = slice(b * BLOCK, (b + 1) * BLOCK)
        row = docs[b : b + 1]
        column = dext_ref[EDGE + b * BLOCK : EDGE + (b + 1) * BLOCK]
        allowed = (target >= source) & (column == row)
        reads, writes = sr_ref[span], sw_ref[span]
        scores = lax.dot_general(
            reads, writes, (((1,), (1,)), ((), ())), preferred_element_type=F32
        )
        run, step = run_ref[:, span], step_ref[:, span]
        run_columns = transposed(run)
        if b == 0:
            prior = before_ref[EDGE - 1 : EDGE, wide + 2 * narrow :].astype(F32)
        else:
            prior = jnp.broadcast_to(docs[b - 1 : b, BLOCK - 1 :], (1, BLOCK))
        reach = jnp.where(row == prior, jnp.exp(run), 0.0)
        last = run[:, BLOCK - 1 :]
        passing = jnp.where(row[:, BLOCK - 1 :] == prior[:, 0:1], jnp.exp(last), 0.0)
        reach_ref[:, span] = reach if gain is None else reach * gain
        gain = passing if gain is None else gain * passing
        reach_columns = transposed(reach)
        if b > 0:
            taken = lax.dot_general(
                reads, enter_ref[b - 1], (((1,), (1,)), ((), ())), preferred_element_type=F32
            )
        for p in range(wide // LANES):
            cols = slice(p * LANES, (p + 1) * LANES)
            weights = []
            for h in (2 * p, 2 * p + 1):
                spread = run_columns[:, h : h + 1] - run[h : h + 1]
                decay = jnp.exp(jnp.where(allowed, spread, -1e30))
                weights.append((decay * scores * step[h : h + 1]).astype(BF16))
            here = sv_ref[span, cols]
            zero = jnp.zeros_like(here)
            both = jnp.concatenate([jnp.where(low, here, zero), jnp.where(low, zero, here)])
            mixed = jnp.dot(
                jnp.concatenate(weights, axis=1), both, preferred_element_type=F32
            )
            if b > 0:
                mixed = mixed + taken[:, cols] * per_channel(reach_columns, p, BLOCK)
            mixed_ref[span, cols] = mixed


def local_mix(before, reads, docs, taps, sv, sw, run, step, enter):
    tokens, narrow = reads.shape
    wide = sv.shape[1]
    heads = step.shape[0]
    return pl.pallas_call(
        inner_kernel,
        out_shape=(
            shape((tokens, narrow), BF16),
            shape((tokens, wide), F32),
            shape((heads, tokens), F32),
        ),
        scratch_shapes=[
            pltpu.VMEM((EDGE + tokens, narrow), F32),
            pltpu.VMEM((EDGE + tokens, LANES), F32),
        ],
        cost_estimate=pl.CostEstimate(flops=800_000_000, transcendentals=0, bytes_accessed=4_000_000),
        name="local_mix",
    )(before, reads, docs, taps, sv, sw, run, step, enter)


def project_kernel(
    core_ref,
    near_ref,
    far_ref,
    sr_ref,
    mixed_ref,
    reach_ref,
    gate_ref,
    gain_ref,
    weight_ref,
    mine_ref,
    other_ref,
    in_ref,
):
    tokens, wide = mixed_ref.shape
    heads = reach_ref.shape[0]
    share = mine_ref.shape[2]
    near = near_ref[0:wide].astype(F32)
    decay = near_ref[wide:].astype(F32)
    held = decayed(near, decay, far_ref[...].astype(F32), heads).astype(BF16)
    for b in range(tokens // BLOCK):
        span = slice(b * BLOCK, (b + 1) * BLOCK)
        taken = lax.dot_general(
            sr_ref[span], held, (((1,), (1,)), ((), ())), preferred_element_type=F32
        )
        columns = transposed(reach_ref[:, span])
        parts, square = [], None
        for p in range(wide // LANES):
            cols = slice(p * LANES, (p + 1) * LANES)
            mixed = mixed_ref[span, cols] + taken[:, cols] * per_channel(columns, p, BLOCK)
            part = mixed * silu(gate_ref[span, cols].astype(F32))
            parts.append(part)
            square = part * part if square is None else square + part * part
        mean = jnp.sum(square, axis=1, keepdims=True) / wide
        scale = lax.rsqrt(mean + norm_eps)
        for p, part in enumerate(parts):
            cols = slice(p * LANES, (p + 1) * LANES)
            in_ref[span, cols] = (part * scale * gain_ref[:, cols].astype(F32)).astype(BF16)
    core = core_ref[0]
    rows = in_ref[...]
    for flip, out_ref in ((1, other_ref), (0, mine_ref)):
        for k in range(out_ref.shape[0]):
            c = 2 * k + (core ^ flip)
            cols = pl.ds(pl.multiple_of(c * share, share), share)
            out_ref[k] = jnp.dot(rows, weight_ref[:, cols], preferred_element_type=F32).astype(BF16)


def vmem():
    return pl.BlockSpec(memory_space=pltpu.VMEM)


def smem():
    return pl.BlockSpec(memory_space=pltpu.SMEM)


def project(core, near, far, sr, mixed, reach, gate, gain, weight, owners):
    tokens, wide = mixed.shape
    share = weight.shape[1] // (2 * owners)
    return pl.pallas_call(
        project_kernel,
        in_specs=[smem()] + [vmem()] * 8,
        out_shape=(shape((owners, tokens, share), BF16),) * 2,
        scratch_shapes=[pltpu.VMEM((tokens, wide), BF16)],
        cost_estimate=pl.CostEstimate(
            flops=2 * tokens * wide * weight.shape[1], transcendentals=0, bytes_accessed=6_000_000
        ),
        name="project",
    )(core, near, far, sr, mixed, reach, gate, gain, weight)


def after_kernel(at_ref, parts_ref, residual_ref, own_ref, out_ref):
    total = residual_ref[...].astype(F32)
    for k in range(parts_ref.shape[0]):
        total = total + parts_ref[k].astype(F32)
    after = total.astype(BF16)
    own_ref[...] = after
    for k in range(out_ref.shape[0]):
        out_ref[k] = after


def after_mix(at, parts, residual):
    owners, tokens, share = parts.shape
    return pl.pallas_call(
        after_kernel,
        grid_spec=pltpu.PrefetchScalarGridSpec(
            num_scalar_prefetch=1,
            grid=(1,),
            in_specs=[
                pl.BlockSpec((owners, tokens, share), lambda i, at: (0, 0, 0)),
                pl.BlockSpec((tokens, share), lambda i, at: (0, at[0])),
            ],
            out_specs=[
                pl.BlockSpec((tokens, share), lambda i, at: (0, 0)),
                pl.BlockSpec((owners, tokens, share), lambda i, at: (0, 0, 0)),
            ],
        ),
        out_shape=(shape((tokens, share), BF16), shape((owners, tokens, share), BF16)),
        name="after_mix",
    )(at, parts, residual)


def normal_kernel(at_ref, mine_ref, other_ref, gain_ref, out_ref):
    owners, _, share = mine_ref.shape
    core = lax.rem(at_ref[0], 2)
    square = None
    for ref in (mine_ref, other_ref):
        for k in range(owners):
            x = ref[k].astype(F32)
            square = x * x if square is None else square + x * x
    scale = lax.rsqrt(jnp.sum(square, axis=1, keepdims=True) / (2 * owners * share) + norm_eps)
    for flip, ref in enumerate((mine_ref, other_ref)):
        for k in range(owners):
            c = 2 * k + (core ^ flip)
            cols = pl.ds(pl.multiple_of(c * share, share), share)
            out_ref[:, cols] = (
                ref[k].astype(F32) * scale * gain_ref[:, cols].astype(F32)
            ).astype(BF16)


def normalised(at, mine, other, gain):
    owners, tokens, share = mine.shape
    return pl.pallas_call(
        normal_kernel,
        in_specs=[smem(), vmem(), vmem(), vmem()],
        out_shape=shape((tokens, 2 * owners * share), BF16),
        name="normalised",
    )(at, mine, other, gain)


def mixer_kernel(tiles, at_ref, normal_ref, weight_ref, *refs):
    mine_far, other_far, mine_near, other_near = refs[:4]
    late, downs, hidden_ref, far, near, late_sem, down_sem, far_sem, near_sem = refs[4:]
    peers, units, _ = downs.shape
    _, turns, _, _ = near.shape
    core, chip = lax.rem(at_ref[0], 2), lax.div(at_ref[0], 2)

    heavy = []
    for t, (first, count) in enumerate(tiles):
        heavy.append(
            [
                pltpu.make_async_copy(
                    weight_ref.at[:, pl.ds(base + first, count)],
                    late.at[:, pl.ds(base + first, count)],
                    late_sem.at[t, half],
                )
                for half, base in enumerate((0, units))
            ]
        )
    heavy.append([pltpu.make_async_copy(weight_ref.at[:, pl.ds(2 * units, units)], downs, down_sem)])
    for copy in (*heavy[0], *heavy[1]):
        copy.start()
    across = (((1,), (1,)), ((), ()))
    normal = normal_ref[...]
    for t, (first, count) in enumerate(tiles):
        for copy in heavy[t]:
            copy.wait()
        if t + 2 < len(heavy):
            for copy in heavy[t + 2]:
                copy.start()
        products = []
        for base in (first, units + first):
            part = jnp.concatenate([late[k, base : base + count] for k in range(peers)], axis=1)
            products.append(
                lax.dot_general(normal, part, across, preferred_element_type=F32)
            )
        hidden_ref[:, first : first + count] = (silu(products[0]) * products[1]).astype(BF16)
    heavy[-1][0].wait()
    hidden = hidden_ref[...]
    stores = []

    def store(source, target, sem):
        copy = pltpu.make_async_copy(source, target, sem)
        copy.start()
        stores.append(copy)

    for turn in (2, 0, 1, 3):
        for flip in (1, 0):
            c = 2 * lax.rem(chip + turn, turns + 1) + (core ^ flip)
            part = jnp.concatenate([downs[2 * c], downs[2 * c + 1]], axis=1)
            product = jnp.dot(hidden, part, preferred_element_type=F32).astype(BF16)
            if turn == 2:
                far[flip] = product
                store(far.at[flip], (mine_far, other_far)[flip], far_sem.at[flip])
            else:
                k = (0, 1, None, 2)[turn]
                near[flip, k] = product
                store(near.at[flip, k], (mine_near, other_near)[flip].at[k], near_sem.at[flip, k])
    for copy in stores:
        copy.wait()


def channel_mixer(at, normal, weights, share):
    tokens = normal.shape[0]
    peers, units, depth = weights.shape[0], weights.shape[1] // 3, weights.shape[2]
    turns = normal.shape[1] // (2 * share) - 1
    tiles = [(f, min(256, units - f)) for f in range(0, units, 256)]
    anywhere = pl.BlockSpec(memory_space=pl.ANY)
    far, near = shape((tokens, share), BF16), shape((turns, tokens, share), BF16)
    return pl.pallas_call(
        functools.partial(mixer_kernel, tiles),
        in_specs=[smem(), vmem(), anywhere],
        out_specs=[anywhere] * 4,
        out_shape=(far, far, near, near),
        scratch_shapes=[
            pltpu.VMEM((peers, 2 * units, depth), BF16),
            pltpu.VMEM((peers, units, depth), BF16),
            pltpu.VMEM((tokens, units), BF16),
            pltpu.VMEM((2, tokens, share), BF16),
            pltpu.VMEM((2, turns, tokens, share), BF16),
            pltpu.SemaphoreType.DMA((len(tiles), 2)),
            pltpu.SemaphoreType.DMA,
            pltpu.SemaphoreType.DMA((2,)),
            pltpu.SemaphoreType.DMA((2, turns)),
        ],
        cost_estimate=pl.CostEstimate(
            flops=6 * tokens * normal.shape[1] * units, transcendentals=0, bytes_accessed=14_000_000
        ),
        name="channel_mixer",
    )(at, normal, weights)


def to_partner(value):
    return lax.ppermute(value, "tp", [(i, i ^ 1) for i in range(lax.axis_size("tp"))])


def to_chip(value, by):
    peers = lax.axis_size("tp")
    return lax.ppermute(value, "tp", [(i, (i + 2 * by) % peers) for i in range(peers)])


def sum_round(parts, after):
    mine_far, other_far, mine_near, other_near = parts
    other_far = to_partner(other_far)
    other_near = to_partner(other_near)
    half = mine_far.shape[0] // 2
    far = mine_far.astype(F32) + other_far.astype(F32)
    low = to_chip(far[:half].astype(BF16), 1)
    high = to_chip(far[half:].astype(BF16), -1)
    near = mine_near.astype(F32) + other_near.astype(F32)
    low = jnp.pad(low, ((0, half), (0, 0))).astype(F32)
    high = jnp.pad(high, ((half, 0), (0, 0))).astype(F32)
    right = to_chip((near[1] + low).astype(BF16), 1)
    left = to_chip((near[2] + high).astype(BF16), -1)
    down = near[0] + right.astype(F32) + left.astype(F32)
    return (after.astype(F32) + down).astype(BF16)


def exchange(value):
    peers = lax.axis_size("tp")
    rows = [[i for i in range(peers) if i % 2 == core] for core in range(2)]
    return lax.all_to_all(value, "tp", 0, 0, axis_index_groups=rows, tiled=True)


def sum_pairs(both):
    return (both[0].astype(F32) + to_partner(both[1]).astype(F32)).astype(BF16)


def on_device(
    residual,
    values,
    out_gate,
    writes,
    reads,
    step_raw,
    decay_rate,
    decay_jump,
    documents,
    taps_values,
    taps_write,
    taps_read,
    mixer_gain,
    mixer_out,
    channel_gain,
    gate_weight,
    up_weight,
    down_rows,
):
    heads = step_raw.shape[0]
    owners = lax.axis_size("tp") // 2
    me = lax.axis_index("tp").astype(jnp.int32)
    at = me.reshape(1)
    core = (me % 2).reshape(1)
    late = jnp.concatenate([gate_weight.T, up_weight.T, down_rows.T], axis=0)
    weights = lax.all_gather(late, "sp", axis=0)

    docs = documents.reshape(-1, BLOCK)
    before = from_behind(pack_edge(values, writes, reads, docs), "sp", 1)
    rate = decay_rate.reshape(-1, 1)
    sv, sw, run, step, enter, send = local_states(
        before, values, writes, step_raw, rate, decay_jump, docs, taps_values, taps_write
    )
    near = from_behind(send, "sp", 1)
    sr, mixed, reach = local_mix(before, reads, docs, taps_read, sv, sw, run, step, enter)
    far = from_behind(join_states(send, near, heads), "sp", 2)
    both = project(
        core, near, far, sr, mixed, reach, out_gate, mixer_gain.reshape(1, -1), mixer_out, owners
    )
    own_after, spread = after_mix(at, exchange(sum_pairs(both)), residual)
    mine = exchange(spread)
    other = to_partner(mine)
    normal = normalised(at, mine, other, channel_gain.reshape(1, -1))
    return sum_round(channel_mixer(at, normal, weights, own_after.shape[1]), own_after)


def solution(mesh):
    return jax.shard_map(
        on_device,
        mesh=mesh,
        in_specs=(
            P(("grp", "sp"), None),
            P(("grp", "sp"), "tp"),
            P(("grp", "sp"), "tp"),
            P(("grp", "sp"), "tp"),
            P(("grp", "sp"), "tp"),
            P("tp", ("grp", "sp")),
            P("tp"),
            P("tp", ("grp", "sp")),
            P(("grp", "sp")),
            P(None, "tp"),
            P(None, "tp"),
            P(None, "tp"),
            P("tp"),
            P("tp", None),
            P(),
            P("sp", "tp"),
            P("sp", "tp"),
            P("sp", "tp"),
        ),
        out_specs=P(("grp", "sp"), "tp"),
        check_vma=False,
    )
```

```python
import functools

import jax
import jax.numpy as jnp
from jax import lax
from jax.experimental import pallas as pl
from jax.experimental.pallas import tpu as pltpu
from jax.sharding import PartitionSpec as P


BLOCK = 128
EDGE = 16
LANES = 128

norm_eps = 1e-06

F32 = jnp.float32
BF16 = jnp.bfloat16


def from_behind(value, axis, by):
    peers = lax.axis_size(axis)
    pairs = [(i, i + by) for i in range(peers) if 0 <= i + by < peers]
    return lax.ppermute(value, axis, pairs)


def silu(x):
    return x * jax.nn.sigmoid(x)


def shape(dims, kind):
    return jax.ShapeDtypeStruct(dims, kind)


def transposed(rows):
    return jnp.transpose(rows, (1, 0))


def doc_rows(docs_ref):
    return docs_ref[...].astype(F32)


def running_sum(x):
    lane = lax.broadcasted_iota(jnp.int32, x.shape, 1)
    shift = 1
    while shift < x.shape[1]:
        x = x + jnp.where(lane >= shift, pltpu.roll(x, shift, 1), 0.0)
        shift *= 2
    return x


def per_channel(columns, pair, rows):
    lane = lax.broadcasted_iota(jnp.int32, (rows, LANES), 1)
    return jnp.where(
        lane < LANES // 2,
        jnp.broadcast_to(columns[:, 2 * pair : 2 * pair + 1], (rows, LANES)),
        jnp.broadcast_to(columns[:, 2 * pair + 1 : 2 * pair + 2], (rows, LANES)),
    )


def place_docs(dext_ref, prior_ref, docs, blocks):
    dext_ref[0:EDGE] = prior_ref[...].astype(F32)
    padded = jnp.concatenate([docs, jnp.zeros((8 - blocks, BLOCK), F32)]) if blocks < 8 else docs
    columns = transposed(padded)
    for b in range(blocks):
        dext_ref[EDGE + b * BLOCK : EDGE + (b + 1) * BLOCK] = jnp.broadcast_to(
            columns[:, b : b + 1], (BLOCK, LANES)
        )


def short_filter(ext_ref, dext_ref, taps_ref, out_ref, blocks, width):
    taps = taps_ref[...].astype(F32)
    count = taps.shape[0]
    for b in range(blocks):
        first = EDGE + b * BLOCK
        own = dext_ref[first : first + BLOCK]
        masks = [
            dext_ref[first - count + 1 + k : first - count + 1 + k + BLOCK] == own
            for k in range(count - 1)
        ]
        for c in range(width // LANES):
            cols = slice(c * LANES, (c + 1) * LANES)
            total = None
            for k in range(count):
                start = first - count + 1 + k
                term = ext_ref[start : start + BLOCK, cols] * taps[k : k + 1, cols]
                if k < count - 1:
                    term = jnp.where(masks[k], term, 0.0)
                total = term if total is None else total + term
            out_ref[b * BLOCK : (b + 1) * BLOCK, cols] = silu(total).astype(BF16)


def pack_kernel(values_ref, writes_ref, reads_ref, docs_ref, out_ref):
    wide, narrow = values_ref.shape[1], writes_ref.shape[1]
    out_ref[:, 0:wide] = values_ref[...]
    out_ref[:, wide : wide + narrow] = writes_ref[...]
    out_ref[:, wide + narrow : wide + 2 * narrow] = reads_ref[...]
    blocks = docs_ref.shape[0]
    last = jnp.broadcast_to(doc_rows(docs_ref)[blocks - 1 :], (8, BLOCK))
    column = transposed(last)[BLOCK - EDGE :, 0:1]
    out_ref[:, wide + 2 * narrow :] = jnp.broadcast_to(column, (EDGE, LANES)).astype(BF16)


def pack_edge(values, writes, reads, docs):
    tokens, wide = values.shape
    narrow = writes.shape[1]
    at = tokens // EDGE - 1
    return pl.pallas_call(
        pack_kernel,
        grid=(1,),
        in_specs=[
            pl.BlockSpec((EDGE, wide), lambda i: (at, 0)),
            pl.BlockSpec((EDGE, narrow), lambda i: (at, 0)),
            pl.BlockSpec((EDGE, narrow), lambda i: (at, 0)),
            pl.BlockSpec(docs.shape, lambda i: (0, 0)),
        ],
        out_specs=pl.BlockSpec((EDGE, wide + 2 * narrow + LANES), lambda i: (0, 0)),
        out_shape=shape((EDGE, wide + 2 * narrow + LANES), BF16),
        name="pack_edge",
    )(values, writes, reads, docs)


def state_kernel(
    before_ref,
    values_ref,
    writes_ref,
    step_ref,
    rate_ref,
    jump_ref,
    docs_ref,
    taps_values_ref,
    taps_write_ref,
    sv_ref,
    sw_ref,
    run_ref,
    stepped_ref,
    enter_ref,
    send_ref,
    ext_ref,
    wext_ref,
    dext_ref,
):
    tokens, wide = values_ref.shape
    narrow = writes_ref.shape[1]
    blocks = tokens // BLOCK
    heads = step_ref.shape[0]
    docs = doc_rows(docs_ref)
    place_docs(dext_ref, before_ref.at[:, wide + 2 * narrow :], docs, blocks)
    ext_ref[0:EDGE] = before_ref[:, 0:wide].astype(F32)
    ext_ref[EDGE:] = values_ref[...].astype(F32)
    wext_ref[0:EDGE] = before_ref[:, wide : wide + narrow].astype(F32)
    wext_ref[EDGE:] = writes_ref[...].astype(F32)
    short_filter(wext_ref, dext_ref, taps_write_ref, sw_ref, blocks, narrow)
    short_filter(ext_ref, dext_ref, taps_values_ref, sv_ref, blocks, wide)

    raw = step_ref[...].astype(F32)
    step = jnp.maximum(raw, 0.0) + jnp.log1p(jnp.exp(-jnp.abs(raw)))
    stepped_ref[...] = step
    log_decay = jump_ref[...] - rate_ref[...] * step
    held = None
    total = jnp.zeros((heads, 1), F32)
    head_size = wide // heads
    for b in range(blocks):
        span = slice(b * BLOCK, (b + 1) * BLOCK)
        run = running_sum(log_decay[:, span])
        run_ref[:, span] = run
        last = run[:, BLOCK - 1 :]
        total = total + last
        row = docs[b : b + 1]
        end = row[:, BLOCK - 1 :]
        factor = jnp.where(row == end, jnp.exp(last - run) * step[:, span], 0.0)
        columns = transposed(factor)
        scaled = jnp.concatenate(
            [
                (
                    sv_ref[span, p * LANES : (p + 1) * LANES].astype(F32)
                    * per_channel(columns, p, BLOCK)
                ).astype(BF16)
                for p in range(wide // LANES)
            ],
            axis=1,
        )
        fresh = lax.dot_general(
            scaled, sw_ref[span], (((0,), (0,)), ((), ())), preferred_element_type=F32
        )
        if held is None:
            held = fresh
        else:
            enter_ref[b - 1] = held.astype(BF16)
            passing = jnp.where(docs[b - 1 : b, BLOCK - 1 :] == end, jnp.exp(last), 0.0)
            held = jnp.concatenate(
                [
                    held[h * head_size : (h + 1) * head_size] * passing[h : h + 1]
                    + fresh[h * head_size : (h + 1) * head_size]
                    for h in range(heads)
                ]
            )
    send_ref[0:wide] = held.astype(BF16)
    behind = before_ref[EDGE - 1 : EDGE, wide + 2 * narrow :].astype(F32)
    whole = jnp.where(
        behind == docs[blocks - 1 :, BLOCK - 1 :], jnp.broadcast_to(jnp.exp(total), (heads, LANES)), 0.0
    )
    send_ref[wide:] = jnp.concatenate([whole, jnp.zeros((16 - heads, LANES), F32)]).astype(BF16)


def local_states(before, values, writes, step_raw, rate, jump, docs, taps_values, taps_write):
    tokens, wide = values.shape
    narrow = writes.shape[1]
    heads = step_raw.shape[0]
    blocks = tokens // BLOCK
    return pl.pallas_call(
        state_kernel,
        out_shape=(
            shape((tokens, wide), BF16),
            shape((tokens, narrow), BF16),
            shape((heads, tokens), F32),
            shape((heads, tokens), F32),
            shape((blocks - 1, wide, narrow), BF16),
            shape((wide + 16, narrow), BF16),
        ),
        scratch_shapes=[
            pltpu.VMEM((EDGE + tokens, wide), F32),
            pltpu.VMEM((EDGE + tokens, narrow), F32),
            pltpu.VMEM((EDGE + tokens, LANES), F32),
        ],
        cost_estimate=pl.CostEstimate(flops=400_000_000, transcendentals=0, bytes_accessed=4_000_000),
        name="local_states",
    )(before, values, writes, step_raw, rate, jump, docs, taps_values, taps_write)


def decayed(near, decay, far, heads):
    size = near.shape[0] // heads
    return jnp.concatenate(
        [
            near[h * size : (h + 1) * size] + decay[h : h + 1] * far[h * size : (h + 1) * size]
            for h in range(heads)
        ]
    )


def join_kernel(heads, own_ref, near_ref, out_ref):
    wide = out_ref.shape[0]
    own = own_ref[0:wide].astype(F32)
    decay = own_ref[wide:].astype(F32)
    out_ref[...] = decayed(own, decay, near_ref[0:wide].astype(F32), heads).astype(BF16)


def join_states(own, near, heads):
    return pl.pallas_call(
        functools.partial(join_kernel, heads),
        out_shape=shape((own.shape[0] - 16, own.shape[1]), BF16),
        name="join_states",
    )(own, near)


def inner_kernel(
    before_ref,
    reads_ref,
    docs_ref,
    taps_ref,
    sv_ref,
    sw_ref,
    run_ref,
    step_ref,
    enter_ref,
    sr_ref,
    mixed_ref,
    reach_ref,
    ext_ref,
    dext_ref,
):
    tokens, narrow = reads_ref.shape
    wide = sv_ref.shape[1]
    blocks = tokens // BLOCK
    docs = doc_rows(docs_ref)
    place_docs(dext_ref, before_ref.at[:, wide + 2 * narrow :], docs, blocks)
    ext_ref[0:EDGE] = before_ref[:, wide + narrow : wide + 2 * narrow].astype(F32)
    ext_ref[EDGE:] = reads_ref[...].astype(F32)
    short_filter(ext_ref, dext_ref, taps_ref, sr_ref, blocks, narrow)
    target = lax.broadcasted_iota(jnp.int32, (BLOCK, BLOCK), 0)
    source = lax.broadcasted_iota(jnp.int32, (BLOCK, BLOCK), 1)
    low = source < LANES // 2
    gain = None
    for b in range(blocks):
        span = slice(b * BLOCK, (b + 1) * BLOCK)
        row = docs[b : b + 1]
        column = dext_ref[EDGE + b * BLOCK : EDGE + (b + 1) * BLOCK]
        allowed = (target >= source) & (column == row)
        reads, writes = sr_ref[span], sw_ref[span]
        scores = lax.dot_general(
            reads, writes, (((1,), (1,)), ((), ())), preferred_element_type=F32
        )
        run, step = run_ref[:, span], step_ref[:, span]
        run_columns = transposed(run)
        if b == 0:
            prior = before_ref[EDGE - 1 : EDGE, wide + 2 * narrow :].astype(F32)
        else:
            prior = jnp.broadcast_to(docs[b - 1 : b, BLOCK - 1 :], (1, BLOCK))
        reach = jnp.where(row == prior, jnp.exp(run), 0.0)
        last = run[:, BLOCK - 1 :]
        passing = jnp.where(row[:, BLOCK - 1 :] == prior[:, 0:1], jnp.exp(last), 0.0)
        reach_ref[:, span] = reach if gain is None else reach * gain
        gain = passing if gain is None else gain * passing
        reach_columns = transposed(reach)
        if b > 0:
            taken = lax.dot_general(
                reads, enter_ref[b - 1], (((1,), (1,)), ((), ())), preferred_element_type=F32
            )
        for p in range(wide // LANES):
            cols = slice(p * LANES, (p + 1) * LANES)
            weights = []
            for h in (2 * p, 2 * p + 1):
                spread = run_columns[:, h : h + 1] - run[h : h + 1]
                decay = jnp.exp(jnp.where(allowed, spread, -1e30))
                weights.append((decay * scores * step[h : h + 1]).astype(BF16))
            here = sv_ref[span, cols]
            zero = jnp.zeros_like(here)
            both = jnp.concatenate([jnp.where(low, here, zero), jnp.where(low, zero, here)])
            mixed = jnp.dot(
                jnp.concatenate(weights, axis=1), both, preferred_element_type=F32
            )
            if b > 0:
                mixed = mixed + taken[:, cols] * per_channel(reach_columns, p, BLOCK)
            mixed_ref[span, cols] = mixed


def local_mix(before, reads, docs, taps, sv, sw, run, step, enter):
    tokens, narrow = reads.shape
    wide = sv.shape[1]
    heads = step.shape[0]
    return pl.pallas_call(
        inner_kernel,
        out_shape=(
            shape((tokens, narrow), BF16),
            shape((tokens, wide), F32),
            shape((heads, tokens), F32),
        ),
        scratch_shapes=[
            pltpu.VMEM((EDGE + tokens, narrow), F32),
            pltpu.VMEM((EDGE + tokens, LANES), F32),
        ],
        cost_estimate=pl.CostEstimate(flops=800_000_000, transcendentals=0, bytes_accessed=4_000_000),
        name="local_mix",
    )(before, reads, docs, taps, sv, sw, run, step, enter)


def project_kernel(
    core_ref,
    near_ref,
    far_ref,
    sr_ref,
    mixed_ref,
    reach_ref,
    gate_ref,
    gain_ref,
    weight_ref,
    mine_ref,
    other_ref,
    in_ref,
):
    tokens, wide = mixed_ref.shape
    heads = reach_ref.shape[0]
    share = mine_ref.shape[2]
    near = near_ref[0:wide].astype(F32)
    decay = near_ref[wide:].astype(F32)
    held = decayed(near, decay, far_ref[...].astype(F32), heads).astype(BF16)
    for b in range(tokens // BLOCK):
        span = slice(b * BLOCK, (b + 1) * BLOCK)
        taken = lax.dot_general(
            sr_ref[span], held, (((1,), (1,)), ((), ())), preferred_element_type=F32
        )
        columns = transposed(reach_ref[:, span])
        parts, square = [], None
        for p in range(wide // LANES):
            cols = slice(p * LANES, (p + 1) * LANES)
            mixed = mixed_ref[span, cols] + taken[:, cols] * per_channel(columns, p, BLOCK)
            part = mixed * silu(gate_ref[span, cols].astype(F32))
            parts.append(part)
            square = part * part if square is None else square + part * part
        mean = jnp.sum(square, axis=1, keepdims=True) / wide
        scale = lax.rsqrt(mean + norm_eps)
        for p, part in enumerate(parts):
            cols = slice(p * LANES, (p + 1) * LANES)
            in_ref[span, cols] = (part * scale * gain_ref[:, cols].astype(F32)).astype(BF16)
    core = core_ref[0]
    rows = in_ref[...]
    for flip, out_ref in ((1, other_ref), (0, mine_ref)):
        for k in range(out_ref.shape[0]):
            c = 2 * k + (core ^ flip)
            cols = pl.ds(pl.multiple_of(c * share, share), share)
            out_ref[k] = jnp.dot(rows, weight_ref[:, cols], preferred_element_type=F32).astype(BF16)


def vmem():
    return pl.BlockSpec(memory_space=pltpu.VMEM)


def smem():
    return pl.BlockSpec(memory_space=pltpu.SMEM)


def project(core, near, far, sr, mixed, reach, gate, gain, weight, owners):
    tokens, wide = mixed.shape
    share = weight.shape[1] // (2 * owners)
    return pl.pallas_call(
        project_kernel,
        in_specs=[smem()] + [vmem()] * 8,
        out_shape=(shape((owners, tokens, share), BF16),) * 2,
        scratch_shapes=[pltpu.VMEM((tokens, wide), BF16)],
        cost_estimate=pl.CostEstimate(
            flops=2 * tokens * wide * weight.shape[1], transcendentals=0, bytes_accessed=6_000_000
        ),
        name="project",
    )(core, near, far, sr, mixed, reach, gate, gain, weight)


def after_kernel(at_ref, parts_ref, residual_ref, own_ref, out_ref):
    total = residual_ref[...].astype(F32)
    for k in range(parts_ref.shape[0]):
        total = total + parts_ref[k].astype(F32)
    after = total.astype(BF16)
    own_ref[...] = after
    for k in range(out_ref.shape[0]):
        out_ref[k] = after


def after_mix(at, parts, residual):
    owners, tokens, share = parts.shape
    return pl.pallas_call(
        after_kernel,
        grid_spec=pltpu.PrefetchScalarGridSpec(
            num_scalar_prefetch=1,
            grid=(1,),
            in_specs=[
                pl.BlockSpec((owners, tokens, share), lambda i, at: (0, 0, 0)),
                pl.BlockSpec((tokens, share), lambda i, at: (0, at[0])),
            ],
            out_specs=[
                pl.BlockSpec((tokens, share), lambda i, at: (0, 0)),
                pl.BlockSpec((owners, tokens, share), lambda i, at: (0, 0, 0)),
            ],
        ),
        out_shape=(shape((tokens, share), BF16), shape((owners, tokens, share), BF16)),
        name="after_mix",
    )(at, parts, residual)


def normal_kernel(at_ref, mine_ref, other_ref, gain_ref, out_ref):
    owners, _, share = mine_ref.shape
    core = lax.rem(at_ref[0], 2)
    square = None
    for ref in (mine_ref, other_ref):
        for k in range(owners):
            x = ref[k].astype(F32)
            square = x * x if square is None else square + x * x
    scale = lax.rsqrt(jnp.sum(square, axis=1, keepdims=True) / (2 * owners * share) + norm_eps)
    for flip, ref in enumerate((mine_ref, other_ref)):
        for k in range(owners):
            c = 2 * k + (core ^ flip)
            cols = pl.ds(pl.multiple_of(c * share, share), share)
            out_ref[:, cols] = (
                ref[k].astype(F32) * scale * gain_ref[:, cols].astype(F32)
            ).astype(BF16)


def normalised(at, mine, other, gain):
    owners, tokens, share = mine.shape
    return pl.pallas_call(
        normal_kernel,
        in_specs=[smem(), vmem(), vmem(), vmem()],
        out_shape=shape((tokens, 2 * owners * share), BF16),
        name="normalised",
    )(at, mine, other, gain)


def mixer_kernel(tiles, at_ref, normal_ref, weight_ref, *refs):
    mine_far, other_far, mine_near, other_near = refs[:4]
    late, downs, hidden_ref, far, near, late_sem, down_sem, far_sem, near_sem = refs[4:]
    peers, units, _ = downs.shape
    _, turns, _, _ = near.shape
    core, chip = lax.rem(at_ref[0], 2), lax.div(at_ref[0], 2)

    heavy = []
    for t, (first, count) in enumerate(tiles):
        heavy.append(
            [
                pltpu.make_async_copy(
                    weight_ref.at[:, pl.ds(base + first, count)],
                    late.at[:, pl.ds(base + first, count)],
                    late_sem.at[t, half],
                )
                for half, base in enumerate((0, units))
            ]
        )
    heavy.append([pltpu.make_async_copy(weight_ref.at[:, pl.ds(2 * units, units)], downs, down_sem)])
    for copy in (*heavy[0], *heavy[1]):
        copy.start()
    across = (((1,), (1,)), ((), ()))
    normal = normal_ref[...]
    for t, (first, count) in enumerate(tiles):
        for copy in heavy[t]:
            copy.wait()
        if t + 2 < len(heavy):
            for copy in heavy[t + 2]:
                copy.start()
        products = []
        for base in (first, units + first):
            part = jnp.concatenate([late[k, base : base + count] for k in range(peers)], axis=1)
            products.append(
                lax.dot_general(normal, part, across, preferred_element_type=F32)
            )
        hidden_ref[:, first : first + count] = (silu(products[0]) * products[1]).astype(BF16)
    heavy[-1][0].wait()
    hidden = hidden_ref[...]
    stores = []

    def store(source, target, sem):
        copy = pltpu.make_async_copy(source, target, sem)
        copy.start()
        stores.append(copy)

    for turn in (2, 0, 1, 3):
        for flip in (1, 0):
            c = 2 * lax.rem(chip + turn, turns + 1) + (core ^ flip)
            part = jnp.concatenate([downs[2 * c], downs[2 * c + 1]], axis=1)
            product = jnp.dot(hidden, part, preferred_element_type=F32).astype(BF16)
            if turn == 2:
                far[flip] = product
                store(far.at[flip], (mine_far, other_far)[flip], far_sem.at[flip])
            else:
                k = (0, 1, None, 2)[turn]
                near[flip, k] = product
                store(near.at[flip, k], (mine_near, other_near)[flip].at[k], near_sem.at[flip, k])
    for copy in stores:
        copy.wait()


def channel_mixer(at, normal, weights, share):
    tokens = normal.shape[0]
    peers, units, depth = weights.shape[0], weights.shape[1] // 3, weights.shape[2]
    turns = normal.shape[1] // (2 * share) - 1
    tiles = [(f, min(256, units - f)) for f in range(0, units, 256)]
    anywhere = pl.BlockSpec(memory_space=pl.ANY)
    far, near = shape((tokens, share), BF16), shape((turns, tokens, share), BF16)
    return pl.pallas_call(
        functools.partial(mixer_kernel, tiles),
        in_specs=[smem(), vmem(), anywhere],
        out_specs=[anywhere] * 4,
        out_shape=(far, far, near, near),
        scratch_shapes=[
            pltpu.VMEM((peers, 2 * units, depth), BF16),
            pltpu.VMEM((peers, units, depth), BF16),
            pltpu.VMEM((tokens, units), BF16),
            pltpu.VMEM((2, tokens, share), BF16),
            pltpu.VMEM((2, turns, tokens, share), BF16),
            pltpu.SemaphoreType.DMA((len(tiles), 2)),
            pltpu.SemaphoreType.DMA,
            pltpu.SemaphoreType.DMA((2,)),
            pltpu.SemaphoreType.DMA((2, turns)),
        ],
        cost_estimate=pl.CostEstimate(
            flops=6 * tokens * normal.shape[1] * units, transcendentals=0, bytes_accessed=14_000_000
        ),
        name="channel_mixer",
    )(at, normal, weights)


def to_partner(value):
    return lax.ppermute(value, "tp", [(i, i ^ 1) for i in range(lax.axis_size("tp"))])


def to_chip(value, by):
    peers = lax.axis_size("tp")
    return lax.ppermute(value, "tp", [(i, (i + 2 * by) % peers) for i in range(peers)])


def sum_round(parts, after):
    mine_far, other_far, mine_near, other_near = parts
    other_far = to_partner(other_far)
    other_near = to_partner(other_near)
    half = mine_far.shape[0] // 2
    far = mine_far.astype(F32) + other_far.astype(F32)
    low = to_chip(far[:half].astype(BF16), 1).astype(F32)
    high = to_chip(far[half:].astype(BF16), -1).astype(F32)
    near = mine_near.astype(F32) + other_near.astype(F32)
    right_high = to_chip(near[1, half:].astype(BF16), 1)
    left_low = to_chip(near[2, :half].astype(BF16), -1)
    right_low = to_chip((near[1, :half] + low).astype(BF16), 1)
    left_high = to_chip((near[2, half:] + high).astype(BF16), -1)
    down = near[0]
    for part, place in (
        (right_low, (0, half)),
        (left_low, (0, half)),
        (right_high, (half, 0)),
        (left_high, (half, 0)),
    ):
        down = down + jnp.pad(part, (place, (0, 0))).astype(F32)
    return (after.astype(F32) + down).astype(BF16)


def exchange(value):
    peers = lax.axis_size("tp")
    rows = [[i for i in range(peers) if i % 2 == core] for core in range(2)]
    return lax.all_to_all(value, "tp", 0, 0, axis_index_groups=rows, tiled=True)


def sum_pairs(both):
    return (both[0].astype(F32) + to_partner(both[1]).astype(F32)).astype(BF16)


def on_device(
    residual,
    values,
    out_gate,
    writes,
    reads,
    step_raw,
    decay_rate,
    decay_jump,
    documents,
    taps_values,
    taps_write,
    taps_read,
    mixer_gain,
    mixer_out,
    channel_gain,
    gate_weight,
    up_weight,
    down_rows,
):
    heads = step_raw.shape[0]
    owners = lax.axis_size("tp") // 2
    me = lax.axis_index("tp").astype(jnp.int32)
    at = me.reshape(1)
    core = (me % 2).reshape(1)
    late = jnp.concatenate([gate_weight.T, up_weight.T, down_rows.T], axis=0)
    weights = lax.all_gather(late, "sp", axis=0)

    docs = documents.reshape(-1, BLOCK)
    before = from_behind(pack_edge(values, writes, reads, docs), "sp", 1)
    rate = decay_rate.reshape(-1, 1)
    sv, sw, run, step, enter, send = local_states(
        before, values, writes, step_raw, rate, decay_jump, docs, taps_values, taps_write
    )
    near = from_behind(send, "sp", 1)
    sr, mixed, reach = local_mix(before, reads, docs, taps_read, sv, sw, run, step, enter)
    far = from_behind(join_states(send, near, heads), "sp", 2)
    both = project(
        core, near, far, sr, mixed, reach, out_gate, mixer_gain.reshape(1, -1), mixer_out, owners
    )
    own_after, spread = after_mix(at, exchange(sum_pairs(both)), residual)
    mine = exchange(spread)
    other = to_partner(mine)
    normal = normalised(at, mine, other, channel_gain.reshape(1, -1))
    return sum_round(channel_mixer(at, normal, weights, own_after.shape[1]), own_after)


def solution(mesh):
    return jax.shard_map(
        on_device,
        mesh=mesh,
        in_specs=(
            P(("grp", "sp"), None),
            P(("grp", "sp"), "tp"),
            P(("grp", "sp"), "tp"),
            P(("grp", "sp"), "tp"),
            P(("grp", "sp"), "tp"),
            P("tp", ("grp", "sp")),
            P("tp"),
            P("tp", ("grp", "sp")),
            P(("grp", "sp")),
            P(None, "tp"),
            P(None, "tp"),
            P(None, "tp"),
            P("tp"),
            P("tp", None),
            P(),
            P("sp", "tp"),
            P("sp", "tp"),
            P("sp", "tp"),
        ),
        out_specs=P(("grp", "sp"), "tp"),
        check_vma=False,
    )
```

```python
import functools

import jax
import jax.numpy as jnp
from jax import lax
from jax.experimental import pallas as pl
from jax.experimental.pallas import tpu as pltpu
from jax.sharding import PartitionSpec as P


BLOCK = 128
EDGE = 16
LANES = 128

norm_eps = 1e-06

F32 = jnp.float32
BF16 = jnp.bfloat16


def from_behind(value, axis, by):
    peers = lax.axis_size(axis)
    pairs = [(i, i + by) for i in range(peers) if 0 <= i + by < peers]
    return lax.ppermute(value, axis, pairs)


def silu(x):
    return x * jax.nn.sigmoid(x)


def shape(dims, kind):
    return jax.ShapeDtypeStruct(dims, kind)


def transposed(rows):
    return jnp.transpose(rows, (1, 0))


def doc_rows(docs_ref):
    return docs_ref[...].astype(F32)


def running_sum(x):
    lane = lax.broadcasted_iota(jnp.int32, x.shape, 1)
    shift = 1
    while shift < x.shape[1]:
        x = x + jnp.where(lane >= shift, pltpu.roll(x, shift, 1), 0.0)
        shift *= 2
    return x


def per_channel(columns, pair, rows):
    lane = lax.broadcasted_iota(jnp.int32, (rows, LANES), 1)
    return jnp.where(
        lane < LANES // 2,
        jnp.broadcast_to(columns[:, 2 * pair : 2 * pair + 1], (rows, LANES)),
        jnp.broadcast_to(columns[:, 2 * pair + 1 : 2 * pair + 2], (rows, LANES)),
    )


def place_docs(dext_ref, prior_ref, docs, blocks):
    dext_ref[0:EDGE] = prior_ref[...].astype(F32)
    padded = jnp.concatenate([docs, jnp.zeros((8 - blocks, BLOCK), F32)]) if blocks < 8 else docs
    columns = transposed(padded)
    for b in range(blocks):
        dext_ref[EDGE + b * BLOCK : EDGE + (b + 1) * BLOCK] = jnp.broadcast_to(
            columns[:, b : b + 1], (BLOCK, LANES)
        )


def short_filter(ext_ref, dext_ref, taps_ref, out_ref, blocks, width):
    taps = taps_ref[...].astype(F32)
    count = taps.shape[0]
    for b in range(blocks):
        first = EDGE + b * BLOCK
        own = dext_ref[first : first + BLOCK]
        masks = [
            dext_ref[first - count + 1 + k : first - count + 1 + k + BLOCK] == own
            for k in range(count - 1)
        ]
        for c in range(width // LANES):
            cols = slice(c * LANES, (c + 1) * LANES)
            total = None
            for k in range(count):
                start = first - count + 1 + k
                term = ext_ref[start : start + BLOCK, cols] * taps[k : k + 1, cols]
                if k < count - 1:
                    term = jnp.where(masks[k], term, 0.0)
                total = term if total is None else total + term
            out_ref[b * BLOCK : (b + 1) * BLOCK, cols] = silu(total).astype(BF16)


def pack_kernel(values_ref, writes_ref, reads_ref, docs_ref, out_ref):
    wide, narrow = values_ref.shape[1], writes_ref.shape[1]
    out_ref[:, 0:wide] = values_ref[...]
    out_ref[:, wide : wide + narrow] = writes_ref[...]
    out_ref[:, wide + narrow : wide + 2 * narrow] = reads_ref[...]
    blocks = docs_ref.shape[0]
    last = jnp.broadcast_to(doc_rows(docs_ref)[blocks - 1 :], (8, BLOCK))
    column = transposed(last)[BLOCK - EDGE :, 0:1]
    out_ref[:, wide + 2 * narrow :] = jnp.broadcast_to(column, (EDGE, LANES)).astype(BF16)


def pack_edge(values, writes, reads, docs):
    tokens, wide = values.shape
    narrow = writes.shape[1]
    at = tokens // EDGE - 1
    return pl.pallas_call(
        pack_kernel,
        grid=(1,),
        in_specs=[
            pl.BlockSpec((EDGE, wide), lambda i: (at, 0)),
            pl.BlockSpec((EDGE, narrow), lambda i: (at, 0)),
            pl.BlockSpec((EDGE, narrow), lambda i: (at, 0)),
            pl.BlockSpec(docs.shape, lambda i: (0, 0)),
        ],
        out_specs=pl.BlockSpec((EDGE, wide + 2 * narrow + LANES), lambda i: (0, 0)),
        out_shape=shape((EDGE, wide + 2 * narrow + LANES), BF16),
        name="pack_edge",
    )(values, writes, reads, docs)


def state_kernel(
    before_ref,
    values_ref,
    writes_ref,
    step_ref,
    rate_ref,
    jump_ref,
    docs_ref,
    taps_values_ref,
    taps_write_ref,
    sv_ref,
    sw_ref,
    run_ref,
    stepped_ref,
    enter_ref,
    send_ref,
    ext_ref,
    wext_ref,
    dext_ref,
):
    tokens, wide = values_ref.shape
    narrow = writes_ref.shape[1]
    blocks = tokens // BLOCK
    heads = step_ref.shape[0]
    docs = doc_rows(docs_ref)
    place_docs(dext_ref, before_ref.at[:, wide + 2 * narrow :], docs, blocks)
    ext_ref[0:EDGE] = before_ref[:, 0:wide].astype(F32)
    ext_ref[EDGE:] = values_ref[...].astype(F32)
    wext_ref[0:EDGE] = before_ref[:, wide : wide + narrow].astype(F32)
    wext_ref[EDGE:] = writes_ref[...].astype(F32)
    short_filter(wext_ref, dext_ref, taps_write_ref, sw_ref, blocks, narrow)
    short_filter(ext_ref, dext_ref, taps_values_ref, sv_ref, blocks, wide)

    raw = step_ref[...].astype(F32)
    step = jnp.maximum(raw, 0.0) + jnp.log1p(jnp.exp(-jnp.abs(raw)))
    stepped_ref[...] = step
    log_decay = jump_ref[...] - rate_ref[...] * step
    held = None
    total = jnp.zeros((heads, 1), F32)
    head_size = wide // heads
    for b in range(blocks):
        span = slice(b * BLOCK, (b + 1) * BLOCK)
        run = running_sum(log_decay[:, span])
        run_ref[:, span] = run
        last = run[:, BLOCK - 1 :]
        total = total + last
        row = docs[b : b + 1]
        end = row[:, BLOCK - 1 :]
        factor = jnp.where(row == end, jnp.exp(last - run) * step[:, span], 0.0)
        columns = transposed(factor)
        scaled = jnp.concatenate(
            [
                (
                    sv_ref[span, p * LANES : (p + 1) * LANES].astype(F32)
                    * per_channel(columns, p, BLOCK)
                ).astype(BF16)
                for p in range(wide // LANES)
            ],
            axis=1,
        )
        fresh = lax.dot_general(
            scaled, sw_ref[span], (((0,), (0,)), ((), ())), preferred_element_type=F32
        )
        if held is None:
            held = fresh
        else:
            enter_ref[b - 1] = held.astype(BF16)
            passing = jnp.where(docs[b - 1 : b, BLOCK - 1 :] == end, jnp.exp(last), 0.0)
            held = jnp.concatenate(
                [
                    held[h * head_size : (h + 1) * head_size] * passing[h : h + 1]
                    + fresh[h * head_size : (h + 1) * head_size]
                    for h in range(heads)
                ]
            )
    send_ref[0:wide] = held.astype(BF16)
    behind = before_ref[EDGE - 1 : EDGE, wide + 2 * narrow :].astype(F32)
    whole = jnp.where(
        behind == docs[blocks - 1 :, BLOCK - 1 :], jnp.broadcast_to(jnp.exp(total), (heads, LANES)), 0.0
    )
    send_ref[wide:] = jnp.concatenate([whole, jnp.zeros((16 - heads, LANES), F32)]).astype(BF16)


def local_states(before, values, writes, step_raw, rate, jump, docs, taps_values, taps_write):
    tokens, wide = values.shape
    narrow = writes.shape[1]
    heads = step_raw.shape[0]
    blocks = tokens // BLOCK
    return pl.pallas_call(
        state_kernel,
        out_shape=(
            shape((tokens, wide), BF16),
            shape((tokens, narrow), BF16),
            shape((heads, tokens), F32),
            shape((heads, tokens), F32),
            shape((blocks - 1, wide, narrow), BF16),
            shape((wide + 16, narrow), BF16),
        ),
        scratch_shapes=[
            pltpu.VMEM((EDGE + tokens, wide), F32),
            pltpu.VMEM((EDGE + tokens, narrow), F32),
            pltpu.VMEM((EDGE + tokens, LANES), F32),
        ],
        cost_estimate=pl.CostEstimate(flops=400_000_000, transcendentals=0, bytes_accessed=4_000_000),
        name="local_states",
    )(before, values, writes, step_raw, rate, jump, docs, taps_values, taps_write)


def decayed(near, decay, far, heads):
    size = near.shape[0] // heads
    return jnp.concatenate(
        [
            near[h * size : (h + 1) * size] + decay[h : h + 1] * far[h * size : (h + 1) * size]
            for h in range(heads)
        ]
    )


def join_kernel(heads, own_ref, near_ref, out_ref):
    wide = out_ref.shape[0]
    own = own_ref[0:wide].astype(F32)
    decay = own_ref[wide:].astype(F32)
    out_ref[...] = decayed(own, decay, near_ref[0:wide].astype(F32), heads).astype(BF16)


def join_states(own, near, heads):
    return pl.pallas_call(
        functools.partial(join_kernel, heads),
        out_shape=shape((own.shape[0] - 16, own.shape[1]), BF16),
        name="join_states",
    )(own, near)


def inner_kernel(
    before_ref,
    reads_ref,
    docs_ref,
    taps_ref,
    sv_ref,
    sw_ref,
    run_ref,
    step_ref,
    enter_ref,
    sr_ref,
    mixed_ref,
    reach_ref,
    ext_ref,
    dext_ref,
):
    tokens, narrow = reads_ref.shape
    wide = sv_ref.shape[1]
    blocks = tokens // BLOCK
    docs = doc_rows(docs_ref)
    place_docs(dext_ref, before_ref.at[:, wide + 2 * narrow :], docs, blocks)
    ext_ref[0:EDGE] = before_ref[:, wide + narrow : wide + 2 * narrow].astype(F32)
    ext_ref[EDGE:] = reads_ref[...].astype(F32)
    short_filter(ext_ref, dext_ref, taps_ref, sr_ref, blocks, narrow)
    target = lax.broadcasted_iota(jnp.int32, (BLOCK, BLOCK), 0)
    source = lax.broadcasted_iota(jnp.int32, (BLOCK, BLOCK), 1)
    low = source < LANES // 2
    gain = None
    for b in range(blocks):
        span = slice(b * BLOCK, (b + 1) * BLOCK)
        row = docs[b : b + 1]
        column = dext_ref[EDGE + b * BLOCK : EDGE + (b + 1) * BLOCK]
        allowed = (target >= source) & (column == row)
        reads, writes = sr_ref[span], sw_ref[span]
        scores = lax.dot_general(
            reads, writes, (((1,), (1,)), ((), ())), preferred_element_type=F32
        )
        run, step = run_ref[:, span], step_ref[:, span]
        run_columns = transposed(run)
        if b == 0:
            prior = before_ref[EDGE - 1 : EDGE, wide + 2 * narrow :].astype(F32)
        else:
            prior = jnp.broadcast_to(docs[b - 1 : b, BLOCK - 1 :], (1, BLOCK))
        reach = jnp.where(row == prior, jnp.exp(run), 0.0)
        last = run[:, BLOCK - 1 :]
        passing = jnp.where(row[:, BLOCK - 1 :] == prior[:, 0:1], jnp.exp(last), 0.0)
        reach_ref[:, span] = reach if gain is None else reach * gain
        gain = passing if gain is None else gain * passing
        reach_columns = transposed(reach)
        if b > 0:
            taken = lax.dot_general(
                reads, enter_ref[b - 1], (((1,), (1,)), ((), ())), preferred_element_type=F32
            )
        for p in range(wide // LANES):
            cols = slice(p * LANES, (p + 1) * LANES)
            weights = []
            for h in (2 * p, 2 * p + 1):
                spread = run_columns[:, h : h + 1] - run[h : h + 1]
                decay = jnp.exp(jnp.where(allowed, spread, -1e30))
                weights.append((decay * scores * step[h : h + 1]).astype(BF16))
            here = sv_ref[span, cols]
            zero = jnp.zeros_like(here)
            both = jnp.concatenate([jnp.where(low, here, zero), jnp.where(low, zero, here)])
            mixed = jnp.dot(
                jnp.concatenate(weights, axis=1), both, preferred_element_type=F32
            )
            if b > 0:
                mixed = mixed + taken[:, cols] * per_channel(reach_columns, p, BLOCK)
            mixed_ref[span, cols] = mixed


def local_mix(before, reads, docs, taps, sv, sw, run, step, enter):
    tokens, narrow = reads.shape
    wide = sv.shape[1]
    heads = step.shape[0]
    return pl.pallas_call(
        inner_kernel,
        out_shape=(
            shape((tokens, narrow), BF16),
            shape((tokens, wide), F32),
            shape((heads, tokens), F32),
        ),
        scratch_shapes=[
            pltpu.VMEM((EDGE + tokens, narrow), F32),
            pltpu.VMEM((EDGE + tokens, LANES), F32),
        ],
        cost_estimate=pl.CostEstimate(flops=800_000_000, transcendentals=0, bytes_accessed=4_000_000),
        name="local_mix",
    )(before, reads, docs, taps, sv, sw, run, step, enter)


def project_kernel(
    core_ref,
    near_ref,
    far_ref,
    sr_ref,
    mixed_ref,
    reach_ref,
    gate_ref,
    gain_ref,
    weight_ref,
    mine_ref,
    other_ref,
    in_ref,
):
    tokens, wide = mixed_ref.shape
    heads = reach_ref.shape[0]
    share = mine_ref.shape[2]
    near = near_ref[0:wide].astype(F32)
    decay = near_ref[wide:].astype(F32)
    held = decayed(near, decay, far_ref[...].astype(F32), heads).astype(BF16)
    for b in range(tokens // BLOCK):
        span = slice(b * BLOCK, (b + 1) * BLOCK)
        taken = lax.dot_general(
            sr_ref[span], held, (((1,), (1,)), ((), ())), preferred_element_type=F32
        )
        columns = transposed(reach_ref[:, span])
        parts, square = [], None
        for p in range(wide // LANES):
            cols = slice(p * LANES, (p + 1) * LANES)
            mixed = mixed_ref[span, cols] + taken[:, cols] * per_channel(columns, p, BLOCK)
            part = mixed * silu(gate_ref[span, cols].astype(F32))
            parts.append(part)
            square = part * part if square is None else square + part * part
        mean = jnp.sum(square, axis=1, keepdims=True) / wide
        scale = lax.rsqrt(mean + norm_eps)
        for p, part in enumerate(parts):
            cols = slice(p * LANES, (p + 1) * LANES)
            in_ref[span, cols] = (part * scale * gain_ref[:, cols].astype(F32)).astype(BF16)
    core = core_ref[0]
    rows = in_ref[...]
    for flip, out_ref in ((1, other_ref), (0, mine_ref)):
        for k in range(out_ref.shape[0]):
            c = 2 * k + (core ^ flip)
            cols = pl.ds(pl.multiple_of(c * share, share), share)
            out_ref[k] = jnp.dot(rows, weight_ref[:, cols], preferred_element_type=F32).astype(BF16)


def vmem():
    return pl.BlockSpec(memory_space=pltpu.VMEM)


def smem():
    return pl.BlockSpec(memory_space=pltpu.SMEM)


def project(core, near, far, sr, mixed, reach, gate, gain, weight, owners):
    tokens, wide = mixed.shape
    share = weight.shape[1] // (2 * owners)
    return pl.pallas_call(
        project_kernel,
        in_specs=[smem()] + [vmem()] * 8,
        out_shape=(shape((owners, tokens, share), BF16),) * 2,
        scratch_shapes=[pltpu.VMEM((tokens, wide), BF16)],
        cost_estimate=pl.CostEstimate(
            flops=2 * tokens * wide * weight.shape[1], transcendentals=0, bytes_accessed=6_000_000
        ),
        name="project",
    )(core, near, far, sr, mixed, reach, gate, gain, weight)


def after_kernel(at_ref, parts_ref, residual_ref, own_ref, out_ref):
    total = residual_ref[...].astype(F32)
    for k in range(parts_ref.shape[0]):
        total = total + parts_ref[k].astype(F32)
    after = total.astype(BF16)
    own_ref[...] = after
    for k in range(out_ref.shape[0]):
        out_ref[k] = after


def after_mix(at, parts, residual):
    owners, tokens, share = parts.shape
    return pl.pallas_call(
        after_kernel,
        grid_spec=pltpu.PrefetchScalarGridSpec(
            num_scalar_prefetch=1,
            grid=(1,),
            in_specs=[
                pl.BlockSpec((owners, tokens, share), lambda i, at: (0, 0, 0)),
                pl.BlockSpec((tokens, share), lambda i, at: (0, at[0])),
            ],
            out_specs=[
                pl.BlockSpec((tokens, share), lambda i, at: (0, 0)),
                pl.BlockSpec((owners, tokens, share), lambda i, at: (0, 0, 0)),
            ],
        ),
        out_shape=(shape((tokens, share), BF16), shape((owners, tokens, share), BF16)),
        name="after_mix",
    )(at, parts, residual)


def normal_kernel(at_ref, mine_ref, other_ref, gain_ref, out_ref):
    owners, _, share = mine_ref.shape
    core = lax.rem(at_ref[0], 2)
    square = None
    for ref in (mine_ref, other_ref):
        for k in range(owners):
            x = ref[k].astype(F32)
            square = x * x if square is None else square + x * x
    scale = lax.rsqrt(jnp.sum(square, axis=1, keepdims=True) / (2 * owners * share) + norm_eps)
    for flip, ref in enumerate((mine_ref, other_ref)):
        for k in range(owners):
            c = 2 * k + (core ^ flip)
            cols = pl.ds(pl.multiple_of(c * share, share), share)
            out_ref[:, cols] = (
                ref[k].astype(F32) * scale * gain_ref[:, cols].astype(F32)
            ).astype(BF16)


def normalised(at, mine, other, gain):
    owners, tokens, share = mine.shape
    return pl.pallas_call(
        normal_kernel,
        in_specs=[smem(), vmem(), vmem(), vmem()],
        out_shape=shape((tokens, 2 * owners * share), BF16),
        name="normalised",
    )(at, mine, other, gain)


def mixer_kernel(tiles, at_ref, normal_ref, weight_ref, *refs):
    mine_far, other_far, mine_near, other_near = refs[:4]
    late, downs, hidden_ref, far, near, late_sem, down_sem, far_sem, near_sem = refs[4:]
    peers, units, _ = downs.shape
    tokens = hidden_ref.shape[0]
    core, chip = lax.rem(at_ref[0], 2), lax.div(at_ref[0], 2)

    heavy = []
    for t, (first, count) in enumerate(tiles):
        heavy.append(
            [
                pltpu.make_async_copy(
                    weight_ref.at[:, pl.ds(base + first, count)],
                    late.at[:, pl.ds(base + first, count)],
                    late_sem.at[t, half],
                )
                for half, base in enumerate((0, units))
            ]
        )
    heavy.append([pltpu.make_async_copy(weight_ref.at[:, pl.ds(2 * units, units)], downs, down_sem)])
    for copy in (*heavy[0], *heavy[1]):
        copy.start()
    across = (((1,), (1,)), ((), ()))
    normal = normal_ref[...]
    for t, (first, count) in enumerate(tiles):
        for copy in heavy[t]:
            copy.wait()
        if t + 2 < len(heavy):
            for copy in heavy[t + 2]:
                copy.start()
        products = []
        for base in (first, units + first):
            part = jnp.concatenate([late[k, base : base + count] for k in range(peers)], axis=1)
            products.append(
                lax.dot_general(normal, part, across, preferred_element_type=F32)
            )
        hidden_ref[:, first : first + count] = (silu(products[0]) * products[1]).astype(BF16)
    heavy[-1][0].wait()
    hidden = hidden_ref[...]
    stores = []

    def store(source, target, sem):
        copy = pltpu.make_async_copy(source, target, sem)
        copy.start()
        stores.append(copy)

    half = tokens // 2
    low, high = slice(0, half), slice(half, tokens)
    for turn in (2, 1, 3, 0):
        for flip in (1, 0):
            c = 2 * lax.rem(chip + turn, 4) + (core ^ flip)
            part = jnp.concatenate([downs[2 * c], downs[2 * c + 1]], axis=1)
            product = jnp.dot(hidden, part, preferred_element_type=F32).astype(BF16)
            if turn == 2:
                far[flip, 0, 0], far[flip, 1, 0] = product[low], product[high]
            elif turn == 1:
                far[flip, 0, 1], near[flip, 2] = product[high], product[low]
            elif turn == 3:
                far[flip, 1, 1], near[flip, 3] = product[low], product[high]
                store(far.at[flip], (mine_far, other_far)[flip], far_sem.at[flip])
            else:
                near[flip, 0], near[flip, 1] = product[low], product[high]
                store(near.at[flip], (mine_near, other_near)[flip], near_sem.at[flip])
    for copy in stores:
        copy.wait()


def channel_mixer(at, normal, weights, share):
    tokens = normal.shape[0]
    peers, units, depth = weights.shape[0], weights.shape[1] // 3, weights.shape[2]
    tiles = [(f, min(256, units - f)) for f in range(0, units, 256)]
    anywhere = pl.BlockSpec(memory_space=pl.ANY)
    far = shape((2, 2, tokens // 2, share), BF16)
    near = shape((4, tokens // 2, share), BF16)
    return pl.pallas_call(
        functools.partial(mixer_kernel, tiles),
        in_specs=[smem(), vmem(), anywhere],
        out_specs=[anywhere] * 4,
        out_shape=(far, far, near, near),
        scratch_shapes=[
            pltpu.VMEM((peers, 2 * units, depth), BF16),
            pltpu.VMEM((peers, units, depth), BF16),
            pltpu.VMEM((tokens, units), BF16),
            pltpu.VMEM((2, *far.shape), BF16),
            pltpu.VMEM((2, *near.shape), BF16),
            pltpu.SemaphoreType.DMA((len(tiles), 2)),
            pltpu.SemaphoreType.DMA,
            pltpu.SemaphoreType.DMA((2,)),
            pltpu.SemaphoreType.DMA((2,)),
        ],
        cost_estimate=pl.CostEstimate(
            flops=6 * tokens * normal.shape[1] * units, transcendentals=0, bytes_accessed=14_000_000
        ),
        name="channel_mixer",
    )(at, normal, weights)


def to_partner(value):
    return lax.ppermute(value, "tp", [(i, i ^ 1) for i in range(lax.axis_size("tp"))])


def to_chip(value, by):
    peers = lax.axis_size("tp")
    return lax.ppermute(value, "tp", [(i, (i + 2 * by) % peers) for i in range(peers)])


def sum_round(parts, after):
    mine_far, other_far, mine_near, other_near = parts
    other_far = to_partner(other_far)
    other_near = to_partner(other_near)
    first = (mine_far.astype(F32) + other_far.astype(F32)).astype(BF16)
    low, right_high = to_chip(first[0], 1)
    high, left_low = to_chip(first[1], -1)
    near = mine_near.astype(F32) + other_near.astype(F32)
    right_low = to_chip((near[2] + low.astype(F32)).astype(BF16), 1)
    left_high = to_chip((near[3] + high.astype(F32)).astype(BF16), -1)
    down = near[:2].reshape(after.shape)
    half = near.shape[1]
    for part, place in (
        (right_low, (0, half)),
        (left_low, (0, half)),
        (right_high, (half, 0)),
        (left_high, (half, 0)),
    ):
        down = down + jnp.pad(part, (place, (0, 0))).astype(F32)
    return (after.astype(F32) + down).astype(BF16)


def exchange(value):
    peers = lax.axis_size("tp")
    rows = [[i for i in range(peers) if i % 2 == core] for core in range(2)]
    return lax.all_to_all(value, "tp", 0, 0, axis_index_groups=rows, tiled=True)


def sum_pairs(both):
    return (both[0].astype(F32) + to_partner(both[1]).astype(F32)).astype(BF16)


def on_device(
    residual,
    values,
    out_gate,
    writes,
    reads,
    step_raw,
    decay_rate,
    decay_jump,
    documents,
    taps_values,
    taps_write,
    taps_read,
    mixer_gain,
    mixer_out,
    channel_gain,
    gate_weight,
    up_weight,
    down_rows,
):
    heads = step_raw.shape[0]
    owners = lax.axis_size("tp") // 2
    me = lax.axis_index("tp").astype(jnp.int32)
    at = me.reshape(1)
    core = (me % 2).reshape(1)
    late = jnp.concatenate([gate_weight.T, up_weight.T, down_rows.T], axis=0)
    weights = lax.all_gather(late, "sp", axis=0)

    docs = documents.reshape(-1, BLOCK)
    before = from_behind(pack_edge(values, writes, reads, docs), "sp", 1)
    rate = decay_rate.reshape(-1, 1)
    sv, sw, run, step, enter, send = local_states(
        before, values, writes, step_raw, rate, decay_jump, docs, taps_values, taps_write
    )
    near = from_behind(send, "sp", 1)
    sr, mixed, reach = local_mix(before, reads, docs, taps_read, sv, sw, run, step, enter)
    far = from_behind(join_states(send, near, heads), "sp", 2)
    both = project(
        core, near, far, sr, mixed, reach, out_gate, mixer_gain.reshape(1, -1), mixer_out, owners
    )
    own_after, spread = after_mix(at, exchange(sum_pairs(both)), residual)
    mine = exchange(spread)
    other = to_partner(mine)
    normal = normalised(at, mine, other, channel_gain.reshape(1, -1))
    return sum_round(channel_mixer(at, normal, weights, own_after.shape[1]), own_after)


def solution(mesh):
    return jax.shard_map(
        on_device,
        mesh=mesh,
        in_specs=(
            P(("grp", "sp"), None),
            P(("grp", "sp"), "tp"),
            P(("grp", "sp"), "tp"),
            P(("grp", "sp"), "tp"),
            P(("grp", "sp"), "tp"),
            P("tp", ("grp", "sp")),
            P("tp"),
            P("tp", ("grp", "sp")),
            P(("grp", "sp")),
            P(None, "tp"),
            P(None, "tp"),
            P(None, "tp"),
            P("tp"),
            P("tp", None),
            P(),
            P("sp", "tp"),
            P("sp", "tp"),
            P("sp", "tp"),
        ),
        out_specs=P(("grp", "sp"), "tp"),
        check_vma=False,
    )
```
